32 devices in a mesh: sp: 8 (over z, y), tp: 4 (over x, core).
Axes of the slice: x: 2, y: 2, z: 4, core: 2. Of those that a mesh axis runs over, the one named last changes fastest.
Arguments:
- residual: bfloat16 [4096, 2048], P(('sp', 'tp')), may hold values from -6 to 6
- query_major: bfloat16 [4096, 1024], P('sp', 'tp'), may hold values from -160 to 160
- keys_major: bfloat16 [4096, 1024], P('sp', 'tp'), may hold values from -6.5 to 6.5
- values_major: bfloat16 [4096, 1024], P('sp', 'tp'), may hold values from -6 to 6
- query_minor: bfloat16 [4096, 512], P('sp', 'tp'), may hold values from -160 to 160
- keys_minor: bfloat16 [4096, 512], P('sp', 'tp'), may hold values from -6.5 to 6.5
- values_minor: bfloat16 [4096, 512], P('sp', 'tp'), may hold values from -6 to 6
- lambda_major: float32 [8], P('tp'), may hold values from 0.3 to 0.8
- lambda_minor: float32 [8], P('tp'), may hold values from 0.3 to 0.8
- gain_major: float32 [128], replicated, may hold values from 0.1 to 1.9
- gain_minor: float32 [64], replicated, may hold values from 0.1 to 1.9
- output_major: bfloat16 [1024, 2048], P('tp'), may hold values from -0.15625 to 0.15625
- output_minor: bfloat16 [512, 2048], P('tp'), may hold values from -0.15625 to 0.15625
- mixer_gain: float32 [2048], replicated, may hold values from 0.1 to 1.9
- up_weight: bfloat16 [2048, 8192], P('sp', 'tp'), may hold values from -0.125 to 0.125
- down_weight: bfloat16 [8192, 2048], P('tp', 'sp'), may hold values from -0.0625 to 0.0625
Outputs:
- layer_out: bfloat16 [4096, 2048], P(('sp', 'tp'))
The draws below stay inside these ranges and needn't reach their ends.
All inputs are finite; a program needn't handle non-finite values.
Results may differ from the reference program's by a relative error of at most 0.018.
Values may be sent and summed in bfloat16 or wider, within the bound.
A program may use at most 128 MiB of HBM per device.

```python
import jax
import jax.numpy as jnp
from jax import lax

D_MODEL = 2048
D_FF = 8192
H_MAJOR = 8
DK_MAJOR = 64
H_MINOR = 8
DK_MINOR = 32
DV_MAJOR = 128
DV_MINOR = 64
SEGMENT = 64
TOKENS = 4096
N_TP = 4


def drawn(key, head_count, key_size):
    key_query, key_keys = jax.random.split(key, 2)
    shape = (TOKENS, head_count, 2, key_size)
    queries = jnp.clip(jax.random.normal(key_query, shape, jnp.float32), -5.0, 5.0) * 1.3
    key_rows = jnp.clip(jax.random.normal(key_keys, shape, jnp.float32), -5.0, 5.0) * 1.3
    width_all = head_count * 2 * key_size
    return (queries.reshape(TOKENS, width_all), key_rows.reshape(TOKENS, width_all))


def draw_query_major(key, part):
    return drawn(jax.random.fold_in(key, 1), H_MAJOR, DK_MAJOR)[0].astype(jnp.bfloat16)


def draw_keys_major(key, part):
    return drawn(jax.random.fold_in(key, 1), H_MAJOR, DK_MAJOR)[1].astype(jnp.bfloat16)


def draw_query_minor(key, part):
    return drawn(jax.random.fold_in(key, 2), H_MINOR, DK_MINOR)[0].astype(jnp.bfloat16)


def draw_keys_minor(key, part):
    return drawn(jax.random.fold_in(key, 2), H_MINOR, DK_MINOR)[1].astype(jnp.bfloat16)


def shard_levels(stream_key, dims, cuts, low, high):
    gain, own = 1.0, jax.random.fold_in(stream_key, 6)
    for axis_at, blocks in cuts:
        draws = jnp.exp(jax.random.uniform(jax.random.fold_in(own, axis_at), (blocks,), jnp.float32, low / len(cuts), high / len(cuts)))
        gain = gain * jnp.repeat(draws, dims[axis_at] // blocks).reshape([-1 if axis == axis_at else 1 for axis in range(len(dims))])
    return gain


def normal_values(rng, dims, width, reach, shards=(), kind=jnp.bfloat16):
    gain = shard_levels(rng, dims, shards, -0.22, 0.18) if shards else 1.0
    result = jax.random.normal(rng, dims, jnp.float32) * width * gain
    return jnp.minimum(jnp.maximum(result, -reach), reach).astype(kind)


def setup_inputs(seed: int = 0) -> dict:
    keys = jax.random.split(jax.random.key(seed), 17)
    residual = normal_values(keys[0], (TOKENS, D_MODEL), 1.0, 6.0, ((0, 32),))
    query_major = draw_query_major(jax.random.fold_in(keys[16], 71), 0)
    keys_major = draw_keys_major(jax.random.fold_in(keys[16], 71), 0)
    values_major = normal_values(keys[3], (TOKENS, H_MAJOR * DV_MAJOR), 1.0, 6.0, ((0, 8), (1, 4)))
    query_minor = draw_query_minor(jax.random.fold_in(keys[16], 71), 0)
    keys_minor = draw_keys_minor(jax.random.fold_in(keys[16], 71), 0)
    values_minor = normal_values(keys[6], (TOKENS, H_MINOR * DV_MINOR), 1.0, 6.0, ((0, 8), (1, 4)))
    lambda_major = jnp.clip(0.3 + 0.5 * jax.random.uniform(keys[7], (H_MAJOR,), jnp.float32) ** shard_levels(keys[7], (H_MAJOR,), ((0, 4),), -0.2, 0.2), 0.3, 0.8)
    lambda_minor = jnp.clip(0.3 + 0.5 * jax.random.uniform(keys[8], (H_MINOR,), jnp.float32) ** shard_levels(keys[8], (H_MINOR,), ((0, 4),), -0.2, 0.2), 0.3, 0.8)
    gain_major = jnp.clip(1.0 + 0.18 * jax.random.normal(keys[9], (DV_MAJOR,), jnp.float32), 0.1, 1.9)
    gain_minor = jnp.clip(1.0 + 0.18 * jax.random.normal(keys[10], (DV_MINOR,), jnp.float32), 0.1, 1.9)
    output_major = normal_values(keys[11], (H_MAJOR * DV_MAJOR, D_MODEL), (H_MAJOR * DV_MAJOR + H_MINOR * DV_MINOR) ** -0.5, 0.15625, ((0, 4),))
    output_minor = normal_values(keys[12], (H_MINOR * DV_MINOR, D_MODEL), (H_MAJOR * DV_MAJOR + H_MINOR * DV_MINOR) ** -0.5, 0.15625, ((0, 4),))
    mixer_gain = jnp.clip(1.0 + 0.18 * jax.random.normal(keys[13], (D_MODEL,), jnp.float32), 0.1, 1.9)
    up_weight = normal_values(keys[14], (D_MODEL, D_FF), D_MODEL ** -0.5, 0.125, ((0, 8), (1, 4)))
    down_weight = normal_values(keys[15], (D_FF, D_MODEL), D_FF ** -0.5, 0.0625, ((0, 4), (1, 8)))
    return {"residual": residual, "query_major": query_major, "keys_major": keys_major, "values_major": values_major, "query_minor": query_minor, "keys_minor": keys_minor, "values_minor": values_minor, "lambda_major": lambda_major, "lambda_minor": lambda_minor, "gain_major": gain_major, "gain_minor": gain_minor, "output_major": output_major, "output_minor": output_minor, "mixer_gain": mixer_gain, "up_weight": up_weight, "down_weight": down_weight}


EPSILON = 1e-06

def to_wire(value):
    return lax.optimization_barrier(value.astype(jnp.bfloat16)).astype(jnp.float32)

def head_group(queries, key_rows, values, lambdas, scaling, head_count, key_size):
    value_size = values.shape[1] // head_count
    block_len = 512 if TOKENS % 512 == 0 else TOKENS
    key_pos = jnp.arange(TOKENS, dtype=jnp.int32)
    keys_all = key_rows.astype(jnp.float32).reshape(TOKENS, head_count, 2, key_size)
    values_all = values.astype(jnp.float32).reshape(TOKENS, head_count, value_size)

    def one_block(block_id):
        first_row = (block_id * block_len).astype(jnp.int32)
        query_block = lax.dynamic_slice_in_dim(queries, first_row, block_len, 0).astype(jnp.float32)
        query_block = query_block.reshape(block_len, head_count, 2, key_size)
        query_pos = first_row + jnp.arange(block_len, dtype=jnp.int32)
        visible = key_pos[None, :] // SEGMENT <= query_pos[:, None] // SEGMENT

        def one_head(head_id):
            query_head = lax.dynamic_index_in_dim(query_block, head_id, 1, keepdims=False)
            keys_head = lax.dynamic_index_in_dim(keys_all, head_id, 1, keepdims=False)
            values_head = lax.dynamic_index_in_dim(values_all, head_id, 1, keepdims=False)
            scores = jnp.einsum('qmd,kmd->mqk', query_head, keys_head) * key_size ** (-0.5)
            scores = jnp.where(visible[None], scores, -jnp.inf)
            peak = lax.optimization_barrier(jnp.max(scores, axis=-1, keepdims=True))
            weights = jnp.where(visible[None], jnp.exp(scores - peak), 0.0)
            totals = lax.optimization_barrier(jnp.sum(weights, axis=-1))
            sums = jnp.einsum('mqk,ke->mqe', to_wire(weights), values_head)
            lam_head = lambdas[head_id]
            output = sums[0] / totals[0][:, None] - lam_head * sums[1] / totals[1][:, None]
            output = output * lax.rsqrt(lax.optimization_barrier(jnp.mean(output * output, axis=-1, keepdims=True)) + EPSILON) * scaling
            return output.astype(jnp.bfloat16)
        per_head = lax.map(one_head, jnp.arange(head_count, dtype=jnp.int32))
        return jnp.transpose(per_head, (1, 0, 2)).reshape(block_len, head_count * value_size)
    blocks = lax.map(one_block, jnp.arange(TOKENS // block_len, dtype=jnp.int32))
    return blocks.reshape(TOKENS, head_count * value_size)

def reference(residual, query_major, keys_major, values_major, query_minor, keys_minor, values_minor, lambda_major, lambda_minor, gain_major, gain_minor, output_major, output_minor, mixer_gain, up_weight, down_weight):
    heads_major = head_group(query_major, keys_major, values_major, lambda_major, gain_major, H_MAJOR, DK_MAJOR)
    heads_minor = head_group(query_minor, keys_minor, values_minor, lambda_minor, gain_minor, H_MINOR, DK_MINOR)
    cols_major = H_MAJOR * DV_MAJOR // N_TP
    cols_minor = H_MINOR * DV_MINOR // N_TP
    mixed = jnp.zeros((TOKENS, D_MODEL), jnp.float32)
    for group in range(N_TP):
        partial_sum = jnp.dot(heads_major[:, group * cols_major:(group + 1) * cols_major], output_major[group * cols_major:(group + 1) * cols_major], preferred_element_type=jnp.float32)
        partial_sum = partial_sum + jnp.dot(heads_minor[:, group * cols_minor:(group + 1) * cols_minor], output_minor[group * cols_minor:(group + 1) * cols_minor], preferred_element_type=jnp.float32)
        mixed = mixed + to_wire(partial_sum)
    stream = residual.astype(jnp.float32) + mixed
    normed = stream * lax.rsqrt(lax.optimization_barrier(jnp.mean(stream * stream, axis=-1, keepdims=True)) + EPSILON) * mixer_gain
    normed = normed.astype(jnp.bfloat16)
    hidden = jnp.square(jax.nn.relu(jnp.dot(normed, up_weight, preferred_element_type=jnp.float32)))
    hidden = hidden.astype(jnp.bfloat16)
    cols_ff = D_FF // N_TP
    down_sum = jnp.zeros((TOKENS, D_MODEL), jnp.float32)
    for group in range(N_TP):
        partial_sum = jnp.dot(hidden[:, group * cols_ff:(group + 1) * cols_ff], down_weight[group * cols_ff:(group + 1) * cols_ff], preferred_element_type=jnp.float32)
        down_sum = down_sum + to_wire(partial_sum)
    return (stream + down_sum).astype(jnp.bfloat16)
```

```python
import functools

import jax
import jax.numpy as jnp
from jax import lax
from jax.experimental import pallas as pl
from jax.experimental.pallas import tpu as pltpu
from jax.sharding import PartitionSpec as P

DK_MAJOR = 64
DK_MINOR = 32
SEGMENT = 64
MAPS = 2

EPSILON = 1e-06
NEGATIVE = -1e30
LOG2_E = 1.4426950408889634
ANY = pl.BlockSpec(memory_space=pl.ANY)
VMEM = pl.BlockSpec(memory_space=pltpu.VMEM)
SMEM = pl.BlockSpec(memory_space=pltpu.SMEM)


def grid_sizes(sp_count):
    y_count = 1 << ((sp_count.bit_length() - 1) // 2)
    return sp_count // y_count, y_count


class Gather:
    def __init__(self, sp_count, places, send_sem, recv_sem):
        self.z_count, self.y_count = grid_sizes(sp_count)
        own = lax.axis_index("sp")
        self.own, self.z, self.y = own, own // self.y_count, lax.rem(own, self.y_count)
        self.places, self.send_sem, self.recv_sem = places, send_sem, recv_sem
        self.copies = []

    def z_peer(self, step):
        return lax.rem(self.z + step, self.z_count) * self.y_count + self.y

    def y_peer(self, step):
        return self.z * self.y_count + lax.rem(self.y + step, self.y_count)

    def send(self, array, source, src_ref, target):
        copy = pltpu.make_async_remote_copy(
            src_ref=src_ref,
            dst_ref=self.places[array](source),
            send_sem=self.send_sem.at[array, len([c for c in self.copies if c[0] == array])],
            recv_sem=self.recv_sem.at[array, source],
            device_id={"sp": target},
            device_id_type=pl.DeviceIdType.MESH,
        )
        copy.start()
        self.copies.append((array, copy))

    def wait_block(self, array, source):
        place = self.places[array](source)
        pltpu.make_async_remote_copy(
            src_ref=place,
            dst_ref=place,
            send_sem=self.send_sem.at[array, 0],
            recv_sem=self.recv_sem.at[array, source],
            device_id={"sp": self.y_peer(1)},
            device_id_type=pl.DeviceIdType.MESH,
        ).wait_recv()

    def send_z(self, array, src_ref):
        for step in range(1, self.z_count):
            self.send(array, self.own, src_ref, self.z_peer(step))

    def send_y(self, array, src_ref):
        for step in range(1, self.y_count):
            self.send(array, self.own, src_ref, self.y_peer(step))

    def pass_on(self, array, step):
        source = self.z_peer(self.z_count - step)
        self.wait_block(array, source)
        for y_step in range(1, self.y_count):
            self.send(array, source, self.places[array](source), self.y_peer(y_step))

    def wait_y(self, array):
        for y_step in range(1, self.y_count):
            for z_step in range(self.z_count):
                z_at = lax.rem(self.z + z_step, self.z_count)
                self.wait_block(array, z_at * self.y_count + lax.rem(self.y + y_step, self.y_count))

    def finish(self):
        for _, copy in self.copies:
            copy.wait_send()


def mixer_kernel(
    sp_count,
    groups,
    q_major,
    k_major,
    v_major,
    q_minor,
    kv_minor,
    lam_major,
    lam_minor,
    gain_major,
    gain_minor,
    up_ref,
    down_ref,
    out_major,
    out_minor,
    up_all,
    down_all,
    k_major_all,
    v_major_all,
    kv_minor_all,
    qm_major,
    qm_minor,
    acc_major,
    acc_minor,
    peaks,
    totals,
    send_sem,
    recv_sem,
    local_sem,
):
    rows = q_major.shape[0]
    up_rows = up_ref.shape[0]

    def rows_of(ref, count):
        return lambda source: ref.at[pl.ds(pl.multiple_of(source * count, count), count), :]

    places = [
        rows_of(k_major_all, rows),
        rows_of(v_major_all, rows),
        rows_of(kv_minor_all, rows),
        rows_of(up_all, up_rows),
        lambda source: down_all.at[source],
    ]
    own_refs = [k_major, v_major, kv_minor, up_ref, down_ref]
    gather = Gather(sp_count, places, send_sem, recv_sem)
    own = gather.own

    barrier = pltpu.get_barrier_semaphore()
    peers = [gather.z_peer(step) for step in range(1, gather.z_count)]
    peers += [gather.y_peer(step) for step in range(1, gather.y_count)]
    for peer in peers:
        pl.semaphore_signal(
            barrier, inc=1, device_id={"sp": peer}, device_id_type=pl.DeviceIdType.MESH
        )
    pl.semaphore_wait(barrier, len(peers))

    for array in range(3):
        gather.send_z(array, own_refs[array])
    for array in range(3):
        gather.send_y(array, own_refs[array])
    for array in (3, 4):
        gather.send_z(array, own_refs[array])
    for array in (3, 4):
        gather.send_y(array, own_refs[array])
    local = []
    for slot, array in enumerate((3, 4)):
        copy = pltpu.make_async_copy(own_refs[array], places[array](own), local_sem.at[slot])
        copy.start()
        local.append(copy)

    heads = []
    for group, (head_count, key_size) in enumerate(groups):
        q_ref, qm_ref = ((q_major, qm_major), (q_minor, qm_minor))[group]
        acc_ref = (acc_major, acc_minor)[group]
        value_size = acc_ref.shape[1]
        lanes = qm_ref.shape[2]
        for head in range(head_count):
            first = head * MAPS * key_size
            lane_first = first // lanes * lanes
            block = q_ref[:, lane_first : lane_first + lanes]
            lane = lax.broadcasted_iota(jnp.int32, block.shape, 1) + lane_first
            for m in range(MAPS):
                low = first + m * key_size
                keep = (lane >= low) & (lane < low + key_size)
                picked = jnp.where(keep, block.astype(jnp.float32), 0.0).astype(block.dtype)
                qm_ref[head, m * rows : (m + 1) * rows, :] = picked
            heads.append((group, head, len(heads), lane_first, lanes, value_size, key_size))

    minor_keys = q_minor.shape[1]
    minor_first = minor_keys // 128 * 128

    def fold(key_refs, value_refs, at, diagonal):
        window = pl.ds(at, rows)
        stored = (value_refs[0][window, :], value_refs[1][window, minor_first:])
        turned = [jnp.transpose(v.astype(jnp.float32)).astype(jnp.bfloat16) for v in stored]
        turned[1] = turned[1][minor_keys - minor_first :, :]
        for group, head, index, lane_first, lanes, value_size, key_size in heads:
            qm_ref = (qm_major, qm_minor)[group]
            acc_ref = (acc_major, acc_minor)[group]
            keys = key_refs[group][window, lane_first : lane_first + lanes]
            values = turned[group][head * value_size : (head + 1) * value_size, :]
            scores = lax.dot_general(
                keys, qm_ref[head], (((1,), (1,)), ((), ())), preferred_element_type=jnp.float32
            ) * (key_size ** (-0.5) * LOG2_E)
            if diagonal:
                key_pos = lax.broadcasted_iota(jnp.int32, scores.shape, 0)
                query_pos = lax.broadcasted_iota(jnp.int32, scores.shape, 1) % rows
                visible = key_pos // SEGMENT <= query_pos // SEGMENT
                scores = jnp.where(visible, scores, NEGATIVE)
            peak = jnp.max(scores, axis=0, keepdims=True)
            if not diagonal:
                peak_old = peaks[index]
                peak = jnp.maximum(peak, peak_old)
            weights = jnp.exp2(scores - peak)
            total = jnp.sum(weights, axis=0, keepdims=True)
            sums = jnp.dot(
                values, weights.astype(jnp.bfloat16), preferred_element_type=jnp.float32
            )
            if not diagonal:
                factor = jnp.exp2(peak_old - peak)
                total = total + totals[index] * factor
                sums = sums + acc_ref[head] * factor
            peaks[index] = peak
            totals[index] = total
            acc_ref[head] = sums

    fold((k_major, kv_minor), (v_major, kv_minor), 0, True)

    for step in range(1, gather.z_count):
        for array in range(3):
            gather.pass_on(array, step)

    def earlier(block, carry):
        at = pl.multiple_of(block * rows, rows)
        fold((k_major_all, kv_minor_all), (v_major_all, kv_minor_all), at, False)
        return carry

    y_count = gather.y_count

    def same_y(z_at, carry):
        return earlier(z_at * y_count + gather.y, carry)

    def other_y(index, carry):
        z_at, place = index // (y_count - 1), lax.rem(index, y_count - 1)
        y_at = place + (place >= gather.y).astype(jnp.int32)
        return earlier(z_at * y_count + y_at, carry)

    lax.fori_loop(0, gather.z, same_y, 0)
    for array in range(3):
        gather.wait_y(array)
    lax.fori_loop(0, gather.z * (y_count - 1) + gather.y, other_y, 0)

    for group, (head_count, _) in enumerate(groups):
        acc_ref = (acc_major, acc_minor)[group]
        lam_ref = (lam_major, lam_minor)[group]
        gain_ref = (gain_major, gain_minor)[group]
        out_ref = (out_major, out_minor)[group]
        done = []
        for head in range(head_count):
            index = next(h[2] for h in heads if h[0] == group and h[1] == head)
            ratio = acc_ref[head] / totals[index]
            diff = ratio[:, :rows] - lam_ref[head] * ratio[:, rows:]
            mean = jnp.mean(diff * diff, axis=0, keepdims=True)
            done.append(diff * lax.rsqrt(mean + EPSILON) * gain_ref[...])
        out_ref[...] = jnp.transpose(jnp.concatenate(done, axis=0)).astype(out_ref.dtype)

    for step in range(1, gather.z_count):
        for array in (3, 4):
            gather.pass_on(array, step)
    for array in (3, 4):
        gather.wait_y(array)
    for copy in local:
        copy.wait()
    gather.finish()


def mixer(sp_count, *args):
    q_major, k_major, v_major, q_minor, kv_minor = args[:5]
    up_weight, down_weight = args[9:11]
    heads_major = k_major.shape[1] // (MAPS * DK_MAJOR)
    heads_minor = q_minor.shape[1] // (MAPS * DK_MINOR)
    rows = q_major.shape[0]
    size_major = v_major.shape[1] // heads_major
    width_minor = kv_minor.shape[1] - q_minor.shape[1]
    size_minor = width_minor // heads_minor
    lanes_major = min(MAPS * DK_MAJOR, q_major.shape[1])
    lanes_minor = min(128, q_minor.shape[1])
    z_count, y_count = grid_sizes(sp_count)
    sends = (z_count - 1) + (y_count - 1) * z_count
    tokens = rows * sp_count
    bf16, f32 = jnp.bfloat16, jnp.float32
    head_total = heads_major + heads_minor
    return pl.pallas_call(
        functools.partial(
            mixer_kernel, sp_count, ((heads_major, DK_MAJOR), (heads_minor, DK_MINOR))
        ),
        out_shape=(
            jax.ShapeDtypeStruct(v_major.shape, bf16),
            jax.ShapeDtypeStruct((rows, width_minor), bf16),
            jax.ShapeDtypeStruct((up_weight.shape[0] * sp_count, up_weight.shape[1]), bf16),
            jax.ShapeDtypeStruct((sp_count, *down_weight.shape), bf16),
        ),
        in_specs=[VMEM] * 5 + [SMEM] * 2 + [VMEM] * 4,
        out_specs=(VMEM, VMEM, ANY, ANY),
        scratch_shapes=[
            pltpu.VMEM((tokens, k_major.shape[1]), bf16),
            pltpu.VMEM((tokens, v_major.shape[1]), bf16),
            pltpu.VMEM((tokens, kv_minor.shape[1]), bf16),
            pltpu.VMEM((heads_major, MAPS * rows, lanes_major), bf16),
            pltpu.VMEM((heads_minor, MAPS * rows, lanes_minor), bf16),
            pltpu.VMEM((heads_major, size_major, MAPS * rows), f32),
            pltpu.VMEM((heads_minor, size_minor, MAPS * rows), f32),
            pltpu.VMEM((head_total, 1, MAPS * rows), f32),
            pltpu.VMEM((head_total, 1, MAPS * rows), f32),
            pltpu.SemaphoreType.DMA((5, sends)),
            pltpu.SemaphoreType.DMA((5, sp_count)),
            pltpu.SemaphoreType.DMA((2,)),
        ],
        compiler_params=pltpu.CompilerParams(
            collective_id=0, has_side_effects=True, vmem_limit_bytes=60 * 1024 * 1024
        ),
    )(*args)


class Exchange:
    def __init__(self, tp_count, send_sem, recv_sem):
        own = lax.axis_index("tp")
        self.x_count = tp_count // 2
        self.own, self.x, self.core = own, own // 2, lax.rem(own, 2)
        self.partner = self.x * 2 + 1 - self.core
        self.send_sem, self.recv_sem = send_sem, recv_sem

    def enter(self):
        barrier = pltpu.get_barrier_semaphore()
        peers = [self.partner] + [self.x_peer(step) for step in range(1, self.x_count)]
        for peer in peers:
            pl.semaphore_signal(
                barrier, inc=1, device_id={"tp": peer}, device_id_type=pl.DeviceIdType.MESH
            )
        pl.semaphore_wait(barrier, len(peers))

    def x_peer(self, step):
        return lax.rem(self.x + step, self.x_count) * 2 + self.core

    def copy(self, src, dst, slot, target):
        made = pltpu.make_async_remote_copy(
            src_ref=src,
            dst_ref=dst,
            send_sem=self.send_sem.at[slot],
            recv_sem=self.recv_sem.at[slot],
            device_id={"tp": target},
            device_id_type=pl.DeviceIdType.MESH,
        )
        made.start()
        return made

    def total(self, partial, pair_in, pair_sum, x_in, rows):
        def block(x_at, core):
            return pl.ds(pl.multiple_of((x_at * 2 + core) * rows, rows), rows)

        steps = list(range(1, self.x_count)) + [0]
        at = [lax.rem(self.x + step, self.x_count) for step in range(self.x_count)]
        pair = {}
        for step in steps:
            pair[step] = self.copy(
                partial.at[block(at[step], 1 - self.core), :], pair_in.at[step], step, self.partner
            )
        across = []
        for step in steps:
            pair[step].wait_recv()
            mine = partial[block(at[step], self.core), :].astype(jnp.float32)
            both = mine + pair_in[step].astype(jnp.float32)
            if step:
                pair_sum[step] = both.astype(jnp.bfloat16)
                across.append(
                    self.copy(
                        pair_sum.at[step], x_in.at[step], self.x_count + step, self.x_peer(step)
                    )
                )
        for made in across:
            made.wait_recv()
        for step in range(1, self.x_count):
            both = both + x_in[step].astype(jnp.float32)
        return both, list(pair.values()) + across


def mix_kernel(
    tp_count, partial, residual, gain, stream_ref, normed_ref, pair_in, pair_sum, x_in, held, send_sem, recv_sem
):
    exchange = Exchange(tp_count, send_sem, recv_sem)
    exchange.enter()
    rows = residual.shape[0]
    mixed, copies = exchange.total(partial, pair_in, pair_sum, x_in, rows)
    stream = residual[...].astype(jnp.float32) + mixed
    stream_ref[...] = stream
    mean = jnp.mean(stream * stream, axis=-1, keepdims=True)
    normed = (stream * lax.rsqrt(mean + EPSILON) * gain[...]).astype(jnp.bfloat16)
    held[...] = normed

    def place(index):
        return normed_ref.at[pl.ds(pl.multiple_of(index * rows, rows), rows), :]

    base, count = 2 * exchange.x_count, exchange.x_count
    sent = [exchange.copy(held, place(exchange.own), base + step, exchange.x_peer(step)) for step in range(1, count)]
    passed = [exchange.copy(held, place(exchange.own), base + count, exchange.partner)]
    normed_ref[pl.ds(pl.multiple_of(exchange.own * rows, rows), rows), :] = normed
    for step in range(1, count):
        sent[step - 1].wait_recv()
        source = exchange.x_peer(count - step)
        passed.append(
            exchange.copy(place(source), place(source), base + count + step, exchange.partner)
        )
    for made in passed:
        made.wait_recv()
    for made in copies + sent + passed:
        made.wait_send()


def sum_kernel(tp_count, partial, stream, out_ref, pair_in, pair_sum, x_in, send_sem, recv_sem):
    exchange = Exchange(tp_count, send_sem, recv_sem)
    exchange.enter()
    total, copies = exchange.total(partial, pair_in, pair_sum, x_in, stream.shape[0])
    out_ref[...] = (stream[...] + total).astype(out_ref.dtype)
    for made in copies:
        made.wait_send()


def tp_call(kernel, identity, inputs, out_shape, rows, holds):
    tp_count = lax.axis_size("tp")
    slots = (tp_count // 2, rows, inputs[0].shape[1])
    held = [pltpu.VMEM(slots[1:], jnp.bfloat16)] if holds else []
    return pl.pallas_call(
        functools.partial(kernel, tp_count),
        out_shape=out_shape,
        in_specs=[VMEM] * len(inputs),
        out_specs=jax.tree.map(lambda _: VMEM, out_shape),
        scratch_shapes=[pltpu.VMEM(slots, jnp.bfloat16)] * 3
        + held
        + [pltpu.SemaphoreType.DMA((2 * tp_count,))] * 2,
        compiler_params=pltpu.CompilerParams(
            collective_id=identity, has_side_effects=True, vmem_limit_bytes=32 * 1024 * 1024
        ),
    )(*inputs)


class Sender:
    def __init__(self, sem):
        self.sem, self.made = sem, []

    def prepare(self, src, dst, recv, target, when=None):
        copy = pltpu.make_async_remote_copy(
            src_ref=src,
            dst_ref=dst,
            send_sem=self.sem.at[len(self.made)],
            recv_sem=recv,
            device_id=target,
            device_id_type=pl.DeviceIdType.MESH,
        )
        self.made.append((when, copy))
        return lambda: run_when(when, copy.start)

    def send(self, src, dst, recv, target, when=None):
        self.prepare(src, dst, recv, target, when)()

    def finish(self):
        for when, copy in self.made:
            run_when(when, copy.wait_send)


def run_when(when, action):
    if when is None:
        action()
    else:
        pl.when(when)(lambda: action())


def layer_kernel(
    sizes,
    residual,
    q_major,
    k_major,
    v_major,
    q_minor,
    k_minor,
    v_minor,
    lam_major,
    lam_minor,
    gain_major,
    gain_minor,
    wo_major,
    wo_minor,
    mixer_gain,
    up_ref,
    down_ref,
    out_ref,
    pack,
    kv_all,
    q_in,
    qm,
    acc,
    peaks,
    totals,
    heads_out,
    cat,
    minor_in,
    wo_all,
    stream,
    normed_all,
    up_all,
    down_all,
    hidden,
    d_send,
    d_in,
    mine,
    x_send,
    x_in,
    x_keep,
    z_send,
    z_in,
    z_keep,
    send_sem,
    relay_sem,
    local_sem,
    r_y,
    r_near,
    r_far,
    r_w,
    r_wo,
    r_h,
    r_g,
    r_d,
    r_x,
    r_z,
):
    z_count, y_count, x_count = sizes
    bf16, f32 = jnp.bfloat16, jnp.float32
    own, tp = lax.axis_index("sp"), lax.axis_index("tp")
    z, y = own // y_count, lax.rem(own, y_count)
    x, c = tp // 2, lax.rem(tp, 2)
    oy, ox, oc = 1 - y, 1 - x, 1 - c
    zl = lax.rem(z, 2)
    oz = z + 1 - 2 * zl
    rows, tile = q_major.shape[0], residual.shape[0]
    width = q_minor.shape[1]
    half = width // 2
    hid = up_ref.shape[1] // 2
    up_rows = up_ref.shape[0]
    cols = down_ref.shape[1]

    def dev(z_at=z, y_at=y, x_at=x, c_at=c):
        return {"sp": z_at * y_count + y_at, "tp": x_at * 2 + c_at}

    def span(start, count):
        return pl.ds(pl.multiple_of(start * count, count), count)

    def arrive(place, recv):
        pltpu.make_async_remote_copy(
            src_ref=place,
            dst_ref=place,
            send_sem=send_sem.at[0],
            recv_sem=recv,
            device_id=dev(y_at=oy),
            device_id_type=pl.DeviceIdType.MESH,
        ).wait_recv()

    k_low = lax.broadcasted_iota(jnp.int32, (rows, width), 1)
    for head in range(2):
        k_part = (k_low >= head * half) & (k_low < (head + 1) * half)
        turned_v = pltpu.roll(v_minor[...].astype(f32), half, 1)
        pack[head] = jnp.where(k_part, k_minor[...].astype(f32), turned_v).astype(bf16)

    barrier = pltpu.get_barrier_semaphore()
    peers = []
    for dy in range(2):
        for dx in range(2):
            for dc in range(2):
                if dy or dx or dc:
                    peers.append(dev(y_at=oy if dy else y, x_at=ox if dx else x, c_at=oc if dc else c))
    peers += [dev(z_at=lax.rem(z + step, z_count)) for step in range(1, z_count)]
    for peer in peers:
        pl.semaphore_signal(barrier, inc=1, device_id=peer, device_id_type=pl.DeviceIdType.MESH)

    kv_all[z, 0, span(y, rows), :] = k_major[:, span(y, width)]
    kv_all[z, 1, span(y, rows), :] = v_major[:, span(y, width)]
    kv_all[z, 2, span(y, rows), :] = pack[y]
    local = []
    local_pairs = [
        (up_ref.at[:, span(zl, hid)], up_all.at[span(own, up_rows), :]),
        (down_ref.at[span(zl, hid), :], down_all.at[own]),
    ]
    major_rows, minor_rows = wo_major.shape[0], wo_minor.shape[0]
    tp_count = 2 * x_count
    minor_base = tp_count * major_rows

    def wo_place(part, index):
        if part == 0:
            return wo_all.at[span(index, major_rows), :]
        return wo_all.at[pl.ds(pl.multiple_of(minor_base + index * minor_rows, minor_rows), minor_rows), :]

    for part, ref in enumerate((wo_major, wo_minor)):
        local_pairs.append((ref, wo_place(part, tp)))
    for slot, (src, dst) in enumerate(local_pairs):
        made = pltpu.make_async_copy(src, dst, local_sem.at[slot])
        made.start()
        local.append(made)

    pl.semaphore_wait(barrier, len(peers))

    sender = Sender(send_sem)
    has_up = z < z_count - 1
    next_z = jnp.minimum(z + 1, z_count - 1)

    def kv_place(z_at, part, side):
        return kv_all.at[z_at, part, span(side, rows), :]

    for part, src in enumerate((k_major.at[:, span(oy, width)], v_major.at[:, span(oy, width)], pack.at[oy])):
        sender.send(src, kv_place(z, part, y), r_y.at[part], dev(y_at=oy))
    sender.send(q_major.at[:, span(oy, width)], q_in.at[0], r_y.at[3], dev(y_at=oy))
    sender.send(q_minor, q_in.at[1], r_y.at[4], dev(y_at=oy))
    for part, src in enumerate((k_major.at[:, span(y, width)], v_major.at[:, span(y, width)], pack.at[y])):
        sender.send(src, kv_place(z, part, y), r_near.at[y, part], dev(z_at=next_z), has_up)

    def weight_src(kind, z_at):
        parity = span(lax.rem(z_at, 2), hid)
        return up_ref.at[:, parity] if kind == 0 else down_ref.at[parity, :]

    def weight_place(kind, source):
        return up_all.at[span(source, up_rows), :] if kind == 0 else down_all.at[source]

    def send_weight(kind, z_at, y_at, when=None):
        return sender.prepare(
            weight_src(kind, z_at), weight_place(kind, own), r_w.at[kind, own], dev(z_at=z_at, y_at=y_at), when
        )

    for kind in range(2):
        for step in range(z_count - 1, 0, -1):
            send_weight(kind, jnp.maximum(z - step, 0), y, z >= step)()
    send_weight(0, z, oy)()
    send_weight(1, z, oy)()
    for part, ref in enumerate((wo_major, wo_minor)):
        for dx, dc in ((0, 1), (1, 0), (1, 1)):
            target = dev(x_at=ox if dx else x, c_at=oc if dc else c)
            sender.send(ref, wo_place(part, tp), r_wo.at[part, tp], target)

    up_sends = []
    for kind in range(2):
        for step in range(1 + kind, z_count):
            z_at = jnp.minimum(z + step, z_count - 1)
            up_sends.append(send_weight(kind, z_at, y, z + step < z_count))
    late_send = send_weight(1, next_z, y, has_up)

    scales = (DK_MAJOR ** (-0.5) * LOG2_E, DK_MINOR ** (-0.5) * LOG2_E)
    lane = lax.broadcasted_iota(jnp.int32, (rows, width), 1)

    def pick(group, side, block):
        first, size = (0, DK_MAJOR) if group == 0 else (y * half, DK_MINOR)
        for m in range(MAPS):
            low = first + m * size
            keep = (lane >= low) & (lane < low + size)
            qm[group, side, m * rows : (m + 1) * rows, :] = jnp.where(keep, block.astype(f32), 0.0).astype(bf16)

    def fold(side, z_at, key_side, diagonal):
        window = span(key_side, rows)
        for group in range(2):
            keys = kv_all[z_at, 2 * group, window, :]
            stored = kv_all[z_at, 1 + group, window, :]
            values = jnp.transpose(stored.astype(f32)).astype(bf16)
            scores = lax.dot_general(
                keys, qm[group, side], (((1,), (1,)), ((), ())), preferred_element_type=f32
            ) * scales[group]
            if diagonal:
                key_pos = lax.broadcasted_iota(jnp.int32, scores.shape, 0)
                query_pos = lax.broadcasted_iota(jnp.int32, scores.shape, 1) % rows
                visible = key_pos // SEGMENT <= query_pos // SEGMENT
                scores = jnp.where(visible, scores, NEGATIVE)
            peak = jnp.max(scores, axis=0, keepdims=True)
            if not diagonal:
                peak_old = peaks[group, side]
                peak = jnp.maximum(peak, peak_old)
            weights = jnp.exp2(scores - peak)
            total = jnp.sum(weights, axis=0, keepdims=True)
            sums = jnp.dot(values, weights.astype(bf16), preferred_element_type=f32)
            if not diagonal:
                factor = jnp.exp2(peak_old - peak)
                total = total + totals[group, side] * factor
                sums = sums + acc[group, side] * factor
            peaks[group, side] = peak
            totals[group, side] = total
            acc[group, side] = sums

    pick(0, y, q_major[:, span(y, width)])
    pick(1, y, q_minor[...])

    for part in range(3):
        arrive(kv_place(z, part, oy), r_y.at[part])
        sender.send(kv_place(z, part, oy), kv_place(z, part, oy), r_near.at[oy, part], dev(z_at=next_z), has_up)
    for part in range(2):
        arrive(q_in.at[part], r_y.at[3 + part])
        pick(part, oy, q_in[part])

    def issue_up():
        for start in up_sends:
            start()

    pl.when(z == 0)(issue_up)

    def diagonal_fold(side, carry):
        fold(side, z, side, True)
        return carry

    lax.fori_loop(0, 2, diagonal_fold, 0)

    def relay_copy(z_at):
        return pltpu.make_async_remote_copy(
            src_ref=kv_all.at[z_at],
            dst_ref=kv_all.at[z_at],
            send_sem=relay_sem.at[z_at],
            recv_sem=r_far.at[z_at],
            device_id=dev(z_at=next_z),
            device_id_type=pl.DeviceIdType.MESH,
        )

    def inner(index, z_at):
        fold(lax.rem(index, 2), z_at, index // 2, False)
        return z_at

    def earlier(step, carry):
        z_at = z - step

        @pl.when(step == 1)
        def _():
            for side in range(2):
                for part in range(3):
                    arrive(kv_place(z_at, part, side), r_near.at[side, part])

        @pl.when(step > 1)
        def _():
            arrive(kv_all.at[z_at], r_far.at[z_at])

        pl.when(has_up)(lambda: relay_copy(z_at).start())
        pl.when(step == z)(issue_up)
        lax.fori_loop(0, 4, inner, z_at)
        return carry

    fold(1, z, 0, False)
    lax.fori_loop(1, z + 1, earlier, 0)

    value_row = lax.broadcasted_iota(jnp.int32, (width, rows), 0)
    value_keep = (value_row >= oy * half) & (value_row < (oy + 1) * half)
    gains = (gain_major[...], gain_minor[...])
    lams = (lam_major[y], lam_minor[y])

    def close(side, carry):
        for group in range(2):
            ratio = acc[group, side] / totals[group, side]
            diff = ratio[:, :rows] - lams[group] * ratio[:, rows:]
            if group == 1:
                diff = jnp.where(value_keep, diff, 0.0)
            count = width if group == 0 else half
            mean = jnp.sum(diff * diff, axis=0, keepdims=True) * (1.0 / count)
            done = jnp.transpose(diff * lax.rsqrt(mean + EPSILON)) * gains[group]
            heads_out[group, span(side, rows), :] = done.astype(bf16)
        return carry

    lax.fori_loop(0, 2, close, 0)

    place = tp * y_count + y

    def token_span(y_at, x_at, c_at):
        return span(y_at * (rows // tile) + x_at * 2 + c_at, tile)

    def head_place(group, index):
        return cat.at[:, span(index, width)] if group == 0 else minor_in.at[index]

    for dy, dx, dc in ((1, 1, 1), (1, 1, 0), (1, 0, 1), (1, 0, 0), (0, 1, 1), (0, 1, 0), (0, 0, 1)):
        y_at, x_at, c_at = oy if dy else y, ox if dx else x, oc if dc else c
        for group in range(2):
            sender.send(
                heads_out.at[group, token_span(y_at, x_at, c_at), :],
                head_place(group, place),
                r_h.at[group, place],
                dev(y_at=y_at, x_at=x_at, c_at=c_at),
            )
    cat[:, span(place, width)] = heads_out[0, token_span(y, x, c), :]
    minor_in[place] = heads_out[1, token_span(y, x, c), :]

    def pass_weight(kind, z_at, when):
        source = z_at * y_count + y
        run_when(when, lambda: arrive(weight_place(kind, source), r_w.at[kind, source]))
        sender.send(weight_place(kind, source), weight_place(kind, source), r_w.at[kind, source], dev(y_at=oy), when)

    for step in range(1, z_count):
        pass_weight(0, lax.rem(z + step, z_count), z + step < z_count)

    for made in local:
        made.wait()
    for dx, dc in ((0, 1), (1, 0), (1, 1)):
        index = (ox if dx else x) * 2 + (oc if dc else c)
        for part in range(2):
            arrive(wo_place(part, index), r_wo.at[part, index])
    for dy, dx, dc in ((0, 0, 1), (0, 1, 0), (0, 1, 1), (1, 0, 0), (1, 0, 1), (1, 1, 0), (1, 1, 1)):
        index = ((ox if dx else x) * 2 + (oc if dc else c)) * y_count + (oy if dy else y)
        for group in range(2):
            arrive(head_place(group, index), r_h.at[group, index])
    major_width = tp_count * y_count * width
    for index in range(tp_count):
        both = minor_in[index * y_count].astype(f32) + minor_in[index * y_count + 1].astype(f32)
        cat[:, major_width + index * width : major_width + (index + 1) * width] = pltpu.roll(both, half, 1).astype(bf16)

    model = residual.shape[1]
    step_cols = 256

    def project(index, carry):
        window = span(index, step_cols)
        mixed = jnp.dot(cat[...], wo_all[:, window], preferred_element_type=f32)
        added = residual[:, window].astype(f32) + mixed
        stream[:, window] = added
        return carry + jnp.sum(added * added, axis=1, keepdims=True)

    square = lax.fori_loop(0, model // step_cols, project, jnp.zeros((tile, 1), f32))
    norm = lax.rsqrt(square * (1.0 / model) + EPSILON)

    def slot(c_at, x_at, zl_at):
        return c_at * (2 * x_count) + x_at * 2 + zl_at

    def rows_at(index):
        return normed_all.at[span(index, tile), :]

    mine_at = slot(c, x, zl)
    normed_all[span(mine_at, tile), :] = (stream[...] * norm * mixer_gain[...]).astype(bf16)

    def share(index, target):
        sender.send(rows_at(index), rows_at(index), r_g.at[index], target)

    partner, x_peer, z_peer = dev(c_at=oc), dev(x_at=ox), dev(z_at=oz)
    share(mine_at, z_peer)
    share(mine_at, x_peer)
    share(mine_at, partner)
    late_send()
    index = slot(c, ox, zl)
    arrive(rows_at(index), r_g.at[index])
    share(index, partner)
    index = slot(c, x, 1 - zl)
    arrive(rows_at(index), r_g.at[index])
    share(index, x_peer)
    share(index, partner)
    for step in range(1, z_count):
        pass_weight(0, lax.rem(z + step, z_count), z + step >= z_count)
    index = slot(c, ox, 1 - zl)
    arrive(rows_at(index), r_g.at[index])
    share(index, partner)
    for step in range(z_count):
        source = lax.rem(z + step, z_count) * y_count + oy
        arrive(weight_place(0, source), r_w.at[0, source])

    group_rows = 2 * x_count * tile
    hid_cols = 256

    def expand(side):
        def one(index, carry):
            window = span(index, hid_cols)
            pre = jnp.dot(
                normed_all[span(side, group_rows), :], up_all[:, window], preferred_element_type=f32
            )
            hidden[span(side, group_rows), window] = jnp.square(jnp.maximum(pre, 0.0)).astype(bf16)
            return carry

        lax.fori_loop(0, hid // hid_cols, one, 0)

    expand(c)
    for x_at in range(x_count):
        for zl_at in range(2):
            index = slot(oc, x_at, zl_at)
            arrive(rows_at(index), r_g.at[index])
    expand(oc)

    x_rows = 2 * tile
    blocks = []

    def stage_x(t):
        arrive(d_in.at[t], r_d.at[t])
        x_send[t] = (mine[t, span(ox, x_rows), :] + d_in[t, span(ox, x_rows), :].astype(f32)).astype(bf16)
        sender.send(x_send.at[t], x_in.at[t], r_x.at[t], x_peer)
        x_keep[t] = mine[t, span(x, x_rows), :] + d_in[t, span(x, x_rows), :].astype(f32)

    def stage_z(t):
        arrive(x_in.at[t], r_x.at[t])
        other, same = span(1 - zl, tile), span(zl, tile)
        z_send[t] = (x_keep[t, other, :] + x_in[t, other, :].astype(f32)).astype(bf16)
        sender.send(z_send.at[t], z_in.at[blocks[t]], r_z.at[blocks[t]], z_peer)
        z_keep[t] = x_keep[t, same, :] + x_in[t, same, :].astype(f32)

    def stage_end(t):
        arrive(z_in.at[blocks[t]], r_z.at[blocks[t]])
        window = span(blocks[t], cols)
        total = stream[:, window] + (z_keep[t] + z_in[blocks[t]].astype(f32))
        out_ref[:, window] = total.astype(out_ref.dtype)

    def advance(t):
        for stage, lag in ((stage_x, 1), (stage_z, 2), (stage_end, 3)):
            if 0 <= t - lag < z_count * y_count:
                stage(t - lag)

    for t in range(z_count * y_count):
        z_at = lax.rem(z - zl + 1 + t // 2, z_count)
        source = z_at * y_count + (oy if t % 2 else y)
        blocks.append(source)
        if t % 2:
            arrive(down_all.at[source], r_w.at[1, source])
        else:
            pass_weight(1, z_at, z_at != z)
        d_send[t] = jnp.dot(
            hidden[span(oc, group_rows), :], down_all[source], preferred_element_type=f32
        ).astype(bf16)
        sender.send(d_send.at[t], d_in.at[t], r_d.at[t], partner)
        mine[t] = jnp.dot(hidden[span(c, group_rows), :], down_all[source], preferred_element_type=f32)
        advance(t)
    for t in range(z_count * y_count, z_count * y_count + 3):
        advance(t)

    sender.finish()
    for step in range(1, z_count):
        source = jnp.maximum(z - step, 0)
        run_when((z >= step) & has_up, relay_copy(source).wait_send)


def fused(sp_count, tp_count, args):
    residual, q_major, _, v_major, q_minor = args[:5]
    wo_major, wo_minor, _, up_weight, down_weight = args[11:16]
    z_count, y_count = grid_sizes(sp_count)
    x_count = tp_count // 2
    rows, tile, width = q_major.shape[0], residual.shape[0], q_minor.shape[1]
    model, hid = residual.shape[1], up_weight.shape[1] // 2
    cols = down_weight.shape[1]
    features = tp_count * (wo_major.shape[0] + wo_minor.shape[0])
    group_rows = 2 * x_count * tile
    steps = sp_count
    bf16, f32 = jnp.bfloat16, jnp.float32
    dma = pltpu.SemaphoreType.DMA
    sends = 128
    hbm = pl.BlockSpec(memory_space=pltpu.HBM)
    return pl.pallas_call(
        functools.partial(layer_kernel, (z_count, y_count, x_count)),
        out_shape=jax.ShapeDtypeStruct(residual.shape, residual.dtype),
        in_specs=[VMEM] * 7 + [SMEM] * 2 + [VMEM] * 2 + [hbm] * 2 + [VMEM] + [hbm] * 2,
        out_specs=VMEM,
        scratch_shapes=[
            pltpu.VMEM((2, rows, width), bf16),
            pltpu.VMEM((z_count, 3, y_count * rows, width), bf16),
            pltpu.VMEM((2, rows, width), bf16),
            pltpu.VMEM((2, 2, MAPS * rows, width), bf16),
            pltpu.VMEM((2, 2, width, MAPS * rows), f32),
            pltpu.VMEM((2, 2, 1, MAPS * rows), f32),
            pltpu.VMEM((2, 2, 1, MAPS * rows), f32),
            pltpu.VMEM((2, y_count * rows, width), bf16),
            pltpu.VMEM((tile, features), bf16),
            pltpu.VMEM((tp_count * y_count, tile, width), bf16),
            pltpu.VMEM((features, model), bf16),
            pltpu.VMEM((tile, model), f32),
            pltpu.VMEM((2 * group_rows, model), bf16),
            pltpu.VMEM((model, hid), bf16),
            pltpu.VMEM((sp_count, hid, cols), bf16),
            pltpu.VMEM((2 * group_rows, hid), bf16),
            pltpu.VMEM((steps, group_rows, cols), bf16),
            pltpu.VMEM((steps, group_rows, cols), bf16),
            pltpu.VMEM((steps, group_rows, cols), f32),
            pltpu.VMEM((steps, 2 * tile, cols), bf16),
            pltpu.VMEM((steps, 2 * tile, cols), bf16),
            pltpu.VMEM((steps, 2 * tile, cols), f32),
            pltpu.VMEM((steps, tile, cols), bf16),
            pltpu.VMEM((steps, tile, cols), bf16),
            pltpu.VMEM((steps, tile, cols), f32),
            dma((sends,)),
            dma((z_count,)),
            dma((4,)),
            dma((5,)),
            dma((2, 3)),
            dma((z_count,)),
            dma((2, sp_count)),
            dma((2, tp_count)),
            dma((2, tp_count * y_count)),
            dma((2 * group_rows // tile,)),
            dma((steps,)),
            dma((steps,)),
            dma((steps,)),
        ],
        compiler_params=pltpu.CompilerParams(
            collective_id=0, has_side_effects=True, vmem_limit_bytes=63 * 1024 * 1024
        ),
    )(*args)


def fits_fused(sp_count, tp_count, args):
    q_major, k_major, v_major, q_minor, k_minor, v_minor = args[1:7]
    z_count, y_count = grid_sizes(sp_count)
    width = q_minor.shape[1]
    return (
        y_count == 2
        and tp_count == 4
        and z_count % 2 == 0
        and width == 2 * MAPS * DK_MINOR
        and width == MAPS * DK_MAJOR
        and width % 128 == 0
        and v_minor.shape[1] == width
        and q_major.shape[1] == v_major.shape[1] == 2 * width
    )


def body(
    residual,
    query_major,
    keys_major,
    values_major,
    query_minor,
    keys_minor,
    values_minor,
    lambda_major,
    lambda_minor,
    gain_major,
    gain_minor,
    output_major,
    output_minor,
    mixer_gain,
    up_weight,
    down_weight,
):
    sp_count, tp_count = lax.axis_size("sp"), lax.axis_size("tp")
    args = (
        residual,
        query_major,
        keys_major,
        values_major,
        query_minor,
        keys_minor,
        values_minor,
        lambda_major,
        lambda_minor,
        gain_major[None, :],
        jnp.tile(gain_minor, 2)[None, :],
        output_major,
        output_minor,
        mixer_gain[None, :],
        up_weight,
        down_weight,
    )
    if fits_fused(sp_count, tp_count, args):
        return fused(sp_count, tp_count, args)
    out_major, out_minor, up_full, down_full = mixer(
        lax.axis_size("sp"),
        query_major,
        keys_major,
        values_major,
        query_minor,
        jnp.concatenate([keys_minor, values_minor], axis=1),
        lambda_major,
        lambda_minor,
        gain_major[:, None],
        gain_minor[:, None],
        up_weight,
        down_weight,
    )
    partial_sum = jnp.dot(out_major, output_major, preferred_element_type=jnp.float32)
    partial_sum = partial_sum + jnp.dot(out_minor, output_minor, preferred_element_type=jnp.float32)
    rows = residual.shape[0]
    stream, normed_all = tp_call(
        mix_kernel,
        1,
        (partial_sum.astype(jnp.bfloat16), residual, mixer_gain[None, :]),
        (
            jax.ShapeDtypeStruct(residual.shape, jnp.float32),
            jax.ShapeDtypeStruct(partial_sum.shape, jnp.bfloat16),
        ),
        rows,
        True,
    )
    pre_act = jnp.dot(
        normed_all,
        up_full,
        preferred_element_type=jnp.float32,
    )
    hidden = jnp.square(jax.nn.relu(pre_act)).astype(jnp.bfloat16)
    down_part = jnp.einsum("th,shd->tsd", hidden, down_full, preferred_element_type=jnp.float32)
    down_part = down_part.astype(jnp.bfloat16).reshape(partial_sum.shape)
    return tp_call(
        sum_kernel,
        2,
        (down_part, stream),
        jax.ShapeDtypeStruct(residual.shape, residual.dtype),
        rows,
        False,
    )


def solution(mesh):
    return jax.shard_map(
        body,
        mesh=mesh,
        in_specs=(
            P(("sp", "tp"), None),
            P("sp", "tp"),
            P("sp", "tp"),
            P("sp", "tp"),
            P("sp", "tp"),
            P("sp", "tp"),
            P("sp", "tp"),
            P("tp"),
            P("tp"),
            P(),
            P(),
            P("tp", None),
            P("tp", None),
            P(),
            P("sp", "tp"),
            P("tp", "sp"),
        ),
        out_specs=P(("sp", "tp"), None),
        check_vma=False,
    )
```

```python
import functools

import jax
import jax.numpy as jnp
from jax import lax
from jax.experimental import pallas as pl
from jax.experimental.pallas import tpu as pltpu
from jax.sharding import PartitionSpec as P

DK_MAJOR = 64
DK_MINOR = 32
SEGMENT = 64
MAPS = 2
DOWN_PARTS = 2

EPSILON = 1e-06
NEGATIVE = -1e30
LOG2_E = 1.4426950408889634
ANY = pl.BlockSpec(memory_space=pl.ANY)
VMEM = pl.BlockSpec(memory_space=pltpu.VMEM)
SMEM = pl.BlockSpec(memory_space=pltpu.SMEM)


def grid_sizes(sp_count):
    y_count = 1 << ((sp_count.bit_length() - 1) // 2)
    return sp_count // y_count, y_count


class Gather:
    def __init__(self, sp_count, places, send_sem, recv_sem):
        self.z_count, self.y_count = grid_sizes(sp_count)
        own = lax.axis_index("sp")
        self.own, self.z, self.y = own, own // self.y_count, lax.rem(own, self.y_count)
        self.places, self.send_sem, self.recv_sem = places, send_sem, recv_sem
        self.copies = []

    def z_peer(self, step):
        return lax.rem(self.z + step, self.z_count) * self.y_count + self.y

    def y_peer(self, step):
        return self.z * self.y_count + lax.rem(self.y + step, self.y_count)

    def send(self, array, source, src_ref, target):
        copy = pltpu.make_async_remote_copy(
            src_ref=src_ref,
            dst_ref=self.places[array](source),
            send_sem=self.send_sem.at[array, len([c for c in self.copies if c[0] == array])],
            recv_sem=self.recv_sem.at[array, source],
            device_id={"sp": target},
            device_id_type=pl.DeviceIdType.MESH,
        )
        copy.start()
        self.copies.append((array, copy))

    def wait_block(self, array, source):
        place = self.places[array](source)
        pltpu.make_async_remote_copy(
            src_ref=place,
            dst_ref=place,
            send_sem=self.send_sem.at[array, 0],
            recv_sem=self.recv_sem.at[array, source],
            device_id={"sp": self.y_peer(1)},
            device_id_type=pl.DeviceIdType.MESH,
        ).wait_recv()

    def send_z(self, array, src_ref):
        for step in range(1, self.z_count):
            self.send(array, self.own, src_ref, self.z_peer(step))

    def send_y(self, array, src_ref):
        for step in range(1, self.y_count):
            self.send(array, self.own, src_ref, self.y_peer(step))

    def pass_on(self, array, step):
        source = self.z_peer(self.z_count - step)
        self.wait_block(array, source)
        for y_step in range(1, self.y_count):
            self.send(array, source, self.places[array](source), self.y_peer(y_step))

    def wait_y(self, array):
        for y_step in range(1, self.y_count):
            for z_step in range(self.z_count):
                z_at = lax.rem(self.z + z_step, self.z_count)
                self.wait_block(array, z_at * self.y_count + lax.rem(self.y + y_step, self.y_count))

    def finish(self):
        for _, copy in self.copies:
            copy.wait_send()


def mixer_kernel(
    sp_count,
    groups,
    q_major,
    k_major,
    v_major,
    q_minor,
    kv_minor,
    lam_major,
    lam_minor,
    gain_major,
    gain_minor,
    up_ref,
    down_ref,
    out_major,
    out_minor,
    up_all,
    down_all,
    k_major_all,
    v_major_all,
    kv_minor_all,
    qm_major,
    qm_minor,
    acc_major,
    acc_minor,
    peaks,
    totals,
    send_sem,
    recv_sem,
    local_sem,
):
    rows = q_major.shape[0]
    up_rows = up_ref.shape[0]

    def rows_of(ref, count):
        return lambda source: ref.at[pl.ds(pl.multiple_of(source * count, count), count), :]

    places = [
        rows_of(k_major_all, rows),
        rows_of(v_major_all, rows),
        rows_of(kv_minor_all, rows),
        rows_of(up_all, up_rows),
        lambda source: down_all.at[source],
    ]
    own_refs = [k_major, v_major, kv_minor, up_ref, down_ref]
    gather = Gather(sp_count, places, send_sem, recv_sem)
    own = gather.own

    barrier = pltpu.get_barrier_semaphore()
    peers = [gather.z_peer(step) for step in range(1, gather.z_count)]
    peers += [gather.y_peer(step) for step in range(1, gather.y_count)]
    for peer in peers:
        pl.semaphore_signal(
            barrier, inc=1, device_id={"sp": peer}, device_id_type=pl.DeviceIdType.MESH
        )
    pl.semaphore_wait(barrier, len(peers))

    for array in range(3):
        gather.send_z(array, own_refs[array])
    for array in range(3):
        gather.send_y(array, own_refs[array])
    for array in (3, 4):
        gather.send_z(array, own_refs[array])
    for array in (3, 4):
        gather.send_y(array, own_refs[array])
    local = []
    for slot, array in enumerate((3, 4)):
        copy = pltpu.make_async_copy(own_refs[array], places[array](own), local_sem.at[slot])
        copy.start()
        local.append(copy)

    heads = []
    for group, (head_count, key_size) in enumerate(groups):
        q_ref, qm_ref = ((q_major, qm_major), (q_minor, qm_minor))[group]
        acc_ref = (acc_major, acc_minor)[group]
        value_size = acc_ref.shape[1]
        lanes = qm_ref.shape[2]
        for head in range(head_count):
            first = head * MAPS * key_size
            lane_first = first // lanes * lanes
            block = q_ref[:, lane_first : lane_first + lanes]
            lane = lax.broadcasted_iota(jnp.int32, block.shape, 1) + lane_first
            for m in range(MAPS):
                low = first + m * key_size
                keep = (lane >= low) & (lane < low + key_size)
                picked = jnp.where(keep, block.astype(jnp.float32), 0.0).astype(block.dtype)
                qm_ref[head, m * rows : (m + 1) * rows, :] = picked
            heads.append((group, head, len(heads), lane_first, lanes, value_size, key_size))

    minor_keys = q_minor.shape[1]
    minor_first = minor_keys // 128 * 128

    def fold(key_refs, value_refs, at, diagonal):
        window = pl.ds(at, rows)
        stored = (value_refs[0][window, :], value_refs[1][window, minor_first:])
        turned = [jnp.transpose(v.astype(jnp.float32)).astype(jnp.bfloat16) for v in stored]
        turned[1] = turned[1][minor_keys - minor_first :, :]
        for group, head, index, lane_first, lanes, value_size, key_size in heads:
            qm_ref = (qm_major, qm_minor)[group]
            acc_ref = (acc_major, acc_minor)[group]
            keys = key_refs[group][window, lane_first : lane_first + lanes]
            values = turned[group][head * value_size : (head + 1) * value_size, :]
            scores = lax.dot_general(
                keys, qm_ref[head], (((1,), (1,)), ((), ())), preferred_element_type=jnp.float32
            ) * (key_size ** (-0.5) * LOG2_E)
            if diagonal:
                key_pos = lax.broadcasted_iota(jnp.int32, scores.shape, 0)
                query_pos = lax.broadcasted_iota(jnp.int32, scores.shape, 1) % rows
                visible = key_pos // SEGMENT <= query_pos // SEGMENT
                scores = jnp.where(visible, scores, NEGATIVE)
            peak = jnp.max(scores, axis=0, keepdims=True)
            if not diagonal:
                peak_old = peaks[index]
                peak = jnp.maximum(peak, peak_old)
            weights = jnp.exp2(scores - peak)
            total = jnp.sum(weights, axis=0, keepdims=True)
            sums = jnp.dot(
                values, weights.astype(jnp.bfloat16), preferred_element_type=jnp.float32
            )
            if not diagonal:
                factor = jnp.exp2(peak_old - peak)
                total = total + totals[index] * factor
                sums = sums + acc_ref[head] * factor
            peaks[index] = peak
            totals[index] = total
            acc_ref[head] = sums

    fold((k_major, kv_minor), (v_major, kv_minor), 0, True)

    for step in range(1, gather.z_count):
        for array in range(3):
            gather.pass_on(array, step)

    def earlier(block, carry):
        at = pl.multiple_of(block * rows, rows)
        fold((k_major_all, kv_minor_all), (v_major_all, kv_minor_all), at, False)
        return carry

    y_count = gather.y_count

    def same_y(z_at, carry):
        return earlier(z_at * y_count + gather.y, carry)

    def other_y(index, carry):
        z_at, place = index // (y_count - 1), lax.rem(index, y_count - 1)
        y_at = place + (place >= gather.y).astype(jnp.int32)
        return earlier(z_at * y_count + y_at, carry)

    lax.fori_loop(0, gather.z, same_y, 0)
    for array in range(3):
        gather.wait_y(array)
    lax.fori_loop(0, gather.z * (y_count - 1) + gather.y, other_y, 0)

    for group, (head_count, _) in enumerate(groups):
        acc_ref = (acc_major, acc_minor)[group]
        lam_ref = (lam_major, lam_minor)[group]
        gain_ref = (gain_major, gain_minor)[group]
        out_ref = (out_major, out_minor)[group]
        done = []
        for head in range(head_count):
            index = next(h[2] for h in heads if h[0] == group and h[1] == head)
            ratio = acc_ref[head] / totals[index]
            diff = ratio[:, :rows] - lam_ref[head] * ratio[:, rows:]
            mean = jnp.mean(diff * diff, axis=0, keepdims=True)
            done.append(diff * lax.rsqrt(mean + EPSILON) * gain_ref[...])
        out_ref[...] = jnp.transpose(jnp.concatenate(done, axis=0)).astype(out_ref.dtype)

    for step in range(1, gather.z_count):
        for array in (3, 4):
            gather.pass_on(array, step)
    for array in (3, 4):
        gather.wait_y(array)
    for copy in local:
        copy.wait()
    gather.finish()


def mixer(sp_count, *args):
    q_major, k_major, v_major, q_minor, kv_minor = args[:5]
    up_weight, down_weight = args[9:11]
    heads_major = k_major.shape[1] // (MAPS * DK_MAJOR)
    heads_minor = q_minor.shape[1] // (MAPS * DK_MINOR)
    rows = q_major.shape[0]
    size_major = v_major.shape[1] // heads_major
    width_minor = kv_minor.shape[1] - q_minor.shape[1]
    size_minor = width_minor // heads_minor
    lanes_major = min(MAPS * DK_MAJOR, q_major.shape[1])
    lanes_minor = min(128, q_minor.shape[1])
    z_count, y_count = grid_sizes(sp_count)
    sends = (z_count - 1) + (y_count - 1) * z_count
    tokens = rows * sp_count
    bf16, f32 = jnp.bfloat16, jnp.float32
    head_total = heads_major + heads_minor
    return pl.pallas_call(
        functools.partial(
            mixer_kernel, sp_count, ((heads_major, DK_MAJOR), (heads_minor, DK_MINOR))
        ),
        out_shape=(
            jax.ShapeDtypeStruct(v_major.shape, bf16),
            jax.ShapeDtypeStruct((rows, width_minor), bf16),
            jax.ShapeDtypeStruct((up_weight.shape[0] * sp_count, up_weight.shape[1]), bf16),
            jax.ShapeDtypeStruct((sp_count, *down_weight.shape), bf16),
        ),
        in_specs=[VMEM] * 5 + [SMEM] * 2 + [VMEM] * 4,
        out_specs=(VMEM, VMEM, ANY, ANY),
        scratch_shapes=[
            pltpu.VMEM((tokens, k_major.shape[1]), bf16),
            pltpu.VMEM((tokens, v_major.shape[1]), bf16),
            pltpu.VMEM((tokens, kv_minor.shape[1]), bf16),
            pltpu.VMEM((heads_major, MAPS * rows, lanes_major), bf16),
            pltpu.VMEM((heads_minor, MAPS * rows, lanes_minor), bf16),
            pltpu.VMEM((heads_major, size_major, MAPS * rows), f32),
            pltpu.VMEM((heads_minor, size_minor, MAPS * rows), f32),
            pltpu.VMEM((head_total, 1, MAPS * rows), f32),
            pltpu.VMEM((head_total, 1, MAPS * rows), f32),
            pltpu.SemaphoreType.DMA((5, sends)),
            pltpu.SemaphoreType.DMA((5, sp_count)),
            pltpu.SemaphoreType.DMA((2,)),
        ],
        compiler_params=pltpu.CompilerParams(
            collective_id=0, has_side_effects=True, vmem_limit_bytes=60 * 1024 * 1024
        ),
    )(*args)


class Exchange:
    def __init__(self, tp_count, send_sem, recv_sem):
        own = lax.axis_index("tp")
        self.x_count = tp_count // 2
        self.own, self.x, self.core = own, own // 2, lax.rem(own, 2)
        self.partner = self.x * 2 + 1 - self.core
        self.send_sem, self.recv_sem = send_sem, recv_sem

    def enter(self):
        barrier = pltpu.get_barrier_semaphore()
        peers = [self.partner] + [self.x_peer(step) for step in range(1, self.x_count)]
        for peer in peers:
            pl.semaphore_signal(
                barrier, inc=1, device_id={"tp": peer}, device_id_type=pl.DeviceIdType.MESH
            )
        pl.semaphore_wait(barrier, len(peers))

    def x_peer(self, step):
        return lax.rem(self.x + step, self.x_count) * 2 + self.core

    def copy(self, src, dst, slot, target):
        made = pltpu.make_async_remote_copy(
            src_ref=src,
            dst_ref=dst,
            send_sem=self.send_sem.at[slot],
            recv_sem=self.recv_sem.at[slot],
            device_id={"tp": target},
            device_id_type=pl.DeviceIdType.MESH,
        )
        made.start()
        return made

    def total(self, partial, pair_in, pair_sum, x_in, rows):
        def block(x_at, core):
            return pl.ds(pl.multiple_of((x_at * 2 + core) * rows, rows), rows)

        steps = list(range(1, self.x_count)) + [0]
        at = [lax.rem(self.x + step, self.x_count) for step in range(self.x_count)]
        pair = {}
        for step in steps:
            pair[step] = self.copy(
                partial.at[block(at[step], 1 - self.core), :], pair_in.at[step], step, self.partner
            )
        across = []
        for step in steps:
            pair[step].wait_recv()
            mine = partial[block(at[step], self.core), :].astype(jnp.float32)
            both = mine + pair_in[step].astype(jnp.float32)
            if step:
                pair_sum[step] = both.astype(jnp.bfloat16)
                across.append(
                    self.copy(
                        pair_sum.at[step], x_in.at[step], self.x_count + step, self.x_peer(step)
                    )
                )
        for made in across:
            made.wait_recv()
        for step in range(1, self.x_count):
            both = both + x_in[step].astype(jnp.float32)
        return both, list(pair.values()) + across


def mix_kernel(
    tp_count, partial, residual, gain, stream_ref, normed_ref, pair_in, pair_sum, x_in, held, send_sem, recv_sem
):
    exchange = Exchange(tp_count, send_sem, recv_sem)
    exchange.enter()
    rows = residual.shape[0]
    mixed, copies = exchange.total(partial, pair_in, pair_sum, x_in, rows)
    stream = residual[...].astype(jnp.float32) + mixed
    stream_ref[...] = stream
    mean = jnp.mean(stream * stream, axis=-1, keepdims=True)
    normed = (stream * lax.rsqrt(mean + EPSILON) * gain[...]).astype(jnp.bfloat16)
    held[...] = normed

    def place(index):
        return normed_ref.at[pl.ds(pl.multiple_of(index * rows, rows), rows), :]

    base, count = 2 * exchange.x_count, exchange.x_count
    sent = [exchange.copy(held, place(exchange.own), base + step, exchange.x_peer(step)) for step in range(1, count)]
    passed = [exchange.copy(held, place(exchange.own), base + count, exchange.partner)]
    normed_ref[pl.ds(pl.multiple_of(exchange.own * rows, rows), rows), :] = normed
    for step in range(1, count):
        sent[step - 1].wait_recv()
        source = exchange.x_peer(count - step)
        passed.append(
            exchange.copy(place(source), place(source), base + count + step, exchange.partner)
        )
    for made in passed:
        made.wait_recv()
    for made in copies + sent + passed:
        made.wait_send()


def sum_kernel(tp_count, partial, stream, out_ref, pair_in, pair_sum, x_in, send_sem, recv_sem):
    exchange = Exchange(tp_count, send_sem, recv_sem)
    exchange.enter()
    total, copies = exchange.total(partial, pair_in, pair_sum, x_in, stream.shape[0])
    out_ref[...] = (stream[...] + total).astype(out_ref.dtype)
    for made in copies:
        made.wait_send()


def tp_call(kernel, identity, inputs, out_shape, rows, holds):
    tp_count = lax.axis_size("tp")
    slots = (tp_count // 2, rows, inputs[0].shape[1])
    held = [pltpu.VMEM(slots[1:], jnp.bfloat16)] if holds else []
    return pl.pallas_call(
        functools.partial(kernel, tp_count),
        out_shape=out_shape,
        in_specs=[VMEM] * len(inputs),
        out_specs=jax.tree.map(lambda _: VMEM, out_shape),
        scratch_shapes=[pltpu.VMEM(slots, jnp.bfloat16)] * 3
        + held
        + [pltpu.SemaphoreType.DMA((2 * tp_count,))] * 2,
        compiler_params=pltpu.CompilerParams(
            collective_id=identity, has_side_effects=True, vmem_limit_bytes=32 * 1024 * 1024
        ),
    )(*inputs)


class Sender:
    def __init__(self, sem):
        self.sem, self.made = sem, []

    def prepare(self, src, dst, recv, target, when=None):
        copy = pltpu.make_async_remote_copy(
            src_ref=src,
            dst_ref=dst,
            send_sem=self.sem.at[len(self.made)],
            recv_sem=recv,
            device_id=target,
            device_id_type=pl.DeviceIdType.MESH,
        )
        self.made.append((when, copy))
        return lambda: run_when(when, copy.start)

    def send(self, src, dst, recv, target, when=None):
        self.prepare(src, dst, recv, target, when)()

    def finish(self):
        for when, copy in self.made:
            run_when(when, copy.wait_send)


def run_when(when, action):
    if when is None:
        action()
    else:
        pl.when(when)(lambda: action())


def layer_kernel(
    sizes,
    residual,
    q_major,
    k_major,
    v_major,
    q_minor,
    k_minor,
    v_minor,
    lam_major,
    lam_minor,
    gain_major,
    gain_minor,
    wo_major,
    wo_minor,
    mixer_gain,
    up_ref,
    down_ref,
    out_ref,
    pack,
    kv_all,
    q_in,
    qm,
    acc,
    peaks,
    totals,
    heads_out,
    cat,
    minor_in,
    wo_all,
    stream,
    normed_all,
    up_all,
    down_all,
    hidden,
    d_send,
    d_in,
    mine,
    x_send,
    x_in,
    x_keep,
    z_send,
    z_in,
    z_keep,
    send_sem,
    relay_sem,
    local_sem,
    r_y,
    r_kv,
    r_w,
    r_wo,
    r_h,
    r_g,
    r_d,
    r_x,
    r_z,
    credits,
):
    z_count, y_count, x_count = sizes
    bf16, f32 = jnp.bfloat16, jnp.float32
    own, tp = lax.axis_index("sp"), lax.axis_index("tp")
    z, y = own // y_count, lax.rem(own, y_count)
    x, c = tp // 2, lax.rem(tp, 2)
    oy, ox, oc = 1 - y, 1 - x, 1 - c
    zl = lax.rem(z, 2)
    oz = z + 1 - 2 * zl
    rows, tile = q_major.shape[0], residual.shape[0]
    width = q_minor.shape[1]
    half = width // 2
    hid = up_ref.shape[1] // 2
    up_rows = up_ref.shape[0]
    cols = down_ref.shape[1]

    def dev(z_at=z, y_at=y, x_at=x, c_at=c):
        return {"sp": z_at * y_count + y_at, "tp": x_at * 2 + c_at}

    def span(start, count):
        return pl.ds(pl.multiple_of(start * count, count), count)

    def arrive(place, recv):
        pltpu.make_async_remote_copy(
            src_ref=place,
            dst_ref=place,
            send_sem=send_sem.at[0],
            recv_sem=recv,
            device_id=dev(y_at=oy),
            device_id_type=pl.DeviceIdType.MESH,
        ).wait_recv()

    k_low = lax.broadcasted_iota(jnp.int32, (rows, width), 1)
    for head in range(2):
        k_part = (k_low >= head * half) & (k_low < (head + 1) * half)
        turned_v = pltpu.roll(v_minor[...].astype(f32), half, 1)
        pack[head] = jnp.where(k_part, k_minor[...].astype(f32), turned_v).astype(bf16)

    barrier = pltpu.get_barrier_semaphore()
    peers = []
    for dy in range(2):
        for dx in range(2):
            for dc in range(2):
                if dy or dx or dc:
                    peers.append(dev(y_at=oy if dy else y, x_at=ox if dx else x, c_at=oc if dc else c))
    peers += [dev(z_at=lax.rem(z + step, z_count)) for step in range(1, z_count)]
    for peer in peers:
        pl.semaphore_signal(barrier, inc=1, device_id=peer, device_id_type=pl.DeviceIdType.MESH)

    kv_all[z, 0, span(y, rows), :] = k_major[:, span(y, width)]
    kv_all[z, 1, span(y, rows), :] = v_major[:, span(y, width)]
    kv_all[z, 2, span(y, rows), :] = pack[y]
    local = []
    local_pairs = [
        (up_ref.at[:, span(zl, hid)], up_all.at[span(own, up_rows), :]),
        (down_ref.at[span(zl, hid), :], down_all.at[own]),
    ]
    major_rows, minor_rows = wo_major.shape[0], wo_minor.shape[0]
    tp_count = 2 * x_count
    minor_base = tp_count * major_rows

    def wo_place(part, index):
        if part == 0:
            return wo_all.at[span(index, major_rows), :]
        return wo_all.at[pl.ds(pl.multiple_of(minor_base + index * minor_rows, minor_rows), minor_rows), :]

    for part, ref in enumerate((wo_major, wo_minor)):
        local_pairs.append((ref, wo_place(part, tp)))
    for slot, (src, dst) in enumerate(local_pairs):
        made = pltpu.make_async_copy(src, dst, local_sem.at[slot])
        made.start()
        local.append(made)

    pl.semaphore_wait(barrier, len(peers))

    sender = Sender(send_sem)
    has_up = z < z_count - 1
    next_z = jnp.minimum(z + 1, z_count - 1)

    def kv_place(z_at, part, side):
        return kv_all.at[z_at, part, span(side, rows), :]

    for part, src in enumerate((k_major.at[:, span(oy, width)], v_major.at[:, span(oy, width)], pack.at[oy])):
        sender.send(src, kv_place(z, part, y), r_y.at[part], dev(y_at=oy))
    sender.send(q_major.at[:, span(oy, width)], q_in.at[0], r_y.at[3], dev(y_at=oy))
    sender.send(q_minor, q_in.at[1], r_y.at[4], dev(y_at=oy))
    for part, src in enumerate((k_major.at[:, span(y, width)], v_major.at[:, span(y, width)], pack.at[y])):
        sender.send(src, kv_place(z, part, y), r_kv.at[z, y, part], dev(z_at=next_z), has_up)

    part_rows = hid // DOWN_PARTS

    def weight_src(kind, z_at):
        parity = lax.rem(z_at, 2)
        if kind == 0:
            return up_ref.at[:, span(parity, hid)]
        return down_ref.at[span(parity * DOWN_PARTS + kind - 1, part_rows), :]

    def weight_place(kind, source):
        if kind == 0:
            return up_all.at[span(source, up_rows), :]
        return down_all.at[source, (kind - 1) * part_rows : kind * part_rows, :]

    def send_weight(kind, z_at, y_at, when=None):
        return sender.prepare(
            weight_src(kind, z_at), weight_place(kind, own), r_w.at[kind, own], dev(z_at=z_at, y_at=y_at), when
        )

    down_kinds = tuple(range(1, 1 + DOWN_PARTS))

    def below(kinds):
        return [
            send_weight(kind, jnp.maximum(z - step, 0), y, z >= step)
            for kind in kinds
            for step in range(z_count - 1, 0, -1)
        ]

    def above(kinds, step, odd=None):
        when = z + step < z_count
        if odd is not None:
            when = when & (lax.rem(z + step, 2) == odd)
        return [send_weight(kind, jnp.minimum(z + step, z_count - 1), y, when) for kind in kinds]

    def issue(starts):
        for start in starts:
            start()

    issue(below((0,)))
    for kind in (0, *down_kinds):
        send_weight(kind, z, oy)()
    for part, ref in enumerate((wo_major, wo_minor)):
        sender.send(ref, wo_place(part, tp), r_wo.at[part, tp], dev(x_at=ox))
        sender.send(ref, wo_place(part, tp), r_wo.at[part, tp], dev(c_at=oc))
    below_down = below(down_kinds)
    near_up = above((0,), 1)

    scales = (DK_MAJOR ** (-0.5) * LOG2_E, DK_MINOR ** (-0.5) * LOG2_E)
    lane = lax.broadcasted_iota(jnp.int32, (rows, width), 1)

    def pick(group, side, block):
        first, size = (0, DK_MAJOR) if group == 0 else (y * half, DK_MINOR)
        for m in range(MAPS):
            low = first + m * size
            keep = (lane >= low) & (lane < low + size)
            qm[group, side, m * rows : (m + 1) * rows, :] = jnp.where(keep, block.astype(f32), 0.0).astype(bf16)

    def fold(side, z_at, key_side, diagonal):
        window = span(key_side, rows)
        for group in range(2):
            keys = kv_all[z_at, 2 * group, window, :]
            stored = kv_all[z_at, 1 + group, window, :]
            values = jnp.transpose(stored.astype(f32)).astype(bf16)
            scores = lax.dot_general(
                keys, qm[group, side], (((1,), (1,)), ((), ())), preferred_element_type=f32
            ) * scales[group]
            if diagonal:
                key_pos = lax.broadcasted_iota(jnp.int32, scores.shape, 0)
                query_pos = lax.broadcasted_iota(jnp.int32, scores.shape, 1) % rows
                visible = key_pos // SEGMENT <= query_pos // SEGMENT
                scores = jnp.where(visible, scores, NEGATIVE)
            peak = jnp.max(scores, axis=0, keepdims=True)
            if not diagonal:
                peak_old = peaks[group, side]
                peak = jnp.maximum(peak, peak_old)
            weights = jnp.exp2(scores - peak)
            total = jnp.sum(weights, axis=0, keepdims=True)
            sums = jnp.dot(values, weights.astype(bf16), preferred_element_type=f32)
            if not diagonal:
                factor = jnp.exp2(peak_old - peak)
                total = total + totals[group, side] * factor
                sums = sums + acc[group, side] * factor
            peaks[group, side] = peak
            totals[group, side] = total
            acc[group, side] = sums

    pick(0, y, q_major[:, span(y, width)])
    pick(1, y, q_minor[...])
    fold(y, z, y, True)

    for part in range(3):
        arrive(kv_place(z, part, oy), r_y.at[part])
        sender.send(kv_place(z, part, oy), kv_place(z, part, oy), r_kv.at[z, oy, part], dev(z_at=next_z), has_up)

    def credit(kind, back):
        pl.semaphore_signal(
            credits.at[kind, z],
            inc=1,
            device_id=dev(z_at=jnp.maximum(z - back, 0)),
            device_id_type=pl.DeviceIdType.MESH,
        )

    def await_credit(kind, step):
        pl.semaphore_wait(credits.at[kind, jnp.minimum(z + step, z_count - 1)], 1)

    def relay_copy(z_at, side, part):
        return pltpu.make_async_remote_copy(
            src_ref=kv_place(z_at, part, side),
            dst_ref=kv_place(z_at, part, side),
            send_sem=relay_sem.at[z_at, side, part],
            recv_sem=r_kv.at[z_at, side, part],
            device_id=dev(z_at=next_z),
            device_id_type=pl.DeviceIdType.MESH,
        )

    def take(z_at, side):
        for part in range(3):
            arrive(kv_place(z_at, part, side), r_kv.at[z_at, side, part])
            run_when(has_up, relay_copy(z_at, side, part).start)

    def after_last():
        issue(near_up)
        for back in range(2, z_count):
            run_when(z >= back, lambda: credit(0, back))
        issue(below_down)

    for part in range(2):
        arrive(q_in.at[part], r_y.at[3 + part])
        pick(part, oy, q_in[part])

    pl.when(z == 0)(lambda: issue(near_up))

    @pl.when(z > 0)
    def _():
        for side in range(2):
            take(z - 1, side)

    pl.when(z == 1)(after_last)
    fold(oy, z, oy, True)
    fold(1, z, 0, False)

    def earlier(index, carry):
        z_at, key_side = z - 1 - index // 2, lax.rem(index, 2)
        pl.when(index > 1)(lambda: take(z_at, key_side))
        pl.when((index == 2 * z - 1) & (z > 1))(after_last)

        def inner(side, carry):
            fold(side, z_at, key_side, False)
            return carry

        lax.fori_loop(0, 2, inner, 0)
        return carry

    lax.fori_loop(0, 2 * z, earlier, 0)

    value_row = lax.broadcasted_iota(jnp.int32, (width, rows), 0)
    value_keep = (value_row >= oy * half) & (value_row < (oy + 1) * half)
    gains = (gain_major[...], gain_minor[...])
    lams = (lam_major[y], lam_minor[y])

    def close(side, carry):
        for group in range(2):
            ratio = acc[group, side] / totals[group, side]
            diff = ratio[:, :rows] - lams[group] * ratio[:, rows:]
            if group == 1:
                diff = jnp.where(value_keep, diff, 0.0)
            count = width if group == 0 else half
            mean = jnp.sum(diff * diff, axis=0, keepdims=True) * (1.0 / count)
            done = jnp.transpose(diff * lax.rsqrt(mean + EPSILON)) * gains[group]
            heads_out[group, span(side, rows), :] = done.astype(bf16)
        return carry

    lax.fori_loop(0, 2, close, 0)

    place = tp * y_count + y

    def token_span(y_at, x_at, c_at):
        return span(y_at * (rows // tile) + x_at * 2 + c_at, tile)

    def head_place(group, index):
        return cat.at[:, span(index, width)] if group == 0 else minor_in.at[index]

    for dy, dx, dc in ((1, 1, 1), (1, 1, 0), (1, 0, 1), (1, 0, 0), (0, 1, 1), (0, 1, 0), (0, 0, 1)):
        y_at, x_at, c_at = oy if dy else y, ox if dx else x, oc if dc else c
        for group in range(2):
            sender.send(
                heads_out.at[group, token_span(y_at, x_at, c_at), :],
                head_place(group, place),
                r_h.at[group, place],
                dev(y_at=y_at, x_at=x_at, c_at=c_at),
            )
    cat[:, span(place, width)] = heads_out[0, token_span(y, x, c), :]
    minor_in[place] = heads_out[1, token_span(y, x, c), :]

    def pass_weight(kind, z_at, when):
        source = z_at * y_count + y
        run_when(when, lambda: arrive(weight_place(kind, source), r_w.at[kind, source]))
        sender.send(weight_place(kind, source), weight_place(kind, source), r_w.at[kind, source], dev(y_at=oy), when)

    for step in range(1, z_count):
        pass_weight(0, lax.rem(z + step, z_count), z + step < z_count)
    for step in range(2, z_count):
        run_when(z + step < z_count, lambda: await_credit(0, step))
        issue(above((0,), step))
    for step in range(2, z_count):
        issue(above(down_kinds, step, 0))

    for made in local:
        made.wait()
    for part in range(2):
        index = ox * 2 + c
        arrive(wo_place(part, index), r_wo.at[part, index])
        sender.send(wo_place(part, index), wo_place(part, index), r_wo.at[part, index], dev(c_at=oc))
    for index in (x * 2 + oc, ox * 2 + oc):
        for part in range(2):
            arrive(wo_place(part, index), r_wo.at[part, index])
    for dy, dx, dc in ((0, 0, 1), (0, 1, 0), (0, 1, 1), (1, 0, 0), (1, 0, 1), (1, 1, 0), (1, 1, 1)):
        index = ((ox if dx else x) * 2 + (oc if dc else c)) * y_count + (oy if dy else y)
        for group in range(2):
            arrive(head_place(group, index), r_h.at[group, index])
    major_width = tp_count * y_count * width
    for index in range(tp_count):
        both = minor_in[index * y_count].astype(f32) + minor_in[index * y_count + 1].astype(f32)
        cat[:, major_width + index * width : major_width + (index + 1) * width] = pltpu.roll(both, half, 1).astype(bf16)

    model = residual.shape[1]
    step_cols = 256

    def project(index, carry):
        window = span(index, step_cols)
        mixed = jnp.dot(cat[...], wo_all[:, window], preferred_element_type=f32)
        added = residual[:, window].astype(f32) + mixed
        stream[:, window] = added
        return carry + jnp.sum(added * added, axis=1, keepdims=True)

    square = lax.fori_loop(0, model // step_cols, project, jnp.zeros((tile, 1), f32))
    norm = lax.rsqrt(square * (1.0 / model) + EPSILON)

    def slot(c_at, x_at, zl_at):
        return c_at * (2 * x_count) + x_at * 2 + zl_at

    def rows_at(index):
        return normed_all.at[span(index, tile), :]

    mine_at = slot(c, x, zl)
    normed_all[span(mine_at, tile), :] = (stream[...] * norm * mixer_gain[...]).astype(bf16)

    def share(index, target):
        sender.send(rows_at(index), rows_at(index), r_g.at[index], target)

    partner, x_peer, z_peer = dev(c_at=oc), dev(x_at=ox), dev(z_at=oz)
    share(mine_at, z_peer)
    share(mine_at, x_peer)
    share(mine_at, partner)
    issue(above(down_kinds, 1))
    for step in range(1, z_count):
        pass_weight(0, lax.rem(z + step, z_count), z + step >= z_count)
    index = slot(c, ox, zl)
    arrive(rows_at(index), r_g.at[index])
    share(index, partner)
    index = slot(c, x, 1 - zl)
    arrive(rows_at(index), r_g.at[index])
    share(index, x_peer)
    share(index, partner)
    for back in range(2, z_count):
        run_when((z >= back) & (zl == 1), lambda: credit(1, back))
    index = slot(c, ox, 1 - zl)
    arrive(rows_at(index), r_g.at[index])
    share(index, partner)
    for step in range(z_count):
        source = lax.rem(z + step, z_count) * y_count + oy
        arrive(weight_place(0, source), r_w.at[0, source])

    for step in range(2, z_count):
        run_when((z + step < z_count) & (lax.rem(z + step, 2) == 1), lambda: await_credit(1, step))
        issue(above(down_kinds, step, 1))

    group_rows = 2 * x_count * tile
    hid_cols = 256

    def expand(side):
        def one(index, carry):
            window = span(index, hid_cols)
            pre = jnp.dot(
                normed_all[span(side, group_rows), :], up_all[:, window], preferred_element_type=f32
            )
            hidden[span(side, group_rows), window] = jnp.square(jnp.maximum(pre, 0.0)).astype(bf16)
            return carry

        lax.fori_loop(0, hid // hid_cols, one, 0)

    expand(c)
    for x_at in range(x_count):
        for zl_at in range(2):
            index = slot(oc, x_at, zl_at)
            arrive(rows_at(index), r_g.at[index])
    expand(oc)

    x_rows = 2 * tile
    blocks = []

    def stage_x(t):
        arrive(d_in.at[t], r_d.at[t])
        x_send[t] = (mine[t, span(ox, x_rows), :] + d_in[t, span(ox, x_rows), :].astype(f32)).astype(bf16)
        sender.send(x_send.at[t], x_in.at[t], r_x.at[t], x_peer)
        x_keep[t] = mine[t, span(x, x_rows), :] + d_in[t, span(x, x_rows), :].astype(f32)

    def stage_z(t):
        arrive(x_in.at[t], r_x.at[t])
        other, same = span(1 - zl, tile), span(zl, tile)
        z_send[t] = (x_keep[t, other, :] + x_in[t, other, :].astype(f32)).astype(bf16)
        sender.send(z_send.at[t], z_in.at[blocks[t]], r_z.at[blocks[t]], z_peer)
        z_keep[t] = x_keep[t, same, :] + x_in[t, same, :].astype(f32)

    def stage_end(t):
        arrive(z_in.at[blocks[t]], r_z.at[blocks[t]])
        window = span(blocks[t], cols)
        total = stream[:, window] + (z_keep[t] + z_in[blocks[t]].astype(f32))
        out_ref[:, window] = total.astype(out_ref.dtype)

    def advance(t):
        for stage, lag in ((stage_x, 1), (stage_z, 2), (stage_end, 3)):
            if 0 <= t - lag < z_count * y_count:
                stage(t - lag)

    def z_of(t):
        return z - zl + 1 - t // 2 if t < 4 else lax.rem(z - zl + t // 2, z_count)

    def pass_down(t):
        for kind in down_kinds:
            pass_weight(kind, z_of(t), z_of(t) != z if t < 4 else None)

    early_pass = {0: (0, 2), 1: (4,)}
    for t in range(2, z_count * y_count):
        if 2 * t + 2 < z_count * y_count:
            early_pass[t] = (2 * t + 2,)
    for t in range(z_count * y_count):
        source = z_of(t) * y_count + (oy if t % 2 else y)
        blocks.append(source)
        for ahead in early_pass.get(t, ()):
            pass_down(ahead)
        if t % 2:
            for kind in down_kinds:
                arrive(weight_place(kind, source), r_w.at[kind, source])
        d_send[t] = jnp.dot(
            hidden[span(oc, group_rows), :], down_all[source], preferred_element_type=f32
        ).astype(bf16)
        sender.send(d_send.at[t], d_in.at[t], r_d.at[t], partner)
        mine[t] = jnp.dot(hidden[span(c, group_rows), :], down_all[source], preferred_element_type=f32)
        advance(t)
    for t in range(z_count * y_count, z_count * y_count + 3):
        advance(t)

    sender.finish()
    for step in range(1, z_count):
        for side in range(2):
            for part in range(3):
                copy = relay_copy(jnp.maximum(z - step, 0), side, part)
                run_when((z >= step) & has_up, copy.wait_send)


def fused(sp_count, tp_count, args):
    residual, q_major, _, v_major, q_minor = args[:5]
    wo_major, wo_minor, _, up_weight, down_weight = args[11:16]
    z_count, y_count = grid_sizes(sp_count)
    x_count = tp_count // 2
    rows, tile, width = q_major.shape[0], residual.shape[0], q_minor.shape[1]
    model, hid = residual.shape[1], up_weight.shape[1] // 2
    cols = down_weight.shape[1]
    features = tp_count * (wo_major.shape[0] + wo_minor.shape[0])
    group_rows = 2 * x_count * tile
    steps = sp_count
    bf16, f32 = jnp.bfloat16, jnp.float32
    dma = pltpu.SemaphoreType.DMA
    sends = 160
    hbm = pl.BlockSpec(memory_space=pltpu.HBM)
    return pl.pallas_call(
        functools.partial(layer_kernel, (z_count, y_count, x_count)),
        out_shape=jax.ShapeDtypeStruct(residual.shape, residual.dtype),
        in_specs=[VMEM] * 7 + [SMEM] * 2 + [VMEM] * 2 + [hbm] * 2 + [VMEM] + [hbm] * 2,
        out_specs=VMEM,
        scratch_shapes=[
            pltpu.VMEM((2, rows, width), bf16),
            pltpu.VMEM((z_count, 3, y_count * rows, width), bf16),
            pltpu.VMEM((2, rows, width), bf16),
            pltpu.VMEM((2, 2, MAPS * rows, width), bf16),
            pltpu.VMEM((2, 2, width, MAPS * rows), f32),
            pltpu.VMEM((2, 2, 1, MAPS * rows), f32),
            pltpu.VMEM((2, 2, 1, MAPS * rows), f32),
            pltpu.VMEM((2, y_count * rows, width), bf16),
            pltpu.VMEM((tile, features), bf16),
            pltpu.VMEM((tp_count * y_count, tile, width), bf16),
            pltpu.VMEM((features, model), bf16),
            pltpu.VMEM((tile, model), f32),
            pltpu.VMEM((2 * group_rows, model), bf16),
            pltpu.VMEM((model, hid), bf16),
            pltpu.VMEM((sp_count, hid, cols), bf16),
            pltpu.VMEM((2 * group_rows, hid), bf16),
            pltpu.VMEM((steps, group_rows, cols), bf16),
            pltpu.VMEM((steps, group_rows, cols), bf16),
            pltpu.VMEM((steps, group_rows, cols), f32),
            pltpu.VMEM((steps, 2 * tile, cols), bf16),
            pltpu.VMEM((steps, 2 * tile, cols), bf16),
            pltpu.VMEM((steps, 2 * tile, cols), f32),
            pltpu.VMEM((steps, tile, cols), bf16),
            pltpu.VMEM((steps, tile, cols), bf16),
            pltpu.VMEM((steps, tile, cols), f32),
            dma((sends,)),
            dma((z_count, 2, 3)),
            dma((4,)),
            dma((5,)),
            dma((z_count, 2, 3)),
            dma((1 + DOWN_PARTS, sp_count)),
            dma((2, tp_count)),
            dma((2, tp_count * y_count)),
            dma((2 * group_rows // tile,)),
            dma((steps,)),
            dma((steps,)),
            dma((steps,)),
            pltpu.SemaphoreType.REGULAR((2, z_count)),
        ],
        compiler_params=pltpu.CompilerParams(
            collective_id=0, has_side_effects=True, vmem_limit_bytes=63 * 1024 * 1024
        ),
    )(*args)


def fits_fused(sp_count, tp_count, args):
    q_major, k_major, v_major, q_minor, k_minor, v_minor = args[1:7]
    z_count, y_count = grid_sizes(sp_count)
    width = q_minor.shape[1]
    return (
        y_count == 2
        and tp_count == 4
        and z_count % 2 == 0
        and width == 2 * MAPS * DK_MINOR
        and width == MAPS * DK_MAJOR
        and width % 128 == 0
        and v_minor.shape[1] == width
        and q_major.shape[1] == v_major.shape[1] == 2 * width
    )


def body(
    residual,
    query_major,
    keys_major,
    values_major,
    query_minor,
    keys_minor,
    values_minor,
    lambda_major,
    lambda_minor,
    gain_major,
    gain_minor,
    output_major,
    output_minor,
    mixer_gain,
    up_weight,
    down_weight,
):
    sp_count, tp_count = lax.axis_size("sp"), lax.axis_size("tp")
    args = (
        residual,
        query_major,
        keys_major,
        values_major,
        query_minor,
        keys_minor,
        values_minor,
        lambda_major,
        lambda_minor,
        gain_major[None, :],
        jnp.tile(gain_minor, 2)[None, :],
        output_major,
        output_minor,
        mixer_gain[None, :],
        up_weight,
        down_weight,
    )
    if fits_fused(sp_count, tp_count, args):
        return fused(sp_count, tp_count, args)
    out_major, out_minor, up_full, down_full = mixer(
        lax.axis_size("sp"),
        query_major,
        keys_major,
        values_major,
        query_minor,
        jnp.concatenate([keys_minor, values_minor], axis=1),
        lambda_major,
        lambda_minor,
        gain_major[:, None],
        gain_minor[:, None],
        up_weight,
        down_weight,
    )
    partial_sum = jnp.dot(out_major, output_major, preferred_element_type=jnp.float32)
    partial_sum = partial_sum + jnp.dot(out_minor, output_minor, preferred_element_type=jnp.float32)
    rows = residual.shape[0]
    stream, normed_all = tp_call(
        mix_kernel,
        1,
        (partial_sum.astype(jnp.bfloat16), residual, mixer_gain[None, :]),
        (
            jax.ShapeDtypeStruct(residual.shape, jnp.float32),
            jax.ShapeDtypeStruct(partial_sum.shape, jnp.bfloat16),
        ),
        rows,
        True,
    )
    pre_act = jnp.dot(
        normed_all,
        up_full,
        preferred_element_type=jnp.float32,
    )
    hidden = jnp.square(jax.nn.relu(pre_act)).astype(jnp.bfloat16)
    down_part = jnp.einsum("th,shd->tsd", hidden, down_full, preferred_element_type=jnp.float32)
    down_part = down_part.astype(jnp.bfloat16).reshape(partial_sum.shape)
    return tp_call(
        sum_kernel,
        2,
        (down_part, stream),
        jax.ShapeDtypeStruct(residual.shape, residual.dtype),
        rows,
        False,
    )


def solution(mesh):
    return jax.shard_map(
        body,
        mesh=mesh,
        in_specs=(
            P(("sp", "tp"), None),
            P("sp", "tp"),
            P("sp", "tp"),
            P("sp", "tp"),
            P("sp", "tp"),
            P("sp", "tp"),
            P("sp", "tp"),
            P("tp"),
            P("tp"),
            P(),
            P(),
            P("tp", None),
            P("tp", None),
            P(),
            P("sp", "tp"),
            P("tp", "sp"),
        ),
        out_specs=P(("sp", "tp"), None),
        check_vma=False,
    )
```

```python
import functools

import jax
import jax.numpy as jnp
from jax import lax
from jax.experimental import pallas as pl
from jax.experimental.pallas import tpu as pltpu
from jax.sharding import PartitionSpec as P

DK_MAJOR = 64
DK_MINOR = 32
SEGMENT = 64
MAPS = 2
PARTS = 2

EPSILON = 1e-06
NEGATIVE = -1e30
LOG2_E = 1.4426950408889634
ANY = pl.BlockSpec(memory_space=pl.ANY)
VMEM = pl.BlockSpec(memory_space=pltpu.VMEM)
SMEM = pl.BlockSpec(memory_space=pltpu.SMEM)


def grid_sizes(sp_count):
    y_count = 1 << ((sp_count.bit_length() - 1) // 2)
    return sp_count // y_count, y_count


class Gather:
    def __init__(self, sp_count, places, send_sem, recv_sem):
        self.z_count, self.y_count = grid_sizes(sp_count)
        own = lax.axis_index("sp")
        self.own, self.z, self.y = own, own // self.y_count, lax.rem(own, self.y_count)
        self.places, self.send_sem, self.recv_sem = places, send_sem, recv_sem
        self.copies = []

    def z_peer(self, step):
        return lax.rem(self.z + step, self.z_count) * self.y_count + self.y

    def y_peer(self, step):
        return self.z * self.y_count + lax.rem(self.y + step, self.y_count)

    def send(self, array, source, src_ref, target):
        copy = pltpu.make_async_remote_copy(
            src_ref=src_ref,
            dst_ref=self.places[array](source),
            send_sem=self.send_sem.at[array, len([c for c in self.copies if c[0] == array])],
            recv_sem=self.recv_sem.at[array, source],
            device_id={"sp": target},
            device_id_type=pl.DeviceIdType.MESH,
        )
        copy.start()
        self.copies.append((array, copy))

    def wait_block(self, array, source):
        place = self.places[array](source)
        pltpu.make_async_remote_copy(
            src_ref=place,
            dst_ref=place,
            send_sem=self.send_sem.at[array, 0],
            recv_sem=self.recv_sem.at[array, source],
            device_id={"sp": self.y_peer(1)},
            device_id_type=pl.DeviceIdType.MESH,
        ).wait_recv()

    def send_z(self, array, src_ref):
        for step in range(1, self.z_count):
            self.send(array, self.own, src_ref, self.z_peer(step))

    def send_y(self, array, src_ref):
        for step in range(1, self.y_count):
            self.send(array, self.own, src_ref, self.y_peer(step))

    def pass_on(self, array, step):
        source = self.z_peer(self.z_count - step)
        self.wait_block(array, source)
        for y_step in range(1, self.y_count):
            self.send(array, source, self.places[array](source), self.y_peer(y_step))

    def wait_y(self, array):
        for y_step in range(1, self.y_count):
            for z_step in range(self.z_count):
                z_at = lax.rem(self.z + z_step, self.z_count)
                self.wait_block(array, z_at * self.y_count + lax.rem(self.y + y_step, self.y_count))

    def finish(self):
        for _, copy in self.copies:
            copy.wait_send()


def mixer_kernel(
    sp_count,
    groups,
    q_major,
    k_major,
    v_major,
    q_minor,
    kv_minor,
    lam_major,
    lam_minor,
    gain_major,
    gain_minor,
    up_ref,
    down_ref,
    out_major,
    out_minor,
    up_all,
    down_all,
    k_major_all,
    v_major_all,
    kv_minor_all,
    qm_major,
    qm_minor,
    acc_major,
    acc_minor,
    peaks,
    totals,
    send_sem,
    recv_sem,
    local_sem,
):
    rows = q_major.shape[0]
    up_rows = up_ref.shape[0]

    def rows_of(ref, count):
        return lambda source: ref.at[pl.ds(pl.multiple_of(source * count, count), count), :]

    places = [
        rows_of(k_major_all, rows),
        rows_of(v_major_all, rows),
        rows_of(kv_minor_all, rows),
        rows_of(up_all, up_rows),
        lambda source: down_all.at[source],
    ]
    own_refs = [k_major, v_major, kv_minor, up_ref, down_ref]
    gather = Gather(sp_count, places, send_sem, recv_sem)
    own = gather.own

    barrier = pltpu.get_barrier_semaphore()
    peers = [gather.z_peer(step) for step in range(1, gather.z_count)]
    peers += [gather.y_peer(step) for step in range(1, gather.y_count)]
    for peer in peers:
        pl.semaphore_signal(
            barrier, inc=1, device_id={"sp": peer}, device_id_type=pl.DeviceIdType.MESH
        )
    pl.semaphore_wait(barrier, len(peers))

    for array in range(3):
        gather.send_z(array, own_refs[array])
    for array in range(3):
        gather.send_y(array, own_refs[array])
    for array in (3, 4):
        gather.send_z(array, own_refs[array])
    for array in (3, 4):
        gather.send_y(array, own_refs[array])
    local = []
    for slot, array in enumerate((3, 4)):
        copy = pltpu.make_async_copy(own_refs[array], places[array](own), local_sem.at[slot])
        copy.start()
        local.append(copy)

    heads = []
    for group, (head_count, key_size) in enumerate(groups):
        q_ref, qm_ref = ((q_major, qm_major), (q_minor, qm_minor))[group]
        acc_ref = (acc_major, acc_minor)[group]
        value_size = acc_ref.shape[1]
        lanes = qm_ref.shape[2]
        for head in range(head_count):
            first = head * MAPS * key_size
            lane_first = first // lanes * lanes
            block = q_ref[:, lane_first : lane_first + lanes]
            lane = lax.broadcasted_iota(jnp.int32, block.shape, 1) + lane_first
            for m in range(MAPS):
                low = first + m * key_size
                keep = (lane >= low) & (lane < low + key_size)
                picked = jnp.where(keep, block.astype(jnp.float32), 0.0).astype(block.dtype)
                qm_ref[head, m * rows : (m + 1) * rows, :] = picked
            heads.append((group, head, len(heads), lane_first, lanes, value_size, key_size))

    minor_keys = q_minor.shape[1]
    minor_first = minor_keys // 128 * 128

    def fold(key_refs, value_refs, at, diagonal):
        window = pl.ds(at, rows)
        stored = (value_refs[0][window, :], value_refs[1][window, minor_first:])
        turned = [jnp.transpose(v.astype(jnp.float32)).astype(jnp.bfloat16) for v in stored]
        turned[1] = turned[1][minor_keys - minor_first :, :]
        for group, head, index, lane_first, lanes, value_size, key_size in heads:
            qm_ref = (qm_major, qm_minor)[group]
            acc_ref = (acc_major, acc_minor)[group]
            keys = key_refs[group][window, lane_first : lane_first + lanes]
            values = turned[group][head * value_size : (head + 1) * value_size, :]
            scores = lax.dot_general(
                keys, qm_ref[head], (((1,), (1,)), ((), ())), preferred_element_type=jnp.float32
            ) * (key_size ** (-0.5) * LOG2_E)
            if diagonal:
                key_pos = lax.broadcasted_iota(jnp.int32, scores.shape, 0)
                query_pos = lax.broadcasted_iota(jnp.int32, scores.shape, 1) % rows
                visible = key_pos // SEGMENT <= query_pos // SEGMENT
                scores = jnp.where(visible, scores, NEGATIVE)
            peak = jnp.max(scores, axis=0, keepdims=True)
            if not diagonal:
                peak_old = peaks[index]
                peak = jnp.maximum(peak, peak_old)
            weights = jnp.exp2(scores - peak)
            total = jnp.sum(weights, axis=0, keepdims=True)
            sums = jnp.dot(
                values, weights.astype(jnp.bfloat16), preferred_element_type=jnp.float32
            )
            if not diagonal:
                factor = jnp.exp2(peak_old - peak)
                total = total + totals[index] * factor
                sums = sums + acc_ref[head] * factor
            peaks[index] = peak
            totals[index] = total
            acc_ref[head] = sums

    fold((k_major, kv_minor), (v_major, kv_minor), 0, True)

    for step in range(1, gather.z_count):
        for array in range(3):
            gather.pass_on(array, step)

    def earlier(block, carry):
        at = pl.multiple_of(block * rows, rows)
        fold((k_major_all, kv_minor_all), (v_major_all, kv_minor_all), at, False)
        return carry

    y_count = gather.y_count

    def same_y(z_at, carry):
        return earlier(z_at * y_count + gather.y, carry)

    def other_y(index, carry):
        z_at, place = index // (y_count - 1), lax.rem(index, y_count - 1)
        y_at = place + (place >= gather.y).astype(jnp.int32)
        return earlier(z_at * y_count + y_at, carry)

    lax.fori_loop(0, gather.z, same_y, 0)
    for array in range(3):
        gather.wait_y(array)
    lax.fori_loop(0, gather.z * (y_count - 1) + gather.y, other_y, 0)

    for group, (head_count, _) in enumerate(groups):
        acc_ref = (acc_major, acc_minor)[group]
        lam_ref = (lam_major, lam_minor)[group]
        gain_ref = (gain_major, gain_minor)[group]
        out_ref = (out_major, out_minor)[group]
        done = []
        for head in range(head_count):
            index = next(h[2] for h in heads if h[0] == group and h[1] == head)
            ratio = acc_ref[head] / totals[index]
            diff = ratio[:, :rows] - lam_ref[head] * ratio[:, rows:]
            mean = jnp.mean(diff * diff, axis=0, keepdims=True)
            done.append(diff * lax.rsqrt(mean + EPSILON) * gain_ref[...])
        out_ref[...] = jnp.transpose(jnp.concatenate(done, axis=0)).astype(out_ref.dtype)

    for step in range(1, gather.z_count):
        for array in (3, 4):
            gather.pass_on(array, step)
    for array in (3, 4):
        gather.wait_y(array)
    for copy in local:
        copy.wait()
    gather.finish()


def mixer(sp_count, *args):
    q_major, k_major, v_major, q_minor, kv_minor = args[:5]
    up_weight, down_weight = args[9:11]
    heads_major = k_major.shape[1] // (MAPS * DK_MAJOR)
    heads_minor = q_minor.shape[1] // (MAPS * DK_MINOR)
    rows = q_major.shape[0]
    size_major = v_major.shape[1] // heads_major
    width_minor = kv_minor.shape[1] - q_minor.shape[1]
    size_minor = width_minor // heads_minor
    lanes_major = min(MAPS * DK_MAJOR, q_major.shape[1])
    lanes_minor = min(128, q_minor.shape[1])
    z_count, y_count = grid_sizes(sp_count)
    sends = (z_count - 1) + (y_count - 1) * z_count
    tokens = rows * sp_count
    bf16, f32 = jnp.bfloat16, jnp.float32
    head_total = heads_major + heads_minor
    return pl.pallas_call(
        functools.partial(
            mixer_kernel, sp_count, ((heads_major, DK_MAJOR), (heads_minor, DK_MINOR))
        ),
        out_shape=(
            jax.ShapeDtypeStruct(v_major.shape, bf16),
            jax.ShapeDtypeStruct((rows, width_minor), bf16),
            jax.ShapeDtypeStruct((up_weight.shape[0] * sp_count, up_weight.shape[1]), bf16),
            jax.ShapeDtypeStruct((sp_count, *down_weight.shape), bf16),
        ),
        in_specs=[VMEM] * 5 + [SMEM] * 2 + [VMEM] * 4,
        out_specs=(VMEM, VMEM, ANY, ANY),
        scratch_shapes=[
            pltpu.VMEM((tokens, k_major.shape[1]), bf16),
            pltpu.VMEM((tokens, v_major.shape[1]), bf16),
            pltpu.VMEM((tokens, kv_minor.shape[1]), bf16),
            pltpu.VMEM((heads_major, MAPS * rows, lanes_major), bf16),
            pltpu.VMEM((heads_minor, MAPS * rows, lanes_minor), bf16),
            pltpu.VMEM((heads_major, size_major, MAPS * rows), f32),
            pltpu.VMEM((heads_minor, size_minor, MAPS * rows), f32),
            pltpu.VMEM((head_total, 1, MAPS * rows), f32),
            pltpu.VMEM((head_total, 1, MAPS * rows), f32),
            pltpu.SemaphoreType.DMA((5, sends)),
            pltpu.SemaphoreType.DMA((5, sp_count)),
            pltpu.SemaphoreType.DMA((2,)),
        ],
        compiler_params=pltpu.CompilerParams(
            collective_id=0, has_side_effects=True, vmem_limit_bytes=60 * 1024 * 1024
        ),
    )(*args)


class Exchange:
    def __init__(self, tp_count, send_sem, recv_sem):
        own = lax.axis_index("tp")
        self.x_count = tp_count // 2
        self.own, self.x, self.core = own, own // 2, lax.rem(own, 2)
        self.partner = self.x * 2 + 1 - self.core
        self.send_sem, self.recv_sem = send_sem, recv_sem

    def enter(self):
        barrier = pltpu.get_barrier_semaphore()
        peers = [self.partner] + [self.x_peer(step) for step in range(1, self.x_count)]
        for peer in peers:
            pl.semaphore_signal(
                barrier, inc=1, device_id={"tp": peer}, device_id_type=pl.DeviceIdType.MESH
            )
        pl.semaphore_wait(barrier, len(peers))

    def x_peer(self, step):
        return lax.rem(self.x + step, self.x_count) * 2 + self.core

    def copy(self, src, dst, slot, target):
        made = pltpu.make_async_remote_copy(
            src_ref=src,
            dst_ref=dst,
            send_sem=self.send_sem.at[slot],
            recv_sem=self.recv_sem.at[slot],
            device_id={"tp": target},
            device_id_type=pl.DeviceIdType.MESH,
        )
        made.start()
        return made

    def total(self, partial, pair_in, pair_sum, x_in, rows):
        def block(x_at, core):
            return pl.ds(pl.multiple_of((x_at * 2 + core) * rows, rows), rows)

        steps = list(range(1, self.x_count)) + [0]
        at = [lax.rem(self.x + step, self.x_count) for step in range(self.x_count)]
        pair = {}
        for step in steps:
            pair[step] = self.copy(
                partial.at[block(at[step], 1 - self.core), :], pair_in.at[step], step, self.partner
            )
        across = []
        for step in steps:
            pair[step].wait_recv()
            mine = partial[block(at[step], self.core), :].astype(jnp.float32)
            both = mine + pair_in[step].astype(jnp.float32)
            if step:
                pair_sum[step] = both.astype(jnp.bfloat16)
                across.append(
                    self.copy(
                        pair_sum.at[step], x_in.at[step], self.x_count + step, self.x_peer(step)
                    )
                )
        for made in across:
            made.wait_recv()
        for step in range(1, self.x_count):
            both = both + x_in[step].astype(jnp.float32)
        return both, list(pair.values()) + across


def mix_kernel(
    tp_count, partial, residual, gain, stream_ref, normed_ref, pair_in, pair_sum, x_in, held, send_sem, recv_sem
):
    exchange = Exchange(tp_count, send_sem, recv_sem)
    exchange.enter()
    rows = residual.shape[0]
    mixed, copies = exchange.total(partial, pair_in, pair_sum, x_in, rows)
    stream = residual[...].astype(jnp.float32) + mixed
    stream_ref[...] = stream
    mean = jnp.mean(stream * stream, axis=-1, keepdims=True)
    normed = (stream * lax.rsqrt(mean + EPSILON) * gain[...]).astype(jnp.bfloat16)
    held[...] = normed

    def place(index):
        return normed_ref.at[pl.ds(pl.multiple_of(index * rows, rows), rows), :]

    base, count = 2 * exchange.x_count, exchange.x_count
    sent = [exchange.copy(held, place(exchange.own), base + step, exchange.x_peer(step)) for step in range(1, count)]
    passed = [exchange.copy(held, place(exchange.own), base + count, exchange.partner)]
    normed_ref[pl.ds(pl.multiple_of(exchange.own * rows, rows), rows), :] = normed
    for step in range(1, count):
        sent[step - 1].wait_recv()
        source = exchange.x_peer(count - step)
        passed.append(
            exchange.copy(place(source), place(source), base + count + step, exchange.partner)
        )
    for made in passed:
        made.wait_recv()
    for made in copies + sent + passed:
        made.wait_send()


def sum_kernel(tp_count, partial, stream, out_ref, pair_in, pair_sum, x_in, send_sem, recv_sem):
    exchange = Exchange(tp_count, send_sem, recv_sem)
    exchange.enter()
    total, copies = exchange.total(partial, pair_in, pair_sum, x_in, stream.shape[0])
    out_ref[...] = (stream[...] + total).astype(out_ref.dtype)
    for made in copies:
        made.wait_send()


def tp_call(kernel, identity, inputs, out_shape, rows, holds):
    tp_count = lax.axis_size("tp")
    slots = (tp_count // 2, rows, inputs[0].shape[1])
    held = [pltpu.VMEM(slots[1:], jnp.bfloat16)] if holds else []
    return pl.pallas_call(
        functools.partial(kernel, tp_count),
        out_shape=out_shape,
        in_specs=[VMEM] * len(inputs),
        out_specs=jax.tree.map(lambda _: VMEM, out_shape),
        scratch_shapes=[pltpu.VMEM(slots, jnp.bfloat16)] * 3
        + held
        + [pltpu.SemaphoreType.DMA((2 * tp_count,))] * 2,
        compiler_params=pltpu.CompilerParams(
            collective_id=identity, has_side_effects=True, vmem_limit_bytes=32 * 1024 * 1024
        ),
    )(*inputs)


class Sender:
    def __init__(self, sem):
        self.sem, self.made = sem, []

    def prepare(self, src, dst, recv, target, when=None):
        copy = pltpu.make_async_remote_copy(
            src_ref=src,
            dst_ref=dst,
            send_sem=self.sem.at[len(self.made)],
            recv_sem=recv,
            device_id=target,
            device_id_type=pl.DeviceIdType.MESH,
        )
        self.made.append((when, copy))
        return lambda: run_when(when, copy.start)

    def send(self, src, dst, recv, target, when=None):
        self.prepare(src, dst, recv, target, when)()

    def finish(self):
        for when, copy in self.made:
            run_when(when, copy.wait_send)


def run_when(when, action):
    if when is None:
        action()
    else:
        pl.when(when)(lambda: action())


def layer_kernel(
    sizes,
    residual,
    q_major,
    k_major,
    v_major,
    q_minor,
    k_minor,
    v_minor,
    lam_major,
    lam_minor,
    gain_major,
    gain_minor,
    wo_major,
    wo_minor,
    mixer_gain,
    up_ref,
    down_ref,
    out_ref,
    pack,
    kv_all,
    q_in,
    qm,
    acc,
    peaks,
    totals,
    heads_out,
    cat,
    minor_in,
    wo_all,
    stream,
    normed_all,
    up_all,
    down_all,
    hidden,
    d_send,
    d_in,
    mine,
    x_send,
    x_in,
    x_keep,
    z_send,
    z_in,
    z_keep,
    send_sem,
    relay_sem,
    local_sem,
    r_y,
    r_kv,
    r_w,
    r_wo,
    r_h,
    r_g,
    r_d,
    r_x,
    r_z,
    credits,
):
    z_count, y_count, x_count = sizes
    bf16, f32 = jnp.bfloat16, jnp.float32
    own, tp = lax.axis_index("sp"), lax.axis_index("tp")
    z, y = own // y_count, lax.rem(own, y_count)
    x, c = tp // 2, lax.rem(tp, 2)
    oy, ox, oc = 1 - y, 1 - x, 1 - c
    zl = lax.rem(z, 2)
    oz = z + 1 - 2 * zl
    rows, tile = q_major.shape[0], residual.shape[0]
    width = q_minor.shape[1]
    half = width // 2
    hid = up_ref.shape[1] // 2
    up_rows = up_ref.shape[0]
    cols = down_ref.shape[1]

    def dev(z_at=z, y_at=y, x_at=x, c_at=c):
        return {"sp": z_at * y_count + y_at, "tp": x_at * 2 + c_at}

    def span(start, count):
        return pl.ds(pl.multiple_of(start * count, count), count)

    def arrive(place, recv):
        pltpu.make_async_remote_copy(
            src_ref=place,
            dst_ref=place,
            send_sem=send_sem.at[0],
            recv_sem=recv,
            device_id=dev(y_at=oy),
            device_id_type=pl.DeviceIdType.MESH,
        ).wait_recv()

    k_low = lax.broadcasted_iota(jnp.int32, (rows, width), 1)
    for head in range(2):
        k_part = (k_low >= head * half) & (k_low < (head + 1) * half)
        turned_v = pltpu.roll(v_minor[...].astype(f32), half, 1)
        pack[head] = jnp.where(k_part, k_minor[...].astype(f32), turned_v).astype(bf16)

    barrier = pltpu.get_barrier_semaphore()
    peers = []
    for dy in range(2):
        for dx in range(2):
            for dc in range(2):
                if dy or dx or dc:
                    peers.append(dev(y_at=oy if dy else y, x_at=ox if dx else x, c_at=oc if dc else c))
    peers += [dev(z_at=lax.rem(z + step, z_count)) for step in range(1, z_count)]
    for peer in peers:
        pl.semaphore_signal(barrier, inc=1, device_id=peer, device_id_type=pl.DeviceIdType.MESH)

    kv_all[z, 0, span(y, rows), :] = k_major[:, span(y, width)]
    kv_all[z, 1, span(y, rows), :] = v_major[:, span(y, width)]
    kv_all[z, 2, span(y, rows), :] = pack[y]
    local = []
    local_pairs = [
        (up_ref.at[:, span(zl, hid)], up_all.at[span(own, up_rows), :]),
        (down_ref.at[span(zl, hid), :], down_all.at[own]),
    ]
    major_rows, minor_rows = wo_major.shape[0], wo_minor.shape[0]
    tp_count = 2 * x_count
    minor_base = tp_count * major_rows

    def wo_place(part, index):
        if part == 0:
            return wo_all.at[span(index, major_rows), :]
        return wo_all.at[pl.ds(pl.multiple_of(minor_base + index * minor_rows, minor_rows), minor_rows), :]

    for part, ref in enumerate((wo_major, wo_minor)):
        local_pairs.append((ref, wo_place(part, tp)))
    for slot, (src, dst) in enumerate(local_pairs):
        made = pltpu.make_async_copy(src, dst, local_sem.at[slot])
        made.start()
        local.append(made)

    pl.semaphore_wait(barrier, len(peers))

    sender = Sender(send_sem)
    has_up = z < z_count - 1
    next_z = jnp.minimum(z + 1, z_count - 1)

    def kv_place(z_at, part, side):
        return kv_all.at[z_at, part, span(side, rows), :]

    for part, src in enumerate((k_major.at[:, span(oy, width)], v_major.at[:, span(oy, width)], pack.at[oy])):
        sender.send(src, kv_place(z, part, y), r_y.at[part], dev(y_at=oy))
    sender.send(q_major.at[:, span(oy, width)], q_in.at[0], r_y.at[3], dev(y_at=oy))
    sender.send(q_minor, q_in.at[1], r_y.at[4], dev(y_at=oy))
    for part, src in enumerate((k_major.at[:, span(y, width)], v_major.at[:, span(y, width)], pack.at[y])):
        sender.send(src, kv_place(z, part, y), r_kv.at[z, y, part], dev(z_at=next_z), has_up)

    up_part, down_part = up_rows // PARTS, hid // PARTS
    up_kinds, down_kinds = tuple(range(PARTS)), tuple(range(PARTS, 2 * PARTS))

    def weight_src(kind, z_at):
        parity = lax.rem(z_at, 2)
        if kind < PARTS:
            return up_ref.at[kind * up_part : (kind + 1) * up_part, span(parity, hid)]
        return down_ref.at[span(parity * PARTS + kind - PARTS, down_part), :]

    def weight_place(kind, source):
        if kind < PARTS:
            return up_all.at[span(source * PARTS + kind, up_part), :]
        return down_all.at[source, (kind - PARTS) * down_part : (kind - PARTS + 1) * down_part, :]

    def send_weight(kind, z_at, y_at, when=None):
        return sender.prepare(
            weight_src(kind, z_at), weight_place(kind, own), r_w.at[kind, own], dev(z_at=z_at, y_at=y_at), when
        )

    def below(kinds, last=1, first=z_count - 1):
        return [
            send_weight(kind, jnp.maximum(z - step, 0), y, z >= step)
            for step in range(first, last - 1, -1)
            for kind in kinds
        ]

    def above(kinds, step, odd=None):
        when = z + step < z_count
        if odd is not None:
            when = when & (lax.rem(z + step, 2) == odd)
        return [send_weight(kind, jnp.minimum(z + step, z_count - 1), y, when) for kind in kinds]

    def issue(starts):
        for start in starts:
            start()

    issue(below(up_kinds))
    for kind in up_kinds + down_kinds:
        send_weight(kind, z, oy)()
    for part, ref in enumerate((wo_major, wo_minor)):
        sender.send(ref, wo_place(part, tp), r_wo.at[part, tp], dev(x_at=ox))
        sender.send(ref, wo_place(part, tp), r_wo.at[part, tp], dev(c_at=oc))
    below_far, below_near = below(down_kinds, 2), below(down_kinds, 1, 1)
    slow = (zl == 1) & (z > 1)
    near_up = above(up_kinds, 1)
    late_up = (zl == 0) & (z > 0)

    scales = (DK_MAJOR ** (-0.5) * LOG2_E, DK_MINOR ** (-0.5) * LOG2_E)
    lane = lax.broadcasted_iota(jnp.int32, (rows, width), 1)

    def pick(group, side, block):
        first, size = (0, DK_MAJOR) if group == 0 else (y * half, DK_MINOR)
        for m in range(MAPS):
            low = first + m * size
            keep = (lane >= low) & (lane < low + size)
            qm[group, side, m * rows : (m + 1) * rows, :] = jnp.where(keep, block.astype(f32), 0.0).astype(bf16)

    def fold(side, z_at, key_side, diagonal):
        window = span(key_side, rows)
        for group in range(2):
            keys = kv_all[z_at, 2 * group, window, :]
            stored = kv_all[z_at, 1 + group, window, :]
            values = jnp.transpose(stored.astype(f32)).astype(bf16)
            scores = lax.dot_general(
                keys, qm[group, side], (((1,), (1,)), ((), ())), preferred_element_type=f32
            ) * scales[group]
            if diagonal:
                key_pos = lax.broadcasted_iota(jnp.int32, scores.shape, 0)
                query_pos = lax.broadcasted_iota(jnp.int32, scores.shape, 1) % rows
                visible = key_pos // SEGMENT <= query_pos // SEGMENT
                scores = jnp.where(visible, scores, NEGATIVE)
            peak = jnp.max(scores, axis=0, keepdims=True)
            if not diagonal:
                peak_old = peaks[group, side]
                peak = jnp.maximum(peak, peak_old)
            weights = jnp.exp2(scores - peak)
            total = jnp.sum(weights, axis=0, keepdims=True)
            sums = jnp.dot(values, weights.astype(bf16), preferred_element_type=f32)
            if not diagonal:
                factor = jnp.exp2(peak_old - peak)
                total = total + totals[group, side] * factor
                sums = sums + acc[group, side] * factor
            peaks[group, side] = peak
            totals[group, side] = total
            acc[group, side] = sums

    pick(0, y, q_major[:, span(y, width)])
    pick(1, y, q_minor[...])
    fold(y, z, y, True)

    for part in range(3):
        arrive(kv_place(z, part, oy), r_y.at[part])
        sender.send(kv_place(z, part, oy), kv_place(z, part, oy), r_kv.at[z, oy, part], dev(z_at=next_z), has_up)

    def credit(kind, back):
        pl.semaphore_signal(
            credits.at[kind, z],
            inc=1,
            device_id=dev(z_at=jnp.maximum(z - back, 0)),
            device_id_type=pl.DeviceIdType.MESH,
        )

    def await_credit(kind, step):
        pl.semaphore_wait(credits.at[kind, jnp.minimum(z + step, z_count - 1)], 1)

    def relay_copy(z_at, side, part):
        return pltpu.make_async_remote_copy(
            src_ref=kv_place(z_at, part, side),
            dst_ref=kv_place(z_at, part, side),
            send_sem=relay_sem.at[z_at, side, part],
            recv_sem=r_kv.at[z_at, side, part],
            device_id=dev(z_at=next_z),
            device_id_type=pl.DeviceIdType.MESH,
        )

    def take(z_at, side):
        for part in range(3):
            arrive(kv_place(z_at, part, side), r_kv.at[z_at, side, part])
            run_when(has_up, relay_copy(z_at, side, part).start)

    def after_last():
        run_when(zl == 1, lambda: issue(near_up))
        for back in range(2, z_count):
            run_when(z >= back, lambda: credit(0, back))

        @pl.when(jnp.logical_not(slow))
        def _():
            issue(below_far)
            issue(below_near)

    for part in range(2):
        arrive(q_in.at[part], r_y.at[3 + part])
        pick(part, oy, q_in[part])

    pl.when(z == 0)(lambda: issue(near_up))

    @pl.when(z > 0)
    def _():
        for side in range(2):
            take(z - 1, side)

    pl.when(z == 1)(after_last)
    fold(oy, z, oy, True)
    fold(1, z, 0, False)

    def earlier(index, carry):
        z_at, key_side = z - 1 - index // 2, lax.rem(index, 2)
        pl.when(index > 1)(lambda: take(z_at, key_side))
        pl.when((index == 2 * z - 1) & (z > 1))(after_last)
        pl.when((index == 2 * z - 2) & slow)(lambda: issue(below_far))

        def inner(side, carry):
            fold(side, z_at, key_side, False)
            return carry

        lax.fori_loop(0, 2, inner, 0)
        return carry

    lax.fori_loop(0, 2 * z, earlier, 0)

    value_row = lax.broadcasted_iota(jnp.int32, (width, rows), 0)
    value_keep = (value_row >= oy * half) & (value_row < (oy + 1) * half)
    gains = (gain_major[...], gain_minor[...])
    lams = (lam_major[y], lam_minor[y])

    def close(side, carry):
        for group in range(2):
            ratio = acc[group, side] / totals[group, side]
            diff = ratio[:, :rows] - lams[group] * ratio[:, rows:]
            if group == 1:
                diff = jnp.where(value_keep, diff, 0.0)
            count = width if group == 0 else half
            mean = jnp.sum(diff * diff, axis=0, keepdims=True) * (1.0 / count)
            done = jnp.transpose(diff * lax.rsqrt(mean + EPSILON)) * gains[group]
            heads_out[group, span(side, rows), :] = done.astype(bf16)
        return carry

    lax.fori_loop(0, 2, close, 0)

    place = tp * y_count + y

    def token_span(y_at, x_at, c_at):
        return span(y_at * (rows // tile) + x_at * 2 + c_at, tile)

    def head_place(group, index):
        return cat.at[:, span(index, width)] if group == 0 else minor_in.at[index]

    for dy, dx, dc in ((1, 1, 1), (1, 1, 0), (1, 0, 1), (1, 0, 0), (0, 1, 1), (0, 1, 0), (0, 0, 1)):
        y_at, x_at, c_at = oy if dy else y, ox if dx else x, oc if dc else c
        for group in range(2):
            sender.send(
                heads_out.at[group, token_span(y_at, x_at, c_at), :],
                head_place(group, place),
                r_h.at[group, place],
                dev(y_at=y_at, x_at=x_at, c_at=c_at),
            )
    cat[:, span(place, width)] = heads_out[0, token_span(y, x, c), :]
    minor_in[place] = heads_out[1, token_span(y, x, c), :]

    def pass_weight(kind, z_at, when):
        source = z_at * y_count + y
        run_when(when, lambda: arrive(weight_place(kind, source), r_w.at[kind, source]))
        sender.send(weight_place(kind, source), weight_place(kind, source), r_w.at[kind, source], dev(y_at=oy), when)

    for step in range(1, z_count):
        for kind in up_kinds:
            pass_weight(kind, lax.rem(z + step, z_count), z + step < z_count)
    for step in range(2, z_count):
        run_when(z + step < z_count, lambda: await_credit(0, step))
        issue(above(up_kinds, step))

    for made in local:
        made.wait()
    for part in range(2):
        index = ox * 2 + c
        arrive(wo_place(part, index), r_wo.at[part, index])
        sender.send(wo_place(part, index), wo_place(part, index), r_wo.at[part, index], dev(c_at=oc))
    for index in (x * 2 + oc, ox * 2 + oc):
        for part in range(2):
            arrive(wo_place(part, index), r_wo.at[part, index])
    for dy, dx, dc in ((0, 0, 1), (0, 1, 0), (0, 1, 1), (1, 0, 0), (1, 0, 1), (1, 1, 0), (1, 1, 1)):
        index = ((ox if dx else x) * 2 + (oc if dc else c)) * y_count + (oy if dy else y)
        for group in range(2):
            arrive(head_place(group, index), r_h.at[group, index])
    major_width = tp_count * y_count * width
    for index in range(tp_count):
        both = minor_in[index * y_count].astype(f32) + minor_in[index * y_count + 1].astype(f32)
        cat[:, major_width + index * width : major_width + (index + 1) * width] = pltpu.roll(both, half, 1).astype(bf16)

    model = residual.shape[1]
    step_cols = 256

    def project(index, carry):
        window = span(index, step_cols)
        mixed = jnp.dot(cat[...], wo_all[:, window], preferred_element_type=f32)
        added = residual[:, window].astype(f32) + mixed
        stream[:, window] = added
        return carry + jnp.sum(added * added, axis=1, keepdims=True)

    square = lax.fori_loop(0, model // step_cols, project, jnp.zeros((tile, 1), f32))
    norm = lax.rsqrt(square * (1.0 / model) + EPSILON)

    def slot(c_at, x_at, zl_at):
        return c_at * (2 * x_count) + x_at * 2 + zl_at

    def rows_at(index):
        return normed_all.at[span(index, tile), :]

    mine_at = slot(c, x, zl)
    normed_all[span(mine_at, tile), :] = (stream[...] * norm * mixer_gain[...]).astype(bf16)

    def share(index, target):
        sender.send(rows_at(index), rows_at(index), r_g.at[index], target)

    partner, x_peer, z_peer = dev(c_at=oc), dev(x_at=ox), dev(z_at=oz)
    share(mine_at, z_peer)
    share(mine_at, x_peer)
    share(mine_at, partner)
    run_when(late_up, lambda: issue(near_up))
    run_when(slow, lambda: issue(below_near))
    issue(above(down_kinds, 1))
    for step in range(1, z_count - 1):
        for kind in up_kinds:
            pass_weight(kind, lax.rem(z + step, z_count), z + step >= z_count)
    index = slot(c, ox, zl)
    arrive(rows_at(index), r_g.at[index])
    share(index, partner)
    for step in range(2, z_count):
        issue(above(down_kinds, step, 0))
    index = slot(c, x, 1 - zl)
    arrive(rows_at(index), r_g.at[index])
    share(index, x_peer)
    share(index, partner)
    for kind in up_kinds:
        pass_weight(kind, lax.rem(z + z_count - 1, z_count), z > 0)
    for back in range(2, z_count):
        run_when((z >= back) & (zl == 1), lambda: credit(1, back))
    index = slot(c, ox, 1 - zl)
    arrive(rows_at(index), r_g.at[index])
    share(index, partner)
    for step in range(z_count):
        source = lax.rem(z + step, z_count) * y_count + oy
        for kind in up_kinds:
            arrive(weight_place(kind, source), r_w.at[kind, source])
    for step in range(1, z_count):
        for kind in down_kinds:
            pass_weight(kind, lax.rem(z + step, z_count), z + step < z_count)

    for step in range(2, z_count):
        run_when((z + step < z_count) & (lax.rem(z + step, 2) == 1), lambda: await_credit(1, step))
        issue(above(down_kinds, step, 1))

    group_rows = 2 * x_count * tile
    hid_cols = 256

    def expand(side):
        def one(index, carry):
            window = span(index, hid_cols)
            pre = jnp.dot(
                normed_all[span(side, group_rows), :], up_all[:, window], preferred_element_type=f32
            )
            hidden[span(side, group_rows), window] = jnp.square(jnp.maximum(pre, 0.0)).astype(bf16)
            return carry

        lax.fori_loop(0, hid // hid_cols, one, 0)

    expand(c)
    for x_at in range(x_count):
        for zl_at in range(2):
            index = slot(oc, x_at, zl_at)
            arrive(rows_at(index), r_g.at[index])
    expand(oc)

    for step in range(1, z_count):
        for kind in down_kinds:
            pass_weight(kind, lax.rem(z + step, z_count), (z + step >= z_count) & jnp.logical_not(slow))

    x_rows = 2 * tile
    blocks = []

    def stage_x(t):
        arrive(d_in.at[t], r_d.at[t])
        x_send[t] = (mine[t, span(ox, x_rows), :] + d_in[t, span(ox, x_rows), :].astype(f32)).astype(bf16)
        sender.send(x_send.at[t], x_in.at[t], r_x.at[t], x_peer)
        x_keep[t] = mine[t, span(x, x_rows), :] + d_in[t, span(x, x_rows), :].astype(f32)

    def stage_z(t):
        arrive(x_in.at[t], r_x.at[t])
        other, same = span(1 - zl, tile), span(zl, tile)
        z_send[t] = (x_keep[t, other, :] + x_in[t, other, :].astype(f32)).astype(bf16)
        sender.send(z_send.at[t], z_in.at[blocks[t]], r_z.at[blocks[t]], z_peer)
        z_keep[t] = x_keep[t, same, :] + x_in[t, same, :].astype(f32)

    def stage_end(t):
        arrive(z_in.at[blocks[t]], r_z.at[blocks[t]])
        window = span(blocks[t], cols)
        total = stream[:, window] + (z_keep[t] + z_in[blocks[t]].astype(f32))
        out_ref[:, window] = total.astype(out_ref.dtype)

    def advance(t):
        for stage, lag in ((stage_x, 1), (stage_z, 4), (stage_end, 7)):
            if 0 <= t - lag < z_count * y_count:
                stage(t - lag)

    def z_of(t):
        return lax.rem(z - zl + 1 + t // 2, z_count)

    late_pass = {}
    for block in range(2, z_count * y_count, 2):
        for kind in down_kinds:
            at = block if kind > PARTS else max(block - 1, 0) if block > 2 else 0
            late_pass.setdefault(at, []).append((block, kind))
    for t in range(z_count * y_count):
        source = z_of(t) * y_count + (oy if t % 2 else y)
        blocks.append(source)
        for ahead, kind in late_pass.get(t, ()):
            pass_weight(kind, z_of(ahead), slow)
        if t % 2:
            for kind in down_kinds:
                arrive(weight_place(kind, source), r_w.at[kind, source])
        d_send[t] = jnp.dot(
            hidden[span(oc, group_rows), :], down_all[source], preferred_element_type=f32
        ).astype(bf16)
        sender.send(d_send.at[t], d_in.at[t], r_d.at[t], partner)
        mine[t] = jnp.dot(hidden[span(c, group_rows), :], down_all[source], preferred_element_type=f32)
        advance(t)
    for t in range(z_count * y_count, z_count * y_count + 7):
        advance(t)

    sender.finish()
    for step in range(1, z_count):
        for side in range(2):
            for part in range(3):
                copy = relay_copy(jnp.maximum(z - step, 0), side, part)
                run_when((z >= step) & has_up, copy.wait_send)


def fused(sp_count, tp_count, args):
    residual, q_major, _, v_major, q_minor = args[:5]
    wo_major, wo_minor, _, up_weight, down_weight = args[11:16]
    z_count, y_count = grid_sizes(sp_count)
    x_count = tp_count // 2
    rows, tile, width = q_major.shape[0], residual.shape[0], q_minor.shape[1]
    model, hid = residual.shape[1], up_weight.shape[1] // 2
    cols = down_weight.shape[1]
    features = tp_count * (wo_major.shape[0] + wo_minor.shape[0])
    group_rows = 2 * x_count * tile
    steps = sp_count
    bf16, f32 = jnp.bfloat16, jnp.float32
    dma = pltpu.SemaphoreType.DMA
    sends = 192
    hbm = pl.BlockSpec(memory_space=pltpu.HBM)
    return pl.pallas_call(
        functools.partial(layer_kernel, (z_count, y_count, x_count)),
        out_shape=jax.ShapeDtypeStruct(residual.shape, residual.dtype),
        in_specs=[VMEM] * 7 + [SMEM] * 2 + [VMEM] * 2 + [hbm] * 2 + [VMEM] + [hbm] * 2,
        out_specs=VMEM,
        scratch_shapes=[
            pltpu.VMEM((2, rows, width), bf16),
            pltpu.VMEM((z_count, 3, y_count * rows, width), bf16),
            pltpu.VMEM((2, rows, width), bf16),
            pltpu.VMEM((2, 2, MAPS * rows, width), bf16),
            pltpu.VMEM((2, 2, width, MAPS * rows), f32),
            pltpu.VMEM((2, 2, 1, MAPS * rows), f32),
            pltpu.VMEM((2, 2, 1, MAPS * rows), f32),
            pltpu.VMEM((2, y_count * rows, width), bf16),
            pltpu.VMEM((tile, features), bf16),
            pltpu.VMEM((tp_count * y_count, tile, width), bf16),
            pltpu.VMEM((features, model), bf16),
            pltpu.VMEM((tile, model), f32),
            pltpu.VMEM((2 * group_rows, model), bf16),
            pltpu.VMEM((model, hid), bf16),
            pltpu.VMEM((sp_count, hid, cols), bf16),
            pltpu.VMEM((2 * group_rows, hid), bf16),
            pltpu.VMEM((steps, group_rows, cols), bf16),
            pltpu.VMEM((steps, group_rows, cols), bf16),
            pltpu.VMEM((steps, group_rows, cols), f32),
            pltpu.VMEM((steps, 2 * tile, cols), bf16),
            pltpu.VMEM((steps, 2 * tile, cols), bf16),
            pltpu.VMEM((steps, 2 * tile, cols), f32),
            pltpu.VMEM((steps, tile, cols), bf16),
            pltpu.VMEM((steps, tile, cols), bf16),
            pltpu.VMEM((steps, tile, cols), f32),
            dma((sends,)),
            dma((z_count, 2, 3)),
            dma((4,)),
            dma((5,)),
            dma((z_count, 2, 3)),
            dma((2 * PARTS, sp_count)),
            dma((2, tp_count)),
            dma((2, tp_count * y_count)),
            dma((2 * group_rows // tile,)),
            dma((steps,)),
            dma((steps,)),
            dma((steps,)),
            pltpu.SemaphoreType.REGULAR((2, z_count)),
        ],
        compiler_params=pltpu.CompilerParams(
            collective_id=0, has_side_effects=True, vmem_limit_bytes=63 * 1024 * 1024
        ),
    )(*args)


def fits_fused(sp_count, tp_count, args):
    q_major, k_major, v_major, q_minor, k_minor, v_minor = args[1:7]
    z_count, y_count = grid_sizes(sp_count)
    width = q_minor.shape[1]
    return (
        y_count == 2
        and tp_count == 4
        and z_count % 2 == 0
        and width == 2 * MAPS * DK_MINOR
        and width == MAPS * DK_MAJOR
        and width % 128 == 0
        and v_minor.shape[1] == width
        and q_major.shape[1] == v_major.shape[1] == 2 * width
    )


def body(
    residual,
    query_major,
    keys_major,
    values_major,
    query_minor,
    keys_minor,
    values_minor,
    lambda_major,
    lambda_minor,
    gain_major,
    gain_minor,
    output_major,
    output_minor,
    mixer_gain,
    up_weight,
    down_weight,
):
    sp_count, tp_count = lax.axis_size("sp"), lax.axis_size("tp")
    args = (
        residual,
        query_major,
        keys_major,
        values_major,
        query_minor,
        keys_minor,
        values_minor,
        lambda_major,
        lambda_minor,
        gain_major[None, :],
        jnp.tile(gain_minor, 2)[None, :],
        output_major,
        output_minor,
        mixer_gain[None, :],
        up_weight,
        down_weight,
    )
    if fits_fused(sp_count, tp_count, args):
        return fused(sp_count, tp_count, args)
    out_major, out_minor, up_full, down_full = mixer(
        lax.axis_size("sp"),
        query_major,
        keys_major,
        values_major,
        query_minor,
        jnp.concatenate([keys_minor, values_minor], axis=1),
        lambda_major,
        lambda_minor,
        gain_major[:, None],
        gain_minor[:, None],
        up_weight,
        down_weight,
    )
    partial_sum = jnp.dot(out_major, output_major, preferred_element_type=jnp.float32)
    partial_sum = partial_sum + jnp.dot(out_minor, output_minor, preferred_element_type=jnp.float32)
    rows = residual.shape[0]
    stream, normed_all = tp_call(
        mix_kernel,
        1,
        (partial_sum.astype(jnp.bfloat16), residual, mixer_gain[None, :]),
        (
            jax.ShapeDtypeStruct(residual.shape, jnp.float32),
            jax.ShapeDtypeStruct(partial_sum.shape, jnp.bfloat16),
        ),
        rows,
        True,
    )
    pre_act = jnp.dot(
        normed_all,
        up_full,
        preferred_element_type=jnp.float32,
    )
    hidden = jnp.square(jax.nn.relu(pre_act)).astype(jnp.bfloat16)
    down_part = jnp.einsum("th,shd->tsd", hidden, down_full, preferred_element_type=jnp.float32)
    down_part = down_part.astype(jnp.bfloat16).reshape(partial_sum.shape)
    return tp_call(
        sum_kernel,
        2,
        (down_part, stream),
        jax.ShapeDtypeStruct(residual.shape, residual.dtype),
        rows,
        False,
    )


def solution(mesh):
    return jax.shard_map(
        body,
        mesh=mesh,
        in_specs=(
            P(("sp", "tp"), None),
            P("sp", "tp"),
            P("sp", "tp"),
            P("sp", "tp"),
            P("sp", "tp"),
            P("sp", "tp"),
            P("sp", "tp"),
            P("tp"),
            P("tp"),
            P(),
            P(),
            P("tp", None),
            P("tp", None),
            P(),
            P("sp", "tp"),
            P("tp", "sp"),
        ),
        out_specs=P(("sp", "tp"), None),
        check_vma=False,
    )
```

```python
import functools

import jax
import jax.numpy as jnp
from jax import lax
from jax.experimental import pallas as pl
from jax.experimental.pallas import tpu as pltpu
from jax.sharding import PartitionSpec as P

DK_MAJOR = 64
DK_MINOR = 32
SEGMENT = 64
MAPS = 2
PART_UNITS = (4, 3, 2)
PARTS = len(PART_UNITS)
UNITS = 16

EPSILON = 1e-06
NEGATIVE = -1e30
LOG2_E = 1.4426950408889634
ANY = pl.BlockSpec(memory_space=pl.ANY)
VMEM = pl.BlockSpec(memory_space=pltpu.VMEM)
SMEM = pl.BlockSpec(memory_space=pltpu.SMEM)


def grid_sizes(sp_count):
    y_count = 1 << ((sp_count.bit_length() - 1) // 2)
    return sp_count // y_count, y_count


class Gather:
    def __init__(self, sp_count, places, send_sem, recv_sem):
        self.z_count, self.y_count = grid_sizes(sp_count)
        own = lax.axis_index("sp")
        self.own, self.z, self.y = own, own // self.y_count, lax.rem(own, self.y_count)
        self.places, self.send_sem, self.recv_sem = places, send_sem, recv_sem
        self.copies = []

    def z_peer(self, step):
        return lax.rem(self.z + step, self.z_count) * self.y_count + self.y

    def y_peer(self, step):
        return self.z * self.y_count + lax.rem(self.y + step, self.y_count)

    def send(self, array, source, src_ref, target):
        copy = pltpu.make_async_remote_copy(
            src_ref=src_ref,
            dst_ref=self.places[array](source),
            send_sem=self.send_sem.at[array, len([c for c in self.copies if c[0] == array])],
            recv_sem=self.recv_sem.at[array, source],
            device_id={"sp": target},
            device_id_type=pl.DeviceIdType.MESH,
        )
        copy.start()
        self.copies.append((array, copy))

    def wait_block(self, array, source):
        place = self.places[array](source)
        pltpu.make_async_remote_copy(
            src_ref=place,
            dst_ref=place,
            send_sem=self.send_sem.at[array, 0],
            recv_sem=self.recv_sem.at[array, source],
            device_id={"sp": self.y_peer(1)},
            device_id_type=pl.DeviceIdType.MESH,
        ).wait_recv()

    def send_z(self, array, src_ref):
        for step in range(1, self.z_count):
            self.send(array, self.own, src_ref, self.z_peer(step))

    def send_y(self, array, src_ref):
        for step in range(1, self.y_count):
            self.send(array, self.own, src_ref, self.y_peer(step))

    def pass_on(self, array, step):
        source = self.z_peer(self.z_count - step)
        self.wait_block(array, source)
        for y_step in range(1, self.y_count):
            self.send(array, source, self.places[array](source), self.y_peer(y_step))

    def wait_y(self, array):
        for y_step in range(1, self.y_count):
            for z_step in range(self.z_count):
                z_at = lax.rem(self.z + z_step, self.z_count)
                self.wait_block(array, z_at * self.y_count + lax.rem(self.y + y_step, self.y_count))

    def finish(self):
        for _, copy in self.copies:
            copy.wait_send()


def mixer_kernel(
    sp_count,
    groups,
    q_major,
    k_major,
    v_major,
    q_minor,
    kv_minor,
    lam_major,
    lam_minor,
    gain_major,
    gain_minor,
    up_ref,
    down_ref,
    out_major,
    out_minor,
    up_all,
    down_all,
    k_major_all,
    v_major_all,
    kv_minor_all,
    qm_major,
    qm_minor,
    acc_major,
    acc_minor,
    peaks,
    totals,
    send_sem,
    recv_sem,
    local_sem,
):
    rows = q_major.shape[0]
    up_rows = up_ref.shape[0]

    def rows_of(ref, count):
        return lambda source: ref.at[pl.ds(pl.multiple_of(source * count, count), count), :]

    places = [
        rows_of(k_major_all, rows),
        rows_of(v_major_all, rows),
        rows_of(kv_minor_all, rows),
        rows_of(up_all, up_rows),
        lambda source: down_all.at[source],
    ]
    own_refs = [k_major, v_major, kv_minor, up_ref, down_ref]
    gather = Gather(sp_count, places, send_sem, recv_sem)
    own = gather.own

    barrier = pltpu.get_barrier_semaphore()
    peers = [gather.z_peer(step) for step in range(1, gather.z_count)]
    peers += [gather.y_peer(step) for step in range(1, gather.y_count)]
    for peer in peers:
        pl.semaphore_signal(
            barrier, inc=1, device_id={"sp": peer}, device_id_type=pl.DeviceIdType.MESH
        )
    pl.semaphore_wait(barrier, len(peers))

    for array in range(3):
        gather.send_z(array, own_refs[array])
    for array in range(3):
        gather.send_y(array, own_refs[array])
    for array in (3, 4):
        gather.send_z(array, own_refs[array])
    for array in (3, 4):
        gather.send_y(array, own_refs[array])
    local = []
    for slot, array in enumerate((3, 4)):
        copy = pltpu.make_async_copy(own_refs[array], places[array](own), local_sem.at[slot])
        copy.start()
        local.append(copy)

    heads = []
    for group, (head_count, key_size) in enumerate(groups):
        q_ref, qm_ref = ((q_major, qm_major), (q_minor, qm_minor))[group]
        acc_ref = (acc_major, acc_minor)[group]
        value_size = acc_ref.shape[1]
        lanes = qm_ref.shape[2]
        for head in range(head_count):
            first = head * MAPS * key_size
            lane_first = first // lanes * lanes
            block = q_ref[:, lane_first : lane_first + lanes]
            lane = lax.broadcasted_iota(jnp.int32, block.shape, 1) + lane_first
            for m in range(MAPS):
                low = first + m * key_size
                keep = (lane >= low) & (lane < low + key_size)
                picked = jnp.where(keep, block.astype(jnp.float32), 0.0).astype(block.dtype)
                qm_ref[head, m * rows : (m + 1) * rows, :] = picked
            heads.append((group, head, len(heads), lane_first, lanes, value_size, key_size))

    minor_keys = q_minor.shape[1]
    minor_first = minor_keys // 128 * 128

    def fold(key_refs, value_refs, at, diagonal):
        window = pl.ds(at, rows)
        stored = (value_refs[0][window, :], value_refs[1][window, minor_first:])
        turned = [jnp.transpose(v.astype(jnp.float32)).astype(jnp.bfloat16) for v in stored]
        turned[1] = turned[1][minor_keys - minor_first :, :]
        for group, head, index, lane_first, lanes, value_size, key_size in heads:
            qm_ref = (qm_major, qm_minor)[group]
            acc_ref = (acc_major, acc_minor)[group]
            keys = key_refs[group][window, lane_first : lane_first + lanes]
            values = turned[group][head * value_size : (head + 1) * value_size, :]
            scores = lax.dot_general(
                keys, qm_ref[head], (((1,), (1,)), ((), ())), preferred_element_type=jnp.float32
            ) * (key_size ** (-0.5) * LOG2_E)
            if diagonal:
                key_pos = lax.broadcasted_iota(jnp.int32, scores.shape, 0)
                query_pos = lax.broadcasted_iota(jnp.int32, scores.shape, 1) % rows
                visible = key_pos // SEGMENT <= query_pos // SEGMENT
                scores = jnp.where(visible, scores, NEGATIVE)
            peak = jnp.max(scores, axis=0, keepdims=True)
            if not diagonal:
                peak_old = peaks[index]
                peak = jnp.maximum(peak, peak_old)
            weights = jnp.exp2(scores - peak)
            total = jnp.sum(weights, axis=0, keepdims=True)
            sums = jnp.dot(
                values, weights.astype(jnp.bfloat16), preferred_element_type=jnp.float32
            )
            if not diagonal:
                factor = jnp.exp2(peak_old - peak)
                total = total + totals[index] * factor
                sums = sums + acc_ref[head] * factor
            peaks[index] = peak
            totals[index] = total
            acc_ref[head] = sums

    fold((k_major, kv_minor), (v_major, kv_minor), 0, True)

    for step in range(1, gather.z_count):
        for array in range(3):
            gather.pass_on(array, step)

    def earlier(block, carry):
        at = pl.multiple_of(block * rows, rows)
        fold((k_major_all, kv_minor_all), (v_major_all, kv_minor_all), at, False)
        return carry

    y_count = gather.y_count

    def same_y(z_at, carry):
        return earlier(z_at * y_count + gather.y, carry)

    def other_y(index, carry):
        z_at, place = index // (y_count - 1), lax.rem(index, y_count - 1)
        y_at = place + (place >= gather.y).astype(jnp.int32)
        return earlier(z_at * y_count + y_at, carry)

    lax.fori_loop(0, gather.z, same_y, 0)
    for array in range(3):
        gather.wait_y(array)
    lax.fori_loop(0, gather.z * (y_count - 1) + gather.y, other_y, 0)

    for group, (head_count, _) in enumerate(groups):
        acc_ref = (acc_major, acc_minor)[group]
        lam_ref = (lam_major, lam_minor)[group]
        gain_ref = (gain_major, gain_minor)[group]
        out_ref = (out_major, out_minor)[group]
        done = []
        for head in range(head_count):
            index = next(h[2] for h in heads if h[0] == group and h[1] == head)
            ratio = acc_ref[head] / totals[index]
            diff = ratio[:, :rows] - lam_ref[head] * ratio[:, rows:]
            mean = jnp.mean(diff * diff, axis=0, keepdims=True)
            done.append(diff * lax.rsqrt(mean + EPSILON) * gain_ref[...])
        out_ref[...] = jnp.transpose(jnp.concatenate(done, axis=0)).astype(out_ref.dtype)

    for step in range(1, gather.z_count):
        for array in (3, 4):
            gather.pass_on(array, step)
    for array in (3, 4):
        gather.wait_y(array)
    for copy in local:
        copy.wait()
    gather.finish()


def mixer(sp_count, *args):
    q_major, k_major, v_major, q_minor, kv_minor = args[:5]
    up_weight, down_weight = args[9:11]
    heads_major = k_major.shape[1] // (MAPS * DK_MAJOR)
    heads_minor = q_minor.shape[1] // (MAPS * DK_MINOR)
    rows = q_major.shape[0]
    size_major = v_major.shape[1] // heads_major
    width_minor = kv_minor.shape[1] - q_minor.shape[1]
    size_minor = width_minor // heads_minor
    lanes_major = min(MAPS * DK_MAJOR, q_major.shape[1])
    lanes_minor = min(128, q_minor.shape[1])
    z_count, y_count = grid_sizes(sp_count)
    sends = (z_count - 1) + (y_count - 1) * z_count
    tokens = rows * sp_count
    bf16, f32 = jnp.bfloat16, jnp.float32
    head_total = heads_major + heads_minor
    return pl.pallas_call(
        functools.partial(
            mixer_kernel, sp_count, ((heads_major, DK_MAJOR), (heads_minor, DK_MINOR))
        ),
        out_shape=(
            jax.ShapeDtypeStruct(v_major.shape, bf16),
            jax.ShapeDtypeStruct((rows, width_minor), bf16),
            jax.ShapeDtypeStruct((up_weight.shape[0] * sp_count, up_weight.shape[1]), bf16),
            jax.ShapeDtypeStruct((sp_count, *down_weight.shape), bf16),
        ),
        in_specs=[VMEM] * 5 + [SMEM] * 2 + [VMEM] * 4,
        out_specs=(VMEM, VMEM, ANY, ANY),
        scratch_shapes=[
            pltpu.VMEM((tokens, k_major.shape[1]), bf16),
            pltpu.VMEM((tokens, v_major.shape[1]), bf16),
            pltpu.VMEM((tokens, kv_minor.shape[1]), bf16),
            pltpu.VMEM((heads_major, MAPS * rows, lanes_major), bf16),
            pltpu.VMEM((heads_minor, MAPS * rows, lanes_minor), bf16),
            pltpu.VMEM((heads_major, size_major, MAPS * rows), f32),
            pltpu.VMEM((heads_minor, size_minor, MAPS * rows), f32),
            pltpu.VMEM((head_total, 1, MAPS * rows), f32),
            pltpu.VMEM((head_total, 1, MAPS * rows), f32),
            pltpu.SemaphoreType.DMA((5, sends)),
            pltpu.SemaphoreType.DMA((5, sp_count)),
            pltpu.SemaphoreType.DMA((2,)),
        ],
        compiler_params=pltpu.CompilerParams(
            collective_id=0, has_side_effects=True, vmem_limit_bytes=60 * 1024 * 1024
        ),
    )(*args)


class Exchange:
    def __init__(self, tp_count, send_sem, recv_sem):
        own = lax.axis_index("tp")
        self.x_count = tp_count // 2
        self.own, self.x, self.core = own, own // 2, lax.rem(own, 2)
        self.partner = self.x * 2 + 1 - self.core
        self.send_sem, self.recv_sem = send_sem, recv_sem

    def enter(self):
        barrier = pltpu.get_barrier_semaphore()
        peers = [self.partner] + [self.x_peer(step) for step in range(1, self.x_count)]
        for peer in peers:
            pl.semaphore_signal(
                barrier, inc=1, device_id={"tp": peer}, device_id_type=pl.DeviceIdType.MESH
            )
        pl.semaphore_wait(barrier, len(peers))

    def x_peer(self, step):
        return lax.rem(self.x + step, self.x_count) * 2 + self.core

    def copy(self, src, dst, slot, target):
        made = pltpu.make_async_remote_copy(
            src_ref=src,
            dst_ref=dst,
            send_sem=self.send_sem.at[slot],
            recv_sem=self.recv_sem.at[slot],
            device_id={"tp": target},
            device_id_type=pl.DeviceIdType.MESH,
        )
        made.start()
        return made

    def total(self, partial, pair_in, pair_sum, x_in, rows):
        def block(x_at, core):
            return pl.ds(pl.multiple_of((x_at * 2 + core) * rows, rows), rows)

        steps = list(range(1, self.x_count)) + [0]
        at = [lax.rem(self.x + step, self.x_count) for step in range(self.x_count)]
        pair = {}
        for step in steps:
            pair[step] = self.copy(
                partial.at[block(at[step], 1 - self.core), :], pair_in.at[step], step, self.partner
            )
        across = []
        for step in steps:
            pair[step].wait_recv()
            mine = partial[block(at[step], self.core), :].astype(jnp.float32)
            both = mine + pair_in[step].astype(jnp.float32)
            if step:
                pair_sum[step] = both.astype(jnp.bfloat16)
                across.append(
                    self.copy(
                        pair_sum.at[step], x_in.at[step], self.x_count + step, self.x_peer(step)
                    )
                )
        for made in across:
            made.wait_recv()
        for step in range(1, self.x_count):
            both = both + x_in[step].astype(jnp.float32)
        return both, list(pair.values()) + across


def mix_kernel(
    tp_count, partial, residual, gain, stream_ref, normed_ref, pair_in, pair_sum, x_in, held, send_sem, recv_sem
):
    exchange = Exchange(tp_count, send_sem, recv_sem)
    exchange.enter()
    rows = residual.shape[0]
    mixed, copies = exchange.total(partial, pair_in, pair_sum, x_in, rows)
    stream = residual[...].astype(jnp.float32) + mixed
    stream_ref[...] = stream
    mean = jnp.mean(stream * stream, axis=-1, keepdims=True)
    normed = (stream * lax.rsqrt(mean + EPSILON) * gain[...]).astype(jnp.bfloat16)
    held[...] = normed

    def place(index):
        return normed_ref.at[pl.ds(pl.multiple_of(index * rows, rows), rows), :]

    base, count = 2 * exchange.x_count, exchange.x_count
    sent = [exchange.copy(held, place(exchange.own), base + step, exchange.x_peer(step)) for step in range(1, count)]
    passed = [exchange.copy(held, place(exchange.own), base + count, exchange.partner)]
    normed_ref[pl.ds(pl.multiple_of(exchange.own * rows, rows), rows), :] = normed
    for step in range(1, count):
        sent[step - 1].wait_recv()
        source = exchange.x_peer(count - step)
        passed.append(
            exchange.copy(place(source), place(source), base + count + step, exchange.partner)
        )
    for made in passed:
        made.wait_recv()
    for made in copies + sent + passed:
        made.wait_send()


def sum_kernel(tp_count, partial, stream, out_ref, pair_in, pair_sum, x_in, send_sem, recv_sem):
    exchange = Exchange(tp_count, send_sem, recv_sem)
    exchange.enter()
    total, copies = exchange.total(partial, pair_in, pair_sum, x_in, stream.shape[0])
    out_ref[...] = (stream[...] + total).astype(out_ref.dtype)
    for made in copies:
        made.wait_send()


def tp_call(kernel, identity, inputs, out_shape, rows, holds):
    tp_count = lax.axis_size("tp")
    slots = (tp_count // 2, rows, inputs[0].shape[1])
    held = [pltpu.VMEM(slots[1:], jnp.bfloat16)] if holds else []
    return pl.pallas_call(
        functools.partial(kernel, tp_count),
        out_shape=out_shape,
        in_specs=[VMEM] * len(inputs),
        out_specs=jax.tree.map(lambda _: VMEM, out_shape),
        scratch_shapes=[pltpu.VMEM(slots, jnp.bfloat16)] * 3
        + held
        + [pltpu.SemaphoreType.DMA((2 * tp_count,))] * 2,
        compiler_params=pltpu.CompilerParams(
            collective_id=identity, has_side_effects=True, vmem_limit_bytes=32 * 1024 * 1024
        ),
    )(*inputs)


class Sender:
    def __init__(self, sem):
        self.sem, self.made = sem, []

    def prepare(self, src, dst, recv, target, when=None):
        copy = pltpu.make_async_remote_copy(
            src_ref=src,
            dst_ref=dst,
            send_sem=self.sem.at[len(self.made)],
            recv_sem=recv,
            device_id=target,
            device_id_type=pl.DeviceIdType.MESH,
        )
        self.made.append((when, copy))
        return lambda: run_when(when, copy.start)

    def send(self, src, dst, recv, target, when=None):
        self.prepare(src, dst, recv, target, when)()

    def finish(self):
        for when, copy in self.made:
            run_when(when, copy.wait_send)


def run_when(when, action):
    if when is None:
        action()
    else:
        pl.when(when)(lambda: action())


def layer_kernel(
    sizes,
    residual,
    q_major,
    k_major,
    v_major,
    q_minor,
    k_minor,
    v_minor,
    lam_major,
    lam_minor,
    gain_major,
    gain_minor,
    wo_major,
    wo_minor,
    mixer_gain,
    up_ref,
    down_ref,
    out_ref,
    pack,
    kv_all,
    q_in,
    qm,
    acc,
    peaks,
    totals,
    heads_out,
    cat,
    minor_in,
    wo_all,
    stream,
    normed_all,
    up_all,
    down_all,
    hidden,
    d_send,
    d_in,
    mine,
    x_send,
    x_in,
    x_keep,
    z_send,
    z_in,
    z_keep,
    send_sem,
    relay_sem,
    local_sem,
    r_y,
    r_kv,
    r_w,
    r_wo,
    r_h,
    r_g,
    r_d,
    r_x,
    r_z,
    credits,
):
    z_count, y_count, x_count = sizes
    bf16, f32 = jnp.bfloat16, jnp.float32
    own, tp = lax.axis_index("sp"), lax.axis_index("tp")
    z, y = own // y_count, lax.rem(own, y_count)
    x, c = tp // 2, lax.rem(tp, 2)
    oy, ox, oc = 1 - y, 1 - x, 1 - c
    zl = lax.rem(z, 2)
    oz = z + 1 - 2 * zl
    rows, tile = q_major.shape[0], residual.shape[0]
    width = q_minor.shape[1]
    half = width // 2
    unit = up_ref.shape[1] // UNITS
    part_size = [units * unit for units in PART_UNITS]
    part_at = [sum(part_size[:part]) for part in range(PARTS)]
    big, small = sum(part_size), sum(part_size[:-1])
    even = zl == 0
    up_rows = up_ref.shape[0]
    cols = down_ref.shape[1]

    def dev(z_at=z, y_at=y, x_at=x, c_at=c):
        return {"sp": z_at * y_count + y_at, "tp": x_at * 2 + c_at}

    def span(start, count):
        return pl.ds(pl.multiple_of(start * count, count), count)

    def arrive(place, recv):
        pltpu.make_async_remote_copy(
            src_ref=place,
            dst_ref=place,
            send_sem=send_sem.at[0],
            recv_sem=recv,
            device_id=dev(y_at=oy),
            device_id_type=pl.DeviceIdType.MESH,
        ).wait_recv()

    k_low = lax.broadcasted_iota(jnp.int32, (rows, width), 1)
    for head in range(2):
        k_part = (k_low >= head * half) & (k_low < (head + 1) * half)
        turned_v = pltpu.roll(v_minor[...].astype(f32), half, 1)
        pack[head] = jnp.where(k_part, k_minor[...].astype(f32), turned_v).astype(bf16)

    barrier = pltpu.get_barrier_semaphore()
    peers = []
    for dy in range(2):
        for dx in range(2):
            for dc in range(2):
                if dy or dx or dc:
                    peers.append(dev(y_at=oy if dy else y, x_at=ox if dx else x, c_at=oc if dc else c))
    peers += [dev(z_at=lax.rem(z + step, z_count)) for step in range(1, z_count)]
    for peer in peers:
        pl.semaphore_signal(barrier, inc=1, device_id=peer, device_id_type=pl.DeviceIdType.MESH)

    kv_all[z, 0, span(y, rows), :] = k_major[:, span(y, width)]
    kv_all[z, 1, span(y, rows), :] = v_major[:, span(y, width)]
    kv_all[z, 2, span(y, rows), :] = pack[y]
    local = []

    def weight_src(kind, z_at):
        part = kind % PARTS
        start = pl.multiple_of(lax.rem(z_at, 2) * big + part_at[part], unit) if part < PARTS - 1 else part_at[part]
        window = pl.ds(start, part_size[part])
        return up_ref.at[:, window] if kind < PARTS else down_ref.at[window, :]

    def weight_place(kind, source):
        window = pl.ds(part_at[kind % PARTS], part_size[kind % PARTS])
        return up_all.at[span(source, up_rows), window] if kind < PARTS else down_all.at[source, window, :]

    def fits(kind, z_at, when):
        if kind % PARTS < PARTS - 1:
            return when
        held = lax.rem(z_at, 2) == 0
        return held if when is None else held & when

    up_kinds, down_kinds = tuple(range(PARTS)), tuple(range(PARTS, 2 * PARTS))
    local_pairs = [
        (weight_src(kind, z), weight_place(kind, own), fits(kind, z, None)) for kind in up_kinds + down_kinds
    ]
    major_rows, minor_rows = wo_major.shape[0], wo_minor.shape[0]
    tp_count = 2 * x_count
    minor_base = tp_count * major_rows

    def wo_place(part, index):
        if part == 0:
            return wo_all.at[span(index, major_rows), :]
        return wo_all.at[pl.ds(pl.multiple_of(minor_base + index * minor_rows, minor_rows), minor_rows), :]

    for part, ref in enumerate((wo_major, wo_minor)):
        local_pairs.append((ref, wo_place(part, tp), None))
    for at, (src, dst, when) in enumerate(local_pairs):
        made = pltpu.make_async_copy(src, dst, local_sem.at[at])
        run_when(when, made.start)
        local.append((when, made))

    pl.semaphore_wait(barrier, len(peers))

    sender = Sender(send_sem)
    has_up = z < z_count - 1
    next_z = jnp.minimum(z + 1, z_count - 1)

    def kv_place(z_at, part, side):
        return kv_all.at[z_at, part, span(side, rows), :]

    for part, src in enumerate((k_major.at[:, span(oy, width)], v_major.at[:, span(oy, width)], pack.at[oy])):
        sender.send(src, kv_place(z, part, y), r_y.at[part], dev(y_at=oy))
    sender.send(q_major.at[:, span(oy, width)], q_in.at[0], r_y.at[3], dev(y_at=oy))
    sender.send(q_minor, q_in.at[1], r_y.at[4], dev(y_at=oy))
    for part, src in enumerate((k_major.at[:, span(y, width)], v_major.at[:, span(y, width)], pack.at[y])):
        sender.send(src, kv_place(z, part, y), r_kv.at[z, y, part], dev(z_at=next_z), has_up)

    def send_weight(kind, z_at, y_at, when=None):
        return sender.prepare(
            weight_src(kind, z_at),
            weight_place(kind, own),
            r_w.at[kind, own],
            dev(z_at=z_at, y_at=y_at),
            fits(kind, z_at, when),
        )

    def below(kinds, last=1, first=z_count - 1):
        return [
            send_weight(kind, jnp.maximum(z - step, 0), y, z >= step)
            for step in range(first, last - 1, -1)
            for kind in kinds
        ]

    def above(kinds, step, odd=None):
        when = z + step < z_count
        if odd is not None:
            when = when & (lax.rem(z + step, 2) == odd)
        if odd == 1:
            kinds = kinds[:-1]
        return [send_weight(kind, jnp.minimum(z + step, z_count - 1), y, when) for kind in kinds]

    def issue(starts):
        for start in starts:
            start()

    issue(below(up_kinds))
    for kind in up_kinds + down_kinds:
        send_weight(kind, z, oy)()
    for part, ref in enumerate((wo_major, wo_minor)):
        sender.send(ref, wo_place(part, tp), r_wo.at[part, tp], dev(x_at=ox))
        sender.send(ref, wo_place(part, tp), r_wo.at[part, tp], dev(c_at=oc))
    below_far, below_mid, below_near = below(down_kinds, 3), below(down_kinds, 2, 2), below(down_kinds, 1, 1)
    slow = (zl == 1) & (z > 1)
    near_up = above(up_kinds, 1)
    late_up = (zl == 0) & (z > 0)

    scales = (DK_MAJOR ** (-0.5) * LOG2_E, DK_MINOR ** (-0.5) * LOG2_E)
    lane = lax.broadcasted_iota(jnp.int32, (rows, width), 1)

    def pick(group, side, block):
        first, size = (0, DK_MAJOR) if group == 0 else (y * half, DK_MINOR)
        for m in range(MAPS):
            low = first + m * size
            keep = (lane >= low) & (lane < low + size)
            qm[group, side, m * rows : (m + 1) * rows, :] = jnp.where(keep, block.astype(f32), 0.0).astype(bf16)

    def fold(side, z_at, key_side, diagonal):
        window = span(key_side, rows)
        for group in range(2):
            keys = kv_all[z_at, 2 * group, window, :]
            stored = kv_all[z_at, 1 + group, window, :]
            values = jnp.transpose(stored.astype(f32)).astype(bf16)
            scores = lax.dot_general(
                keys, qm[group, side], (((1,), (1,)), ((), ())), preferred_element_type=f32
            ) * scales[group]
            if diagonal:
                key_pos = lax.broadcasted_iota(jnp.int32, scores.shape, 0)
                query_pos = lax.broadcasted_iota(jnp.int32, scores.shape, 1) % rows
                visible = key_pos // SEGMENT <= query_pos // SEGMENT
                scores = jnp.where(visible, scores, NEGATIVE)
            peak = jnp.max(scores, axis=0, keepdims=True)
            if not diagonal:
                peak_old = peaks[group, side]
                peak = jnp.maximum(peak, peak_old)
            weights = jnp.exp2(scores - peak)
            total = jnp.sum(weights, axis=0, keepdims=True)
            sums = jnp.dot(values, weights.astype(bf16), preferred_element_type=f32)
            if not diagonal:
                factor = jnp.exp2(peak_old - peak)
                total = total + totals[group, side] * factor
                sums = sums + acc[group, side] * factor
            peaks[group, side] = peak
            totals[group, side] = total
            acc[group, side] = sums

    pick(0, y, q_major[:, span(y, width)])
    pick(1, y, q_minor[...])
    fold(y, z, y, True)

    for part in range(3):
        arrive(kv_place(z, part, oy), r_y.at[part])
        sender.send(kv_place(z, part, oy), kv_place(z, part, oy), r_kv.at[z, oy, part], dev(z_at=next_z), has_up)

    def credit(kind, back):
        pl.semaphore_signal(
            credits.at[kind, z],
            inc=1,
            device_id=dev(z_at=jnp.maximum(z - back, 0)),
            device_id_type=pl.DeviceIdType.MESH,
        )

    def await_credit(kind, step):
        pl.semaphore_wait(credits.at[kind, jnp.minimum(z + step, z_count - 1)], 1)

    def relay_copy(z_at, side, part):
        return pltpu.make_async_remote_copy(
            src_ref=kv_place(z_at, part, side),
            dst_ref=kv_place(z_at, part, side),
            send_sem=relay_sem.at[z_at, side, part],
            recv_sem=r_kv.at[z_at, side, part],
            device_id=dev(z_at=next_z),
            device_id_type=pl.DeviceIdType.MESH,
        )

    def take(z_at, side):
        for part in range(3):
            arrive(kv_place(z_at, part, side), r_kv.at[z_at, side, part])
            run_when(has_up, relay_copy(z_at, side, part).start)

    def after_last():
        run_when(zl == 1, lambda: issue(near_up))
        for back in range(2, z_count):
            run_when(z >= back, lambda: credit(0, back))

        @pl.when(jnp.logical_not(slow))
        def _():
            issue(below_far + below_mid + below_near)

    for part in range(2):
        arrive(q_in.at[part], r_y.at[3 + part])
        pick(part, oy, q_in[part])

    pl.when(z == 0)(lambda: issue(near_up))

    @pl.when(z > 0)
    def _():
        for side in range(2):
            take(z - 1, side)

    pl.when(z == 1)(after_last)
    fold(oy, z, oy, True)
    fold(1, z, 0, False)

    def earlier(index, carry):
        z_at, key_side = z - 1 - index // 2, lax.rem(index, 2)
        pl.when(index > 1)(lambda: take(z_at, key_side))
        pl.when((index == 2 * z - 1) & (z > 1))(after_last)
        pl.when((index == 2 * z - 4) & slow)(lambda: issue(below_near))
        pl.when((index == 2 * z - 2) & slow)(lambda: issue(below_far))

        def inner(side, carry):
            fold(side, z_at, key_side, False)
            return carry

        lax.fori_loop(0, 2, inner, 0)
        return carry

    lax.fori_loop(0, 2 * z, earlier, 0)

    value_row = lax.broadcasted_iota(jnp.int32, (width, rows), 0)
    value_keep = (value_row >= oy * half) & (value_row < (oy + 1) * half)
    gains = (gain_major[...], gain_minor[...])
    lams = (lam_major[y], lam_minor[y])

    def close(side, carry):
        for group in range(2):
            ratio = acc[group, side] / totals[group, side]
            diff = ratio[:, :rows] - lams[group] * ratio[:, rows:]
            if group == 1:
                diff = jnp.where(value_keep, diff, 0.0)
            count = width if group == 0 else half
            mean = jnp.sum(diff * diff, axis=0, keepdims=True) * (1.0 / count)
            done = jnp.transpose(diff * lax.rsqrt(mean + EPSILON)) * gains[group]
            heads_out[group, span(side, rows), :] = done.astype(bf16)
        return carry

    lax.fori_loop(0, 2, close, 0)

    place = tp * y_count + y

    def token_span(y_at, x_at, c_at):
        return span(y_at * (rows // tile) + x_at * 2 + c_at, tile)

    def head_place(group, index):
        return cat.at[:, span(index, width)] if group == 0 else minor_in.at[index]

    for dy, dx, dc in ((1, 1, 1), (1, 1, 0), (1, 0, 1), (1, 0, 0), (0, 1, 1), (0, 1, 0), (0, 0, 1)):
        y_at, x_at, c_at = oy if dy else y, ox if dx else x, oc if dc else c
        for group in range(2):
            sender.send(
                heads_out.at[group, token_span(y_at, x_at, c_at), :],
                head_place(group, place),
                r_h.at[group, place],
                dev(y_at=y_at, x_at=x_at, c_at=c_at),
            )
    cat[:, span(place, width)] = heads_out[0, token_span(y, x, c), :]
    minor_in[place] = heads_out[1, token_span(y, x, c), :]

    def take_weight(kind, source):
        run_when(fits(kind, z, None), lambda: arrive(weight_place(kind, source), r_w.at[kind, source]))

    def pass_weight(kind, z_at, when):
        source = z_at * y_count + y
        when = fits(kind, z, when)
        run_when(when, lambda: arrive(weight_place(kind, source), r_w.at[kind, source]))
        sender.send(weight_place(kind, source), weight_place(kind, source), r_w.at[kind, source], dev(y_at=oy), when)

    for step in range(1, z_count):
        for kind in up_kinds:
            pass_weight(kind, lax.rem(z + step, z_count), z + step < z_count)
    for step in range(2, z_count):
        run_when(z + step < z_count, lambda: await_credit(0, step))
        issue(above(up_kinds, step))

    for when, made in local:
        run_when(when, made.wait)
    for part in range(2):
        index = ox * 2 + c
        arrive(wo_place(part, index), r_wo.at[part, index])
        sender.send(wo_place(part, index), wo_place(part, index), r_wo.at[part, index], dev(c_at=oc))
    for index in (x * 2 + oc, ox * 2 + oc):
        for part in range(2):
            arrive(wo_place(part, index), r_wo.at[part, index])
    for dy, dx, dc in ((0, 0, 1), (0, 1, 0), (0, 1, 1), (1, 0, 0), (1, 0, 1), (1, 1, 0), (1, 1, 1)):
        index = ((ox if dx else x) * 2 + (oc if dc else c)) * y_count + (oy if dy else y)
        for group in range(2):
            arrive(head_place(group, index), r_h.at[group, index])
    major_width = tp_count * y_count * width
    for index in range(tp_count):
        both = minor_in[index * y_count].astype(f32) + minor_in[index * y_count + 1].astype(f32)
        cat[:, major_width + index * width : major_width + (index + 1) * width] = pltpu.roll(both, half, 1).astype(bf16)

    model = residual.shape[1]
    step_cols = 256

    def project(index, carry):
        window = span(index, step_cols)
        mixed = jnp.dot(cat[...], wo_all[:, window], preferred_element_type=f32)
        added = residual[:, window].astype(f32) + mixed
        stream[:, window] = added
        return carry + jnp.sum(added * added, axis=1, keepdims=True)

    square = lax.fori_loop(0, model // step_cols, project, jnp.zeros((tile, 1), f32))
    norm = lax.rsqrt(square * (1.0 / model) + EPSILON)

    def slot(c_at, x_at, zl_at):
        return c_at * (2 * x_count) + x_at * 2 + zl_at

    def rows_at(index):
        return normed_all.at[span(index, tile), :]

    mine_at = slot(c, x, zl)
    normed_all[span(mine_at, tile), :] = (stream[...] * norm * mixer_gain[...]).astype(bf16)

    def share(index, target):
        sender.send(rows_at(index), rows_at(index), r_g.at[index], target)

    partner, x_peer, z_peer = dev(c_at=oc), dev(x_at=ox), dev(z_at=oz)
    share(mine_at, z_peer)
    share(mine_at, x_peer)
    share(mine_at, partner)
    run_when(late_up, lambda: issue(near_up))
    run_when(slow, lambda: issue(below_mid))
    issue(above(down_kinds, 1))
    for step in range(1, z_count - 1):
        for kind in up_kinds:
            pass_weight(kind, lax.rem(z + step, z_count), z + step >= z_count)
    for step in range(z_count - 1, 0, -1):
        for kind in down_kinds:
            pass_weight(kind, lax.rem(z + step, z_count), even & (z + step < z_count))
    index = slot(c, ox, zl)
    arrive(rows_at(index), r_g.at[index])
    share(index, partner)
    for step in range(2, z_count):
        issue(above(down_kinds, step, 0))
    index = slot(c, x, 1 - zl)
    arrive(rows_at(index), r_g.at[index])
    share(index, x_peer)
    share(index, partner)
    for kind in up_kinds:
        pass_weight(kind, lax.rem(z + z_count - 1, z_count), z > 0)
    for back in range(2, z_count):
        run_when((z >= back) & (zl == 1), lambda: credit(1, back))
    for step in range(z_count - 1, 0, -1):
        for kind in down_kinds[:-1]:
            pass_weight(kind, lax.rem(z + step, z_count), (zl == 1) & ((z + step < z_count) | (z == 1)))
    for step in range(2, z_count):
        run_when((z + step < z_count) & (lax.rem(z + step, 2) == 1), lambda: await_credit(1, step))
        issue(above(down_kinds, step, 1))
    index = slot(c, ox, 1 - zl)
    arrive(rows_at(index), r_g.at[index])
    share(index, partner)
    for step in range(z_count):
        source = lax.rem(z + step, z_count) * y_count + oy
        for kind in up_kinds:
            take_weight(kind, source)

    group_rows = 2 * x_count * tile
    hid_cols = 256

    def expand(side):
        def one(index, carry):
            window = span(index, hid_cols)
            pre = jnp.dot(
                normed_all[span(side, group_rows), :], up_all[:, window], preferred_element_type=f32
            )
            hidden[span(side, group_rows), window] = jnp.square(jnp.maximum(pre, 0.0)).astype(bf16)
            return carry

        full = jnp.where(even, big // hid_cols, small // hid_cols)
        lax.fori_loop(0, full, one, 0)
        rest = big % hid_cols
        assert rest == small % hid_cols
        if rest:
            window = pl.ds(pl.multiple_of(full * hid_cols, hid_cols), rest)
            pre = jnp.dot(
                normed_all[span(side, group_rows), :], up_all[:, window], preferred_element_type=f32
            )
            hidden[span(side, group_rows), window] = jnp.square(jnp.maximum(pre, 0.0)).astype(bf16)

    expand(c)
    for x_at in range(x_count):
        for zl_at in range(2):
            index = slot(oc, x_at, zl_at)
            arrive(rows_at(index), r_g.at[index])
    expand(oc)

    for step in range(1, z_count):
        for kind in down_kinds:
            pass_weight(kind, lax.rem(z + step, z_count), even & (z + step >= z_count))

    x_rows = 2 * tile
    blocks = []

    def stage_x(t):
        arrive(d_in.at[t], r_d.at[t])
        x_send[t] = (mine[t, span(ox, x_rows), :] + d_in[t, span(ox, x_rows), :].astype(f32)).astype(bf16)
        sender.send(x_send.at[t], x_in.at[t], r_x.at[t], x_peer)
        x_keep[t] = mine[t, span(x, x_rows), :] + d_in[t, span(x, x_rows), :].astype(f32)

    def stage_z(t):
        arrive(x_in.at[t], r_x.at[t])
        other, same = span(1 - zl, tile), span(zl, tile)
        z_send[t] = (x_keep[t, other, :] + x_in[t, other, :].astype(f32)).astype(bf16)
        sender.send(z_send.at[t], z_in.at[blocks[t]], r_z.at[blocks[t]], z_peer)
        z_keep[t] = x_keep[t, same, :] + x_in[t, same, :].astype(f32)

    def stage_end(t):
        arrive(z_in.at[blocks[t]], r_z.at[blocks[t]])
        window = span(blocks[t], cols)
        total = stream[:, window] + (z_keep[t] + z_in[blocks[t]].astype(f32))
        out_ref[:, window] = total.astype(out_ref.dtype)

    def advance(t):
        for stage, lag in ((stage_x, 1), (stage_z, 4), (stage_end, 7)):
            if 0 <= t - lag < z_count * y_count:
                stage(t - lag)

    lower = [0, *range(z_count - 1, 0, -1)]
    upper = [*range(1, z_count - 1), 0, z_count - 1]

    def z_of(block):
        return lax.rem(z - zl + jnp.where(z < 2, lower[block], upper[block]), z_count)

    count = z_count
    order = [(0, 0), (0, 1), (1, 0)]
    for block in range(2, count):
        order += [(block, 0), (block - 1, 1)]
    order.append((count - 1, 1))
    for t, (block, side) in enumerate(order):
        source = z_of(block) * y_count + (oy if side else y)
        blocks.append(source)
        for ahead, kind in ([(1, PARTS)] if t == 0 else []) + [
            (block, kind) for kind in down_kinds[:-1] if block and not side and (block > 1 or kind > PARTS)
        ]:
            pass_weight(kind, z_of(ahead), slow)
        if side:
            for kind in down_kinds:
                take_weight(kind, source)
        start = sender.prepare(d_send.at[t], d_in.at[t], r_d.at[t], partner)

        def multiply(depth):
            block = down_all[source, :depth, :]
            sent = jnp.dot(hidden[span(oc, group_rows), :depth], block, preferred_element_type=f32)
            d_send[t] = sent.astype(bf16)
            start()
            mine[t] = jnp.dot(hidden[span(c, group_rows), :depth], block, preferred_element_type=f32)

        pl.when(even)(lambda: multiply(big))
        pl.when(jnp.logical_not(even))(lambda: multiply(small))
        advance(t)
    for t in range(z_count * y_count, z_count * y_count + 7):
        advance(t)

    sender.finish()
    for step in range(1, z_count):
        for side in range(2):
            for part in range(3):
                copy = relay_copy(jnp.maximum(z - step, 0), side, part)
                run_when((z >= step) & has_up, copy.wait_send)


def fused(sp_count, tp_count, args):
    residual, q_major, _, v_major, q_minor = args[:5]
    wo_major, wo_minor, _, up_weight, down_weight = args[11:16]
    z_count, y_count = grid_sizes(sp_count)
    x_count = tp_count // 2
    rows, tile, width = q_major.shape[0], residual.shape[0], q_minor.shape[1]
    model = residual.shape[1]
    hid = up_weight.shape[1] // UNITS * sum(PART_UNITS)
    cols = down_weight.shape[1]
    features = tp_count * (wo_major.shape[0] + wo_minor.shape[0])
    group_rows = 2 * x_count * tile
    steps = sp_count
    bf16, f32 = jnp.bfloat16, jnp.float32
    dma = pltpu.SemaphoreType.DMA
    sends = 192
    hbm = pl.BlockSpec(memory_space=pltpu.HBM)
    return pl.pallas_call(
        functools.partial(layer_kernel, (z_count, y_count, x_count)),
        out_shape=jax.ShapeDtypeStruct(residual.shape, residual.dtype),
        in_specs=[VMEM] * 7 + [SMEM] * 2 + [VMEM] * 2 + [hbm] * 2 + [VMEM] + [hbm] * 2,
        out_specs=VMEM,
        scratch_shapes=[
            pltpu.VMEM((2, rows, width), bf16),
            pltpu.VMEM((z_count, 3, y_count * rows, width), bf16),
            pltpu.VMEM((2, rows, width), bf16),
            pltpu.VMEM((2, 2, MAPS * rows, width), bf16),
            pltpu.VMEM((2, 2, width, MAPS * rows), f32),
            pltpu.VMEM((2, 2, 1, MAPS * rows), f32),
            pltpu.VMEM((2, 2, 1, MAPS * rows), f32),
            pltpu.VMEM((2, y_count * rows, width), bf16),
            pltpu.VMEM((tile, features), bf16),
            pltpu.VMEM((tp_count * y_count, tile, width), bf16),
            pltpu.VMEM((features, model), bf16),
            pltpu.VMEM((tile, model), f32),
            pltpu.VMEM((2 * group_rows, model), bf16),
            pltpu.VMEM((model, hid), bf16),
            pltpu.VMEM((sp_count, hid, cols), bf16),
            pltpu.VMEM((2 * group_rows, hid), bf16),
            pltpu.VMEM((steps, group_rows, cols), bf16),
            pltpu.VMEM((steps, group_rows, cols), bf16),
            pltpu.VMEM((steps, group_rows, cols), f32),
            pltpu.VMEM((steps, 2 * tile, cols), bf16),
            pltpu.VMEM((steps, 2 * tile, cols), bf16),
            pltpu.VMEM((steps, 2 * tile, cols), f32),
            pltpu.VMEM((steps, tile, cols), bf16),
            pltpu.VMEM((steps, tile, cols), bf16),
            pltpu.VMEM((steps, tile, cols), f32),
            dma((sends,)),
            dma((z_count, 2, 3)),
            dma((2 * PARTS + 2,)),
            dma((5,)),
            dma((z_count, 2, 3)),
            dma((2 * PARTS, sp_count)),
            dma((2, tp_count)),
            dma((2, tp_count * y_count)),
            dma((2 * group_rows // tile,)),
            dma((steps,)),
            dma((steps,)),
            dma((steps,)),
            pltpu.SemaphoreType.REGULAR((2, z_count)),
        ],
        compiler_params=pltpu.CompilerParams(
            collective_id=0, has_side_effects=True, vmem_limit_bytes=63 * 1024 * 1024
        ),
    )(*args)


def fits_fused(sp_count, tp_count, args):
    q_major, k_major, v_major, q_minor, k_minor, v_minor = args[1:7]
    z_count, y_count = grid_sizes(sp_count)
    width = q_minor.shape[1]
    return (
        y_count == 2
        and tp_count == 4
        and z_count % 2 == 0
        and width == 2 * MAPS * DK_MINOR
        and width == MAPS * DK_MAJOR
        and width % 128 == 0
        and args[14].shape[1] % (UNITS * 128) == 0
        and v_minor.shape[1] == width
        and q_major.shape[1] == v_major.shape[1] == 2 * width
    )


def body(
    residual,
    query_major,
    keys_major,
    values_major,
    query_minor,
    keys_minor,
    values_minor,
    lambda_major,
    lambda_minor,
    gain_major,
    gain_minor,
    output_major,
    output_minor,
    mixer_gain,
    up_weight,
    down_weight,
):
    sp_count, tp_count = lax.axis_size("sp"), lax.axis_size("tp")
    args = (
        residual,
        query_major,
        keys_major,
        values_major,
        query_minor,
        keys_minor,
        values_minor,
        lambda_major,
        lambda_minor,
        gain_major[None, :],
        jnp.tile(gain_minor, 2)[None, :],
        output_major,
        output_minor,
        mixer_gain[None, :],
        up_weight,
        down_weight,
    )
    if fits_fused(sp_count, tp_count, args):
        return fused(sp_count, tp_count, args)
    out_major, out_minor, up_full, down_full = mixer(
        lax.axis_size("sp"),
        query_major,
        keys_major,
        values_major,
        query_minor,
        jnp.concatenate([keys_minor, values_minor], axis=1),
        lambda_major,
        lambda_minor,
        gain_major[:, None],
        gain_minor[:, None],
        up_weight,
        down_weight,
    )
    partial_sum = jnp.dot(out_major, output_major, preferred_element_type=jnp.float32)
    partial_sum = partial_sum + jnp.dot(out_minor, output_minor, preferred_element_type=jnp.float32)
    rows = residual.shape[0]
    stream, normed_all = tp_call(
        mix_kernel,
        1,
        (partial_sum.astype(jnp.bfloat16), residual, mixer_gain[None, :]),
        (
            jax.ShapeDtypeStruct(residual.shape, jnp.float32),
            jax.ShapeDtypeStruct(partial_sum.shape, jnp.bfloat16),
        ),
        rows,
        True,
    )
    pre_act = jnp.dot(
        normed_all,
        up_full,
        preferred_element_type=jnp.float32,
    )
    hidden = jnp.square(jax.nn.relu(pre_act)).astype(jnp.bfloat16)
    down_part = jnp.einsum("th,shd->tsd", hidden, down_full, preferred_element_type=jnp.float32)
    down_part = down_part.astype(jnp.bfloat16).reshape(partial_sum.shape)
    return tp_call(
        sum_kernel,
        2,
        (down_part, stream),
        jax.ShapeDtypeStruct(residual.shape, residual.dtype),
        rows,
        False,
    )


def solution(mesh):
    return jax.shard_map(
        body,
        mesh=mesh,
        in_specs=(
            P(("sp", "tp"), None),
            P("sp", "tp"),
            P("sp", "tp"),
            P("sp", "tp"),
            P("sp", "tp"),
            P("sp", "tp"),
            P("sp", "tp"),
            P("tp"),
            P("tp"),
            P(),
            P(),
            P("tp", None),
            P("tp", None),
            P(),
            P("sp", "tp"),
            P("tp", "sp"),
        ),
        out_specs=P(("sp", "tp"), None),
        check_vma=False,
    )
```

```python
import functools

import jax
import jax.numpy as jnp
from jax import lax
from jax.experimental import pallas as pl
from jax.experimental.pallas import tpu as pltpu
from jax.sharding import PartitionSpec as P

DK_MAJOR = 64
DK_MINOR = 32
SEGMENT = 64
MAPS = 2
PART_UNITS = (4, 3, 2)
PARTS = len(PART_UNITS)
UNITS = 16

EPSILON = 1e-06
NEGATIVE = -1e30
LOG2_E = 1.4426950408889634
ANY = pl.BlockSpec(memory_space=pl.ANY)
VMEM = pl.BlockSpec(memory_space=pltpu.VMEM)
SMEM = pl.BlockSpec(memory_space=pltpu.SMEM)


def grid_sizes(sp_count):
    y_count = 1 << ((sp_count.bit_length() - 1) // 2)
    return sp_count // y_count, y_count


class Gather:
    def __init__(self, sp_count, places, send_sem, recv_sem):
        self.z_count, self.y_count = grid_sizes(sp_count)
        own = lax.axis_index("sp")
        self.own, self.z, self.y = own, own // self.y_count, lax.rem(own, self.y_count)
        self.places, self.send_sem, self.recv_sem = places, send_sem, recv_sem
        self.copies = []

    def z_peer(self, step):
        return lax.rem(self.z + step, self.z_count) * self.y_count + self.y

    def y_peer(self, step):
        return self.z * self.y_count + lax.rem(self.y + step, self.y_count)

    def send(self, array, source, src_ref, target):
        copy = pltpu.make_async_remote_copy(
            src_ref=src_ref,
            dst_ref=self.places[array](source),
            send_sem=self.send_sem.at[array, len([c for c in self.copies if c[0] == array])],
            recv_sem=self.recv_sem.at[array, source],
            device_id={"sp": target},
            device_id_type=pl.DeviceIdType.MESH,
        )
        copy.start()
        self.copies.append((array, copy))

    def wait_block(self, array, source):
        place = self.places[array](source)
        pltpu.make_async_remote_copy(
            src_ref=place,
            dst_ref=place,
            send_sem=self.send_sem.at[array, 0],
            recv_sem=self.recv_sem.at[array, source],
            device_id={"sp": self.y_peer(1)},
            device_id_type=pl.DeviceIdType.MESH,
        ).wait_recv()

    def send_z(self, array, src_ref):
        for step in range(1, self.z_count):
            self.send(array, self.own, src_ref, self.z_peer(step))

    def send_y(self, array, src_ref):
        for step in range(1, self.y_count):
            self.send(array, self.own, src_ref, self.y_peer(step))

    def pass_on(self, array, step):
        source = self.z_peer(self.z_count - step)
        self.wait_block(array, source)
        for y_step in range(1, self.y_count):
            self.send(array, source, self.places[array](source), self.y_peer(y_step))

    def wait_y(self, array):
        for y_step in range(1, self.y_count):
            for z_step in range(self.z_count):
                z_at = lax.rem(self.z + z_step, self.z_count)
                self.wait_block(array, z_at * self.y_count + lax.rem(self.y + y_step, self.y_count))

    def finish(self):
        for _, copy in self.copies:
            copy.wait_send()


def mixer_kernel(
    sp_count,
    groups,
    q_major,
    k_major,
    v_major,
    q_minor,
    kv_minor,
    lam_major,
    lam_minor,
    gain_major,
    gain_minor,
    up_ref,
    down_ref,
    out_major,
    out_minor,
    up_all,
    down_all,
    k_major_all,
    v_major_all,
    kv_minor_all,
    qm_major,
    qm_minor,
    acc_major,
    acc_minor,
    peaks,
    totals,
    send_sem,
    recv_sem,
    local_sem,
):
    rows = q_major.shape[0]
    up_rows = up_ref.shape[0]

    def rows_of(ref, count):
        return lambda source: ref.at[pl.ds(pl.multiple_of(source * count, count), count), :]

    places = [
        rows_of(k_major_all, rows),
        rows_of(v_major_all, rows),
        rows_of(kv_minor_all, rows),
        rows_of(up_all, up_rows),
        lambda source: down_all.at[source],
    ]
    own_refs = [k_major, v_major, kv_minor, up_ref, down_ref]
    gather = Gather(sp_count, places, send_sem, recv_sem)
    own = gather.own

    barrier = pltpu.get_barrier_semaphore()
    peers = [gather.z_peer(step) for step in range(1, gather.z_count)]
    peers += [gather.y_peer(step) for step in range(1, gather.y_count)]
    for peer in peers:
        pl.semaphore_signal(
            barrier, inc=1, device_id={"sp": peer}, device_id_type=pl.DeviceIdType.MESH
        )
    pl.semaphore_wait(barrier, len(peers))

    for array in range(3):
        gather.send_z(array, own_refs[array])
    for array in range(3):
        gather.send_y(array, own_refs[array])
    for array in (3, 4):
        gather.send_z(array, own_refs[array])
    for array in (3, 4):
        gather.send_y(array, own_refs[array])
    local = []
    for slot, array in enumerate((3, 4)):
        copy = pltpu.make_async_copy(own_refs[array], places[array](own), local_sem.at[slot])
        copy.start()
        local.append(copy)

    heads = []
    for group, (head_count, key_size) in enumerate(groups):
        q_ref, qm_ref = ((q_major, qm_major), (q_minor, qm_minor))[group]
        acc_ref = (acc_major, acc_minor)[group]
        value_size = acc_ref.shape[1]
        lanes = qm_ref.shape[2]
        for head in range(head_count):
            first = head * MAPS * key_size
            lane_first = first // lanes * lanes
            block = q_ref[:, lane_first : lane_first + lanes]
            lane = lax.broadcasted_iota(jnp.int32, block.shape, 1) + lane_first
            for m in range(MAPS):
                low = first + m * key_size
                keep = (lane >= low) & (lane < low + key_size)
                picked = jnp.where(keep, block.astype(jnp.float32), 0.0).astype(block.dtype)
                qm_ref[head, m * rows : (m + 1) * rows, :] = picked
            heads.append((group, head, len(heads), lane_first, lanes, value_size, key_size))

    minor_keys = q_minor.shape[1]
    minor_first = minor_keys // 128 * 128

    def fold(key_refs, value_refs, at, diagonal):
        window = pl.ds(at, rows)
        stored = (value_refs[0][window, :], value_refs[1][window, minor_first:])
        turned = [jnp.transpose(v.astype(jnp.float32)).astype(jnp.bfloat16) for v in stored]
        turned[1] = turned[1][minor_keys - minor_first :, :]
        for group, head, index, lane_first, lanes, value_size, key_size in heads:
            qm_ref = (qm_major, qm_minor)[group]
            acc_ref = (acc_major, acc_minor)[group]
            keys = key_refs[group][window, lane_first : lane_first + lanes]
            values = turned[group][head * value_size : (head + 1) * value_size, :]
            scores = lax.dot_general(
                keys, qm_ref[head], (((1,), (1,)), ((), ())), preferred_element_type=jnp.float32
            ) * (key_size ** (-0.5) * LOG2_E)
            if diagonal:
                key_pos = lax.broadcasted_iota(jnp.int32, scores.shape, 0)
                query_pos = lax.broadcasted_iota(jnp.int32, scores.shape, 1) % rows
                visible = key_pos // SEGMENT <= query_pos // SEGMENT
                scores = jnp.where(visible, scores, NEGATIVE)
            peak = jnp.max(scores, axis=0, keepdims=True)
            if not diagonal:
                peak_old = peaks[index]
                peak = jnp.maximum(peak, peak_old)
            weights = jnp.exp2(scores - peak)
            total = jnp.sum(weights, axis=0, keepdims=True)
            sums = jnp.dot(
                values, weights.astype(jnp.bfloat16), preferred_element_type=jnp.float32
            )
            if not diagonal:
                factor = jnp.exp2(peak_old - peak)
                total = total + totals[index] * factor
                sums = sums + acc_ref[head] * factor
            peaks[index] = peak
            totals[index] = total
            acc_ref[head] = sums

    fold((k_major, kv_minor), (v_major, kv_minor), 0, True)

    for step in range(1, gather.z_count):
        for array in range(3):
            gather.pass_on(array, step)

    def earlier(block, carry):
        at = pl.multiple_of(block * rows, rows)
        fold((k_major_all, kv_minor_all), (v_major_all, kv_minor_all), at, False)
        return carry

    y_count = gather.y_count

    def same_y(z_at, carry):
        return earlier(z_at * y_count + gather.y, carry)

    def other_y(index, carry):
        z_at, place = index // (y_count - 1), lax.rem(index, y_count - 1)
        y_at = place + (place >= gather.y).astype(jnp.int32)
        return earlier(z_at * y_count + y_at, carry)

    lax.fori_loop(0, gather.z, same_y, 0)
    for array in range(3):
        gather.wait_y(array)
    lax.fori_loop(0, gather.z * (y_count - 1) + gather.y, other_y, 0)

    for group, (head_count, _) in enumerate(groups):
        acc_ref = (acc_major, acc_minor)[group]
        lam_ref = (lam_major, lam_minor)[group]
        gain_ref = (gain_major, gain_minor)[group]
        out_ref = (out_major, out_minor)[group]
        done = []
        for head in range(head_count):
            index = next(h[2] for h in heads if h[0] == group and h[1] == head)
            ratio = acc_ref[head] / totals[index]
            diff = ratio[:, :rows] - lam_ref[head] * ratio[:, rows:]
            mean = jnp.mean(diff * diff, axis=0, keepdims=True)
            done.append(diff * lax.rsqrt(mean + EPSILON) * gain_ref[...])
        out_ref[...] = jnp.transpose(jnp.concatenate(done, axis=0)).astype(out_ref.dtype)

    for step in range(1, gather.z_count):
        for array in (3, 4):
            gather.pass_on(array, step)
    for array in (3, 4):
        gather.wait_y(array)
    for copy in local:
        copy.wait()
    gather.finish()


def mixer(sp_count, *args):
    q_major, k_major, v_major, q_minor, kv_minor = args[:5]
    up_weight, down_weight = args[9:11]
    heads_major = k_major.shape[1] // (MAPS * DK_MAJOR)
    heads_minor = q_minor.shape[1] // (MAPS * DK_MINOR)
    rows = q_major.shape[0]
    size_major = v_major.shape[1] // heads_major
    width_minor = kv_minor.shape[1] - q_minor.shape[1]
    size_minor = width_minor // heads_minor
    lanes_major = min(MAPS * DK_MAJOR, q_major.shape[1])
    lanes_minor = min(128, q_minor.shape[1])
    z_count, y_count = grid_sizes(sp_count)
    sends = (z_count - 1) + (y_count - 1) * z_count
    tokens = rows * sp_count
    bf16, f32 = jnp.bfloat16, jnp.float32
    head_total = heads_major + heads_minor
    return pl.pallas_call(
        functools.partial(
            mixer_kernel, sp_count, ((heads_major, DK_MAJOR), (heads_minor, DK_MINOR))
        ),
        out_shape=(
            jax.ShapeDtypeStruct(v_major.shape, bf16),
            jax.ShapeDtypeStruct((rows, width_minor), bf16),
            jax.ShapeDtypeStruct((up_weight.shape[0] * sp_count, up_weight.shape[1]), bf16),
            jax.ShapeDtypeStruct((sp_count, *down_weight.shape), bf16),
        ),
        in_specs=[VMEM] * 5 + [SMEM] * 2 + [VMEM] * 4,
        out_specs=(VMEM, VMEM, ANY, ANY),
        scratch_shapes=[
            pltpu.VMEM((tokens, k_major.shape[1]), bf16),
            pltpu.VMEM((tokens, v_major.shape[1]), bf16),
            pltpu.VMEM((tokens, kv_minor.shape[1]), bf16),
            pltpu.VMEM((heads_major, MAPS * rows, lanes_major), bf16),
            pltpu.VMEM((heads_minor, MAPS * rows, lanes_minor), bf16),
            pltpu.VMEM((heads_major, size_major, MAPS * rows), f32),
            pltpu.VMEM((heads_minor, size_minor, MAPS * rows), f32),
            pltpu.VMEM((head_total, 1, MAPS * rows), f32),
            pltpu.VMEM((head_total, 1, MAPS * rows), f32),
            pltpu.SemaphoreType.DMA((5, sends)),
            pltpu.SemaphoreType.DMA((5, sp_count)),
            pltpu.SemaphoreType.DMA((2,)),
        ],
        compiler_params=pltpu.CompilerParams(
            collective_id=0, has_side_effects=True, vmem_limit_bytes=60 * 1024 * 1024
        ),
    )(*args)


class Exchange:
    def __init__(self, tp_count, send_sem, recv_sem):
        own = lax.axis_index("tp")
        self.x_count = tp_count // 2
        self.own, self.x, self.core = own, own // 2, lax.rem(own, 2)
        self.partner = self.x * 2 + 1 - self.core
        self.send_sem, self.recv_sem = send_sem, recv_sem

    def enter(self):
        barrier = pltpu.get_barrier_semaphore()
        peers = [self.partner] + [self.x_peer(step) for step in range(1, self.x_count)]
        for peer in peers:
            pl.semaphore_signal(
                barrier, inc=1, device_id={"tp": peer}, device_id_type=pl.DeviceIdType.MESH
            )
        pl.semaphore_wait(barrier, len(peers))

    def x_peer(self, step):
        return lax.rem(self.x + step, self.x_count) * 2 + self.core

    def copy(self, src, dst, slot, target):
        made = pltpu.make_async_remote_copy(
            src_ref=src,
            dst_ref=dst,
            send_sem=self.send_sem.at[slot],
            recv_sem=self.recv_sem.at[slot],
            device_id={"tp": target},
            device_id_type=pl.DeviceIdType.MESH,
        )
        made.start()
        return made

    def total(self, partial, pair_in, pair_sum, x_in, rows):
        def block(x_at, core):
            return pl.ds(pl.multiple_of((x_at * 2 + core) * rows, rows), rows)

        steps = list(range(1, self.x_count)) + [0]
        at = [lax.rem(self.x + step, self.x_count) for step in range(self.x_count)]
        pair = {}
        for step in steps:
            pair[step] = self.copy(
                partial.at[block(at[step], 1 - self.core), :], pair_in.at[step], step, self.partner
            )
        across = []
        for step in steps:
            pair[step].wait_recv()
            mine = partial[block(at[step], self.core), :].astype(jnp.float32)
            both = mine + pair_in[step].astype(jnp.float32)
            if step:
                pair_sum[step] = both.astype(jnp.bfloat16)
                across.append(
                    self.copy(
                        pair_sum.at[step], x_in.at[step], self.x_count + step, self.x_peer(step)
                    )
                )
        for made in across:
            made.wait_recv()
        for step in range(1, self.x_count):
            both = both + x_in[step].astype(jnp.float32)
        return both, list(pair.values()) + across


def mix_kernel(
    tp_count, partial, residual, gain, stream_ref, normed_ref, pair_in, pair_sum, x_in, held, send_sem, recv_sem
):
    exchange = Exchange(tp_count, send_sem, recv_sem)
    exchange.enter()
    rows = residual.shape[0]
    mixed, copies = exchange.total(partial, pair_in, pair_sum, x_in, rows)
    stream = residual[...].astype(jnp.float32) + mixed
    stream_ref[...] = stream
    mean = jnp.mean(stream * stream, axis=-1, keepdims=True)
    normed = (stream * lax.rsqrt(mean + EPSILON) * gain[...]).astype(jnp.bfloat16)
    held[...] = normed

    def place(index):
        return normed_ref.at[pl.ds(pl.multiple_of(index * rows, rows), rows), :]

    base, count = 2 * exchange.x_count, exchange.x_count
    sent = [exchange.copy(held, place(exchange.own), base + step, exchange.x_peer(step)) for step in range(1, count)]
    passed = [exchange.copy(held, place(exchange.own), base + count, exchange.partner)]
    normed_ref[pl.ds(pl.multiple_of(exchange.own * rows, rows), rows), :] = normed
    for step in range(1, count):
        sent[step - 1].wait_recv()
        source = exchange.x_peer(count - step)
        passed.append(
            exchange.copy(place(source), place(source), base + count + step, exchange.partner)
        )
    for made in passed:
        made.wait_recv()
    for made in copies + sent + passed:
        made.wait_send()


def sum_kernel(tp_count, partial, stream, out_ref, pair_in, pair_sum, x_in, send_sem, recv_sem):
    exchange = Exchange(tp_count, send_sem, recv_sem)
    exchange.enter()
    total, copies = exchange.total(partial, pair_in, pair_sum, x_in, stream.shape[0])
    out_ref[...] = (stream[...] + total).astype(out_ref.dtype)
    for made in copies:
        made.wait_send()


def tp_call(kernel, identity, inputs, out_shape, rows, holds):
    tp_count = lax.axis_size("tp")
    slots = (tp_count // 2, rows, inputs[0].shape[1])
    held = [pltpu.VMEM(slots[1:], jnp.bfloat16)] if holds else []
    return pl.pallas_call(
        functools.partial(kernel, tp_count),
        out_shape=out_shape,
        in_specs=[VMEM] * len(inputs),
        out_specs=jax.tree.map(lambda _: VMEM, out_shape),
        scratch_shapes=[pltpu.VMEM(slots, jnp.bfloat16)] * 3
        + held
        + [pltpu.SemaphoreType.DMA((2 * tp_count,))] * 2,
        compiler_params=pltpu.CompilerParams(
            collective_id=identity, has_side_effects=True, vmem_limit_bytes=32 * 1024 * 1024
        ),
    )(*inputs)


class Sender:
    def __init__(self, sem):
        self.sem, self.made = sem, []

    def prepare(self, src, dst, recv, target, when=None):
        copy = pltpu.make_async_remote_copy(
            src_ref=src,
            dst_ref=dst,
            send_sem=self.sem.at[len(self.made)],
            recv_sem=recv,
            device_id=target,
            device_id_type=pl.DeviceIdType.MESH,
        )
        self.made.append((when, copy))
        return lambda: run_when(when, copy.start)

    def send(self, src, dst, recv, target, when=None):
        self.prepare(src, dst, recv, target, when)()

    def finish(self):
        for when, copy in self.made:
            run_when(when, copy.wait_send)


def run_when(when, action):
    if when is None:
        action()
    else:
        pl.when(when)(lambda: action())


def layer_kernel(
    sizes,
    residual,
    q_major,
    k_major,
    v_major,
    q_minor,
    k_minor,
    v_minor,
    lam_major,
    lam_minor,
    gain_major,
    gain_minor,
    wo_major,
    wo_minor,
    mixer_gain,
    up_ref,
    down_ref,
    out_ref,
    pack,
    kv_all,
    q_in,
    qm,
    acc,
    peaks,
    totals,
    heads_out,
    cat,
    minor_in,
    wo_all,
    stream,
    normed_all,
    up_all,
    down_all,
    hidden,
    d_send,
    d_in,
    mine,
    x_send,
    x_in,
    x_keep,
    z_send,
    z_in,
    z_keep,
    send_sem,
    relay_sem,
    local_sem,
    r_y,
    r_kv,
    r_w,
    r_wo,
    r_h,
    r_g,
    r_d,
    r_x,
    r_z,
    credits,
):
    z_count, y_count, x_count = sizes
    bf16, f32 = jnp.bfloat16, jnp.float32
    own, tp = lax.axis_index("sp"), lax.axis_index("tp")
    z, y = own // y_count, lax.rem(own, y_count)
    x, c = tp // 2, lax.rem(tp, 2)
    oy, ox, oc = 1 - y, 1 - x, 1 - c
    zl = lax.rem(z, 2)
    oz = z + 1 - 2 * zl
    rows, tile = q_major.shape[0], residual.shape[0]
    width = q_minor.shape[1]
    half = width // 2
    unit = up_ref.shape[1] // UNITS
    part_size = [units * unit for units in PART_UNITS]
    part_at = [sum(part_size[:part]) for part in range(PARTS)]
    big, small = sum(part_size), sum(part_size[:-1])
    even = zl == 0
    up_rows = up_ref.shape[0]
    cols = down_ref.shape[1]

    def dev(z_at=z, y_at=y, x_at=x, c_at=c):
        return {"sp": z_at * y_count + y_at, "tp": x_at * 2 + c_at}

    def span(start, count):
        return pl.ds(pl.multiple_of(start * count, count), count)

    def arrive(place, recv):
        pltpu.make_async_remote_copy(
            src_ref=place,
            dst_ref=place,
            send_sem=send_sem.at[0],
            recv_sem=recv,
            device_id=dev(y_at=oy),
            device_id_type=pl.DeviceIdType.MESH,
        ).wait_recv()

    barrier = pltpu.get_barrier_semaphore()
    peers = []
    for dy in range(2):
        for dx in range(2):
            for dc in range(2):
                if dy or dx or dc:
                    peers.append(dev(y_at=oy if dy else y, x_at=ox if dx else x, c_at=oc if dc else c))
    peers += [dev(z_at=lax.rem(z + step, z_count)) for step in range(1, z_count)]
    for peer in peers:
        pl.semaphore_signal(barrier, inc=1, device_id=peer, device_id_type=pl.DeviceIdType.MESH)

    k_low = lax.broadcasted_iota(jnp.int32, (rows, width), 1)
    for head in range(2):
        k_part = (k_low >= head * half) & (k_low < (head + 1) * half)
        turned_v = pltpu.roll(v_minor[...].astype(f32), half, 1)
        pack[head] = jnp.where(k_part, k_minor[...].astype(f32), turned_v).astype(bf16)

    kv_all[z, 0, span(y, rows), :] = k_major[:, span(y, width)]
    kv_all[z, 1, span(y, rows), :] = v_major[:, span(y, width)]
    kv_all[z, 2, span(y, rows), :] = pack[y]
    local = []

    def weight_src(kind, z_at):
        part = kind % PARTS
        start = pl.multiple_of(lax.rem(z_at, 2) * big + part_at[part], unit) if part < PARTS - 1 else part_at[part]
        window = pl.ds(start, part_size[part])
        return up_ref.at[:, window] if kind < PARTS else down_ref.at[window, :]

    def weight_place(kind, source):
        window = pl.ds(part_at[kind % PARTS], part_size[kind % PARTS])
        return up_all.at[span(source, up_rows), window] if kind < PARTS else down_all.at[source, window, :]

    def fits(kind, z_at, when):
        if kind % PARTS < PARTS - 1:
            return when
        held = lax.rem(z_at, 2) == 0
        return held if when is None else held & when

    up_kinds, down_kinds = tuple(range(PARTS)), tuple(range(PARTS, 2 * PARTS))
    local_pairs = [
        (weight_src(kind, z), weight_place(kind, own), fits(kind, z, None)) for kind in up_kinds + down_kinds
    ]
    major_rows, minor_rows = wo_major.shape[0], wo_minor.shape[0]
    tp_count = 2 * x_count
    minor_base = tp_count * major_rows

    def wo_place(part, index):
        if part == 0:
            return wo_all.at[span(index, major_rows), :]
        return wo_all.at[pl.ds(pl.multiple_of(minor_base + index * minor_rows, minor_rows), minor_rows), :]

    for part, ref in enumerate((wo_major, wo_minor)):
        local_pairs.append((ref, wo_place(part, tp), None))
    for at, (src, dst, when) in enumerate(local_pairs):
        made = pltpu.make_async_copy(src, dst, local_sem.at[at])
        run_when(when, made.start)
        local.append((when, made))

    pl.semaphore_wait(barrier, len(peers))

    sender = Sender(send_sem)
    has_up = z < z_count - 1
    next_z = jnp.minimum(z + 1, z_count - 1)

    def kv_place(z_at, part, side):
        return kv_all.at[z_at, part, span(side, rows), :]

    for part, src in enumerate((k_major.at[:, span(oy, width)], v_major.at[:, span(oy, width)], pack.at[oy])):
        sender.send(src, kv_place(z, part, y), r_y.at[part], dev(y_at=oy))
    sender.send(q_major.at[:, span(oy, width)], q_in.at[0], r_y.at[3], dev(y_at=oy))
    sender.send(q_minor, q_in.at[1], r_y.at[4], dev(y_at=oy))
    for part, src in enumerate((k_major.at[:, span(y, width)], v_major.at[:, span(y, width)], pack.at[y])):
        sender.send(src, kv_place(z, part, y), r_kv.at[z, y, part], dev(z_at=next_z), has_up)

    def send_weight(kind, z_at, y_at, when=None):
        return sender.prepare(
            weight_src(kind, z_at),
            weight_place(kind, own),
            r_w.at[kind, own],
            dev(z_at=z_at, y_at=y_at),
            fits(kind, z_at, when),
        )

    def below(kinds, last=1, first=z_count - 1):
        return [
            send_weight(kind, jnp.maximum(z - step, 0), y, z >= step)
            for step in range(first, last - 1, -1)
            for kind in kinds
        ]

    def above(kinds, step, odd=None):
        when = z + step < z_count
        if odd is not None:
            when = when & (lax.rem(z + step, 2) == odd)
        if odd == 1:
            kinds = kinds[:-1]
        return [send_weight(kind, jnp.minimum(z + step, z_count - 1), y, when) for kind in kinds]

    def issue(starts):
        for start in starts:
            start()

    issue(below(up_kinds))
    for kind in up_kinds + down_kinds:
        send_weight(kind, z, oy)()
    for part, ref in enumerate((wo_major, wo_minor)):
        sender.send(ref, wo_place(part, tp), r_wo.at[part, tp], dev(x_at=ox))
        sender.send(ref, wo_place(part, tp), r_wo.at[part, tp], dev(c_at=oc))
    below_far, below_mid, below_near = below(down_kinds, 3), below(down_kinds, 2, 2), below(down_kinds, 1, 1)
    slow = (zl == 1) & (z > 1)
    near_up = above(up_kinds, 1)
    late_up = (zl == 0) & (z > 0)

    scales = (DK_MAJOR ** (-0.5) * LOG2_E, DK_MINOR ** (-0.5) * LOG2_E)
    lane = lax.broadcasted_iota(jnp.int32, (rows, width), 1)

    def pick(group, side, block):
        first, size = (0, DK_MAJOR) if group == 0 else (y * half, DK_MINOR)
        for m in range(MAPS):
            low = first + m * size
            keep = (lane >= low) & (lane < low + size)
            qm[group, side, m * rows : (m + 1) * rows, :] = jnp.where(keep, block.astype(f32), 0.0).astype(bf16)

    def fold(side, z_at, key_side, diagonal):
        window = span(key_side, rows)
        for group in range(2):
            keys = kv_all[z_at, 2 * group, window, :]
            stored = kv_all[z_at, 1 + group, window, :]
            values = jnp.transpose(stored.astype(f32)).astype(bf16)
            scores = lax.dot_general(
                keys, qm[group, side], (((1,), (1,)), ((), ())), preferred_element_type=f32
            ) * scales[group]
            if diagonal:
                key_pos = lax.broadcasted_iota(jnp.int32, scores.shape, 0)
                query_pos = lax.broadcasted_iota(jnp.int32, scores.shape, 1) % rows
                visible = key_pos // SEGMENT <= query_pos // SEGMENT
                scores = jnp.where(visible, scores, NEGATIVE)
            peak = jnp.max(scores, axis=0, keepdims=True)
            if not diagonal:
                peak_old = peaks[group, side]
                peak = jnp.maximum(peak, peak_old)
            weights = jnp.exp2(scores - peak)
            total = jnp.sum(weights, axis=0, keepdims=True)
            sums = jnp.dot(values, weights.astype(bf16), preferred_element_type=f32)
            if not diagonal:
                factor = jnp.exp2(peak_old - peak)
                total = total + totals[group, side] * factor
                sums = sums + acc[group, side] * factor
            peaks[group, side] = peak
            totals[group, side] = total
            acc[group, side] = sums

    pick(0, y, q_major[:, span(y, width)])
    pick(1, y, q_minor[...])
    fold(y, z, y, True)

    for part in range(3):
        arrive(kv_place(z, part, oy), r_y.at[part])
        sender.send(kv_place(z, part, oy), kv_place(z, part, oy), r_kv.at[z, oy, part], dev(z_at=next_z), has_up)

    def credit(kind, back):
        pl.semaphore_signal(
            credits.at[kind, z],
            inc=1,
            device_id=dev(z_at=jnp.maximum(z - back, 0)),
            device_id_type=pl.DeviceIdType.MESH,
        )

    def await_credit(kind, step):
        pl.semaphore_wait(credits.at[kind, jnp.minimum(z + step, z_count - 1)], 1)

    def relay_copy(z_at, side, part):
        return pltpu.make_async_remote_copy(
            src_ref=kv_place(z_at, part, side),
            dst_ref=kv_place(z_at, part, side),
            send_sem=relay_sem.at[z_at, side, part],
            recv_sem=r_kv.at[z_at, side, part],
            device_id=dev(z_at=next_z),
            device_id_type=pl.DeviceIdType.MESH,
        )

    def take(z_at, side):
        for part in range(3):
            arrive(kv_place(z_at, part, side), r_kv.at[z_at, side, part])
            run_when(has_up, relay_copy(z_at, side, part).start)

    def after_last():
        run_when(zl == 1, lambda: issue(near_up))
        for back in range(2, z_count):
            run_when(z >= back, lambda: credit(0, back))

        @pl.when(jnp.logical_not(slow))
        def _():
            issue(below_far + below_mid + below_near)

    for part in range(2):
        arrive(q_in.at[part], r_y.at[3 + part])
        pick(part, oy, q_in[part])

    pl.when(z == 0)(lambda: issue(near_up))

    @pl.when(z > 0)
    def _():
        for side in range(2):
            take(z - 1, side)

    pl.when(z == 1)(after_last)
    fold(oy, z, oy, True)
    fold(1, z, 0, False)

    def earlier(index, carry):
        z_at, key_side = z - 1 - index // 2, lax.rem(index, 2)
        pl.when(index > 1)(lambda: take(z_at, key_side))
        pl.when((index == 2 * z - 1) & (z > 1))(after_last)
        pl.when((index == 2 * z - 4) & slow)(lambda: issue(below_near))
        pl.when((index == 2 * z - 2) & slow)(lambda: issue(below_far))

        def inner(side, carry):
            fold(side, z_at, key_side, False)
            return carry

        lax.fori_loop(0, 2, inner, 0)
        return carry

    lax.fori_loop(0, 2 * z, earlier, 0)

    value_row = lax.broadcasted_iota(jnp.int32, (width, rows), 0)
    value_keep = (value_row >= oy * half) & (value_row < (oy + 1) * half)
    gains = (gain_major[...], jnp.concatenate([gain_minor[...], gain_minor[...]], axis=1))
    lams = (lam_major[y], lam_minor[y])

    def close(side, carry):
        for group in range(2):
            ratio = acc[group, side] / totals[group, side]
            diff = ratio[:, :rows] - lams[group] * ratio[:, rows:]
            if group == 1:
                diff = jnp.where(value_keep, diff, 0.0)
            count = width if group == 0 else half
            mean = jnp.sum(diff * diff, axis=0, keepdims=True) * (1.0 / count)
            done = jnp.transpose(diff * lax.rsqrt(mean + EPSILON)) * gains[group]
            heads_out[group, span(side, rows), :] = done.astype(bf16)
        return carry

    lax.fori_loop(0, 2, close, 0)

    place = tp * y_count + y

    def token_span(y_at, x_at, c_at):
        return span(y_at * (rows // tile) + x_at * 2 + c_at, tile)

    def head_place(group, index):
        return cat.at[:, span(index, width)] if group == 0 else minor_in.at[index]

    for dy, dx, dc in ((1, 1, 1), (1, 1, 0), (1, 0, 1), (1, 0, 0), (0, 1, 1), (0, 1, 0), (0, 0, 1)):
        y_at, x_at, c_at = oy if dy else y, ox if dx else x, oc if dc else c
        for group in range(2):
            sender.send(
                heads_out.at[group, token_span(y_at, x_at, c_at), :],
                head_place(group, place),
                r_h.at[group, place],
                dev(y_at=y_at, x_at=x_at, c_at=c_at),
            )
    cat[:, span(place, width)] = heads_out[0, token_span(y, x, c), :]
    minor_in[place] = heads_out[1, token_span(y, x, c), :]

    def take_weight(kind, source):
        run_when(fits(kind, z, None), lambda: arrive(weight_place(kind, source), r_w.at[kind, source]))

    def pass_weight(kind, z_at, when):
        source = z_at * y_count + y
        when = fits(kind, z, when)
        run_when(when, lambda: arrive(weight_place(kind, source), r_w.at[kind, source]))
        sender.send(weight_place(kind, source), weight_place(kind, source), r_w.at[kind, source], dev(y_at=oy), when)

    for step in range(1, z_count):
        for kind in up_kinds:
            pass_weight(kind, lax.rem(z + step, z_count), z + step < z_count)
    for step in range(2, z_count):
        run_when(z + step < z_count, lambda: await_credit(0, step))
        issue(above(up_kinds, step))

    for when, made in local:
        run_when(when, made.wait)
    for part in range(2):
        index = ox * 2 + c
        arrive(wo_place(part, index), r_wo.at[part, index])
        sender.send(wo_place(part, index), wo_place(part, index), r_wo.at[part, index], dev(c_at=oc))
    for index in (x * 2 + oc, ox * 2 + oc):
        for part in range(2):
            arrive(wo_place(part, index), r_wo.at[part, index])
    for dy, dx, dc in ((0, 0, 1), (0, 1, 0), (0, 1, 1), (1, 0, 0), (1, 0, 1), (1, 1, 0), (1, 1, 1)):
        index = ((ox if dx else x) * 2 + (oc if dc else c)) * y_count + (oy if dy else y)
        for group in range(2):
            arrive(head_place(group, index), r_h.at[group, index])
    major_width = tp_count * y_count * width
    for index in range(tp_count):
        both = minor_in[index * y_count].astype(f32) + minor_in[index * y_count + 1].astype(f32)
        cat[:, major_width + index * width : major_width + (index + 1) * width] = pltpu.roll(both, half, 1).astype(bf16)

    model = residual.shape[1]
    step_cols = 256

    def project(index, carry):
        window = span(index, step_cols)
        mixed = jnp.dot(cat[...], wo_all[:, window], preferred_element_type=f32)
        added = residual[:, window].astype(f32) + mixed
        stream[:, window] = added
        return carry + jnp.sum(added * added, axis=1, keepdims=True)

    square = lax.fori_loop(0, model // step_cols, project, jnp.zeros((tile, 1), f32))
    norm = lax.rsqrt(square * (1.0 / model) + EPSILON)

    def slot(c_at, x_at, zl_at):
        return c_at * (2 * x_count) + x_at * 2 + zl_at

    def rows_at(index):
        return normed_all.at[span(index, tile), :]

    mine_at = slot(c, x, zl)
    normed_all[span(mine_at, tile), :] = (stream[...] * norm * mixer_gain[...]).astype(bf16)

    def share(index, target):
        sender.send(rows_at(index), rows_at(index), r_g.at[index], target)

    partner, x_peer, z_peer = dev(c_at=oc), dev(x_at=ox), dev(z_at=oz)
    share(mine_at, z_peer)
    share(mine_at, x_peer)
    share(mine_at, partner)
    run_when(late_up, lambda: issue(near_up))
    run_when(slow, lambda: issue(below_mid))
    issue(above(down_kinds, 1))
    for step in range(1, z_count - 1):
        for kind in up_kinds:
            pass_weight(kind, lax.rem(z + step, z_count), z + step >= z_count)
    for step in range(z_count - 1, 0, -1):
        for kind in down_kinds:
            pass_weight(kind, lax.rem(z + step, z_count), even & (z + step < z_count))
    index = slot(c, ox, zl)
    arrive(rows_at(index), r_g.at[index])
    share(index, partner)
    for step in range(2, z_count):
        issue(above(down_kinds, step, 0))
    index = slot(c, x, 1 - zl)
    arrive(rows_at(index), r_g.at[index])
    share(index, x_peer)
    share(index, partner)
    for kind in up_kinds:
        pass_weight(kind, lax.rem(z + z_count - 1, z_count), z > 0)
    for back in range(2, z_count):
        run_when((z >= back) & (zl == 1), lambda: credit(1, back))
    for step in range(z_count - 1, 0, -1):
        for kind in down_kinds[:-1]:
            pass_weight(kind, lax.rem(z + step, z_count), (zl == 1) & ((z + step < z_count) | (z == 1)))
    for step in range(2, z_count):
        run_when((z + step < z_count) & (lax.rem(z + step, 2) == 1), lambda: await_credit(1, step))
        issue(above(down_kinds, step, 1))
    index = slot(c, ox, 1 - zl)
    arrive(rows_at(index), r_g.at[index])
    share(index, partner)
    for step in range(z_count):
        source = lax.rem(z + step, z_count) * y_count + oy
        for kind in up_kinds:
            take_weight(kind, source)

    group_rows = 2 * x_count * tile
    hid_cols = 256

    def expand(side):
        def one(index, carry):
            window = span(index, hid_cols)
            pre = jnp.dot(
                normed_all[span(side, group_rows), :], up_all[:, window], preferred_element_type=f32
            )
            hidden[span(side, group_rows), window] = jnp.square(jnp.maximum(pre, 0.0)).astype(bf16)
            return carry

        full = jnp.where(even, big // hid_cols, small // hid_cols)
        lax.fori_loop(0, full, one, 0)
        rest = big % hid_cols
        assert rest == small % hid_cols
        if rest:
            window = pl.ds(pl.multiple_of(full * hid_cols, hid_cols), rest)
            pre = jnp.dot(
                normed_all[span(side, group_rows), :], up_all[:, window], preferred_element_type=f32
            )
            hidden[span(side, group_rows), window] = jnp.square(jnp.maximum(pre, 0.0)).astype(bf16)

    expand(c)
    for x_at in range(x_count):
        for zl_at in range(2):
            index = slot(oc, x_at, zl_at)
            arrive(rows_at(index), r_g.at[index])
    expand(oc)

    for step in range(1, z_count):
        for kind in down_kinds:
            pass_weight(kind, lax.rem(z + step, z_count), even & (z + step >= z_count))

    x_rows = 2 * tile
    blocks = []

    def stage_x(t):
        arrive(d_in.at[t], r_d.at[t])
        x_send[t] = (mine[t, span(ox, x_rows), :] + d_in[t, span(ox, x_rows), :].astype(f32)).astype(bf16)
        sender.send(x_send.at[t], x_in.at[t], r_x.at[t], x_peer)
        x_keep[t] = mine[t, span(x, x_rows), :] + d_in[t, span(x, x_rows), :].astype(f32)

    def stage_z(t):
        arrive(x_in.at[t], r_x.at[t])
        other, same = span(1 - zl, tile), span(zl, tile)
        z_send[t] = (x_keep[t, other, :] + x_in[t, other, :].astype(f32)).astype(bf16)
        sender.send(z_send.at[t], z_in.at[blocks[t]], r_z.at[blocks[t]], z_peer)
        z_keep[t] = x_keep[t, same, :] + x_in[t, same, :].astype(f32)

    def stage_end(t):
        arrive(z_in.at[blocks[t]], r_z.at[blocks[t]])
        window = span(blocks[t], cols)
        total = stream[:, window] + (z_keep[t] + z_in[blocks[t]].astype(f32))
        out_ref[:, window] = total.astype(out_ref.dtype)

    reached = {stage_x: 0, stage_z: 0, stage_end: 0}

    def advance(*targets):
        for stage, target in zip((stage_x, stage_z, stage_end), targets):
            while reached[stage] < min(target, z_count * y_count):
                stage(reached[stage])
                reached[stage] += 1

    lower = [0, *range(z_count - 1, 0, -1)]
    upper = [*range(1, z_count - 1), 0, z_count - 1]

    def z_of(block):
        return lax.rem(z - zl + jnp.where(z < 2, lower[block], upper[block]), z_count)

    count = z_count
    order = [(0, 0), (0, 1), (1, 0)]
    for block in range(2, count):
        order += [(block, 0), (block - 1, 1)]
    order.append((count - 1, 1))
    late_pass = {0: [(count - 2, PARTS)], 1: [(1, PARTS)], 2: [(1, kind) for kind in down_kinds[1:-1]]}
    for t, (block, side) in enumerate(order):
        if block > 1 and not side:
            first = PARTS + 1 if block == count - 2 else PARTS
            late_pass[t] = [(block, kind) for kind in range(first, 2 * PARTS - 1)]
    for t, (block, side) in enumerate(order):
        source = z_of(block) * y_count + (oy if side else y)
        blocks.append(source)
        for ahead, kind in late_pass.get(t, ()):
            pass_weight(kind, z_of(ahead), slow)
        if t == len(order) - 1:
            advance(t, t - 2, t - 6)
        if side:
            for kind in down_kinds:
                take_weight(kind, source)
        start = sender.prepare(d_send.at[t], d_in.at[t], r_d.at[t], partner)

        def multiply(depth):
            block = down_all[source, :depth, :]
            sent = jnp.dot(hidden[span(oc, group_rows), :depth], block, preferred_element_type=f32)
            d_send[t] = sent.astype(bf16)
            start()
            mine[t] = jnp.dot(hidden[span(c, group_rows), :depth], block, preferred_element_type=f32)

        pl.when(even)(lambda: multiply(big))
        pl.when(jnp.logical_not(even))(lambda: multiply(small))
        advance(t, t - 3, t - 6)
    for t in range(len(order) + 1):
        advance(len(order), t, t - 1)
    advance(len(order), len(order), len(order))

    sender.finish()
    for step in range(1, z_count):
        for side in range(2):
            for part in range(3):
                copy = relay_copy(jnp.maximum(z - step, 0), side, part)
                run_when((z >= step) & has_up, copy.wait_send)


def fused(sp_count, tp_count, args):
    residual, q_major, _, v_major, q_minor = args[:5]
    wo_major, wo_minor, _, up_weight, down_weight = args[11:16]
    z_count, y_count = grid_sizes(sp_count)
    x_count = tp_count // 2
    rows, tile, width = q_major.shape[0], residual.shape[0], q_minor.shape[1]
    model = residual.shape[1]
    hid = up_weight.shape[1] // UNITS * sum(PART_UNITS)
    cols = down_weight.shape[1]
    features = tp_count * (wo_major.shape[0] + wo_minor.shape[0])
    group_rows = 2 * x_count * tile
    steps = sp_count
    bf16, f32 = jnp.bfloat16, jnp.float32
    dma = pltpu.SemaphoreType.DMA
    sends = 192
    hbm = pl.BlockSpec(memory_space=pltpu.HBM)
    return pl.pallas_call(
        functools.partial(layer_kernel, (z_count, y_count, x_count)),
        out_shape=jax.ShapeDtypeStruct(residual.shape, residual.dtype),
        in_specs=[VMEM] * 7 + [SMEM] * 2 + [VMEM] * 2 + [hbm] * 2 + [VMEM] + [hbm] * 2,
        out_specs=VMEM,
        scratch_shapes=[
            pltpu.VMEM((2, rows, width), bf16),
            pltpu.VMEM((z_count, 3, y_count * rows, width), bf16),
            pltpu.VMEM((2, rows, width), bf16),
            pltpu.VMEM((2, 2, MAPS * rows, width), bf16),
            pltpu.VMEM((2, 2, width, MAPS * rows), f32),
            pltpu.VMEM((2, 2, 1, MAPS * rows), f32),
            pltpu.VMEM((2, 2, 1, MAPS * rows), f32),
            pltpu.VMEM((2, y_count * rows, width), bf16),
            pltpu.VMEM((tile, features), bf16),
            pltpu.VMEM((tp_count * y_count, tile, width), bf16),
            pltpu.VMEM((features, model), bf16),
            pltpu.VMEM((tile, model), f32),
            pltpu.VMEM((2 * group_rows, model), bf16),
            pltpu.VMEM((model, hid), bf16),
            pltpu.VMEM((sp_count, hid, cols), bf16),
            pltpu.VMEM((2 * group_rows, hid), bf16),
            pltpu.VMEM((steps, group_rows, cols), bf16),
            pltpu.VMEM((steps, group_rows, cols), bf16),
            pltpu.VMEM((steps, group_rows, cols), f32),
            pltpu.VMEM((steps, 2 * tile, cols), bf16),
            pltpu.VMEM((steps, 2 * tile, cols), bf16),
            pltpu.VMEM((steps, 2 * tile, cols), f32),
            pltpu.VMEM((steps, tile, cols), bf16),
            pltpu.VMEM((steps, tile, cols), bf16),
            pltpu.VMEM((steps, tile, cols), f32),
            dma((sends,)),
            dma((z_count, 2, 3)),
            dma((2 * PARTS + 2,)),
            dma((5,)),
            dma((z_count, 2, 3)),
            dma((2 * PARTS, sp_count)),
            dma((2, tp_count)),
            dma((2, tp_count * y_count)),
            dma((2 * group_rows // tile,)),
            dma((steps,)),
            dma((steps,)),
            dma((steps,)),
            pltpu.SemaphoreType.REGULAR((2, z_count)),
        ],
        compiler_params=pltpu.CompilerParams(
            collective_id=0, has_side_effects=True, vmem_limit_bytes=63 * 1024 * 1024
        ),
    )(*args)


def fits_fused(sp_count, tp_count, args):
    q_major, k_major, v_major, q_minor, k_minor, v_minor = args[1:7]
    z_count, y_count = grid_sizes(sp_count)
    width = q_minor.shape[1]
    return (
        y_count == 2
        and tp_count == 4
        and z_count % 2 == 0
        and width == 2 * MAPS * DK_MINOR
        and width == MAPS * DK_MAJOR
        and width % 128 == 0
        and z_count >= 4
        and args[14].shape[1] % (UNITS * 128) == 0
        and v_minor.shape[1] == width
        and q_major.shape[1] == v_major.shape[1] == 2 * width
    )


def body(
    residual,
    query_major,
    keys_major,
    values_major,
    query_minor,
    keys_minor,
    values_minor,
    lambda_major,
    lambda_minor,
    gain_major,
    gain_minor,
    output_major,
    output_minor,
    mixer_gain,
    up_weight,
    down_weight,
):
    sp_count, tp_count = lax.axis_size("sp"), lax.axis_size("tp")
    args = (
        residual,
        query_major,
        keys_major,
        values_major,
        query_minor,
        keys_minor,
        values_minor,
        lambda_major,
        lambda_minor,
        gain_major[None, :],
        gain_minor[None, :],
        output_major,
        output_minor,
        mixer_gain[None, :],
        up_weight,
        down_weight,
    )
    if fits_fused(sp_count, tp_count, args):
        return fused(sp_count, tp_count, args)
    out_major, out_minor, up_full, down_full = mixer(
        lax.axis_size("sp"),
        query_major,
        keys_major,
        values_major,
        query_minor,
        jnp.concatenate([keys_minor, values_minor], axis=1),
        lambda_major,
        lambda_minor,
        gain_major[:, None],
        gain_minor[:, None],
        up_weight,
        down_weight,
    )
    partial_sum = jnp.dot(out_major, output_major, preferred_element_type=jnp.float32)
    partial_sum = partial_sum + jnp.dot(out_minor, output_minor, preferred_element_type=jnp.float32)
    rows = residual.shape[0]
    stream, normed_all = tp_call(
        mix_kernel,
        1,
        (partial_sum.astype(jnp.bfloat16), residual, mixer_gain[None, :]),
        (
            jax.ShapeDtypeStruct(residual.shape, jnp.float32),
            jax.ShapeDtypeStruct(partial_sum.shape, jnp.bfloat16),
        ),
        rows,
        True,
    )
    pre_act = jnp.dot(
        normed_all,
        up_full,
        preferred_element_type=jnp.float32,
    )
    hidden = jnp.square(jax.nn.relu(pre_act)).astype(jnp.bfloat16)
    down_part = jnp.einsum("th,shd->tsd", hidden, down_full, preferred_element_type=jnp.float32)
    down_part = down_part.astype(jnp.bfloat16).reshape(partial_sum.shape)
    return tp_call(
        sum_kernel,
        2,
        (down_part, stream),
        jax.ShapeDtypeStruct(residual.shape, residual.dtype),
        rows,
        False,
    )


def solution(mesh):
    return jax.shard_map(
        body,
        mesh=mesh,
        in_specs=(
            P(("sp", "tp"), None),
            P("sp", "tp"),
            P("sp", "tp"),
            P("sp", "tp"),
            P("sp", "tp"),
            P("sp", "tp"),
            P("sp", "tp"),
            P("tp"),
            P("tp"),
            P(),
            P(),
            P("tp", None),
            P("tp", None),
            P(),
            P("sp", "tp"),
            P("tp", "sp"),
        ),
        out_specs=P(("sp", "tp"), None),
        check_vma=False,
    )
```

```python
import functools

import jax
import jax.numpy as jnp
from jax import lax
from jax.experimental import pallas as pl
from jax.experimental.pallas import tpu as pltpu
from jax.sharding import PartitionSpec as P

DK_MAJOR = 64
DK_MINOR = 32
SEGMENT = 64
MAPS = 2
PART_UNITS = (3, 3, 4)
PARTS = len(PART_UNITS)
UNITS = 16

EPSILON = 1e-06
NEGATIVE = -1e30
LOG2_E = 1.4426950408889634
ANY = pl.BlockSpec(memory_space=pl.ANY)
VMEM = pl.BlockSpec(memory_space=pltpu.VMEM)
SMEM = pl.BlockSpec(memory_space=pltpu.SMEM)


def grid_sizes(sp_count):
    y_count = 1 << ((sp_count.bit_length() - 1) // 2)
    return sp_count // y_count, y_count


class Gather:
    def __init__(self, sp_count, places, send_sem, recv_sem):
        self.z_count, self.y_count = grid_sizes(sp_count)
        own = lax.axis_index("sp")
        self.own, self.z, self.y = own, own // self.y_count, lax.rem(own, self.y_count)
        self.places, self.send_sem, self.recv_sem = places, send_sem, recv_sem
        self.copies = []

    def z_peer(self, step):
        return lax.rem(self.z + step, self.z_count) * self.y_count + self.y

    def y_peer(self, step):
        return self.z * self.y_count + lax.rem(self.y + step, self.y_count)

    def send(self, array, source, src_ref, target):
        copy = pltpu.make_async_remote_copy(
            src_ref=src_ref,
            dst_ref=self.places[array](source),
            send_sem=self.send_sem.at[array, len([c for c in self.copies if c[0] == array])],
            recv_sem=self.recv_sem.at[array, source],
            device_id={"sp": target},
            device_id_type=pl.DeviceIdType.MESH,
        )
        copy.start()
        self.copies.append((array, copy))

    def wait_block(self, array, source):
        place = self.places[array](source)
        pltpu.make_async_remote_copy(
            src_ref=place,
            dst_ref=place,
            send_sem=self.send_sem.at[array, 0],
            recv_sem=self.recv_sem.at[array, source],
            device_id={"sp": self.y_peer(1)},
            device_id_type=pl.DeviceIdType.MESH,
        ).wait_recv()

    def send_z(self, array, src_ref):
        for step in range(1, self.z_count):
            self.send(array, self.own, src_ref, self.z_peer(step))

    def send_y(self, array, src_ref):
        for step in range(1, self.y_count):
            self.send(array, self.own, src_ref, self.y_peer(step))

    def pass_on(self, array, step):
        source = self.z_peer(self.z_count - step)
        self.wait_block(array, source)
        for y_step in range(1, self.y_count):
            self.send(array, source, self.places[array](source), self.y_peer(y_step))

    def wait_y(self, array):
        for y_step in range(1, self.y_count):
            for z_step in range(self.z_count):
                z_at = lax.rem(self.z + z_step, self.z_count)
                self.wait_block(array, z_at * self.y_count + lax.rem(self.y + y_step, self.y_count))

    def finish(self):
        for _, copy in self.copies:
            copy.wait_send()


def mixer_kernel(
    sp_count,
    groups,
    q_major,
    k_major,
    v_major,
    q_minor,
    kv_minor,
    lam_major,
    lam_minor,
    gain_major,
    gain_minor,
    up_ref,
    down_ref,
    out_major,
    out_minor,
    up_all,
    down_all,
    k_major_all,
    v_major_all,
    kv_minor_all,
    qm_major,
    qm_minor,
    acc_major,
    acc_minor,
    peaks,
    totals,
    send_sem,
    recv_sem,
    local_sem,
):
    rows = q_major.shape[0]
    up_rows = up_ref.shape[0]

    def rows_of(ref, count):
        return lambda source: ref.at[pl.ds(pl.multiple_of(source * count, count), count), :]

    places = [
        rows_of(k_major_all, rows),
        rows_of(v_major_all, rows),
        rows_of(kv_minor_all, rows),
        rows_of(up_all, up_rows),
        lambda source: down_all.at[source],
    ]
    own_refs = [k_major, v_major, kv_minor, up_ref, down_ref]
    gather = Gather(sp_count, places, send_sem, recv_sem)
    own = gather.own

    barrier = pltpu.get_barrier_semaphore()
    peers = [gather.z_peer(step) for step in range(1, gather.z_count)]
    peers += [gather.y_peer(step) for step in range(1, gather.y_count)]
    for peer in peers:
        pl.semaphore_signal(
            barrier, inc=1, device_id={"sp": peer}, device_id_type=pl.DeviceIdType.MESH
        )
    pl.semaphore_wait(barrier, len(peers))

    for array in range(3):
        gather.send_z(array, own_refs[array])
    for array in range(3):
        gather.send_y(array, own_refs[array])
    for array in (3, 4):
        gather.send_z(array, own_refs[array])
    for array in (3, 4):
        gather.send_y(array, own_refs[array])
    local = []
    for slot, array in enumerate((3, 4)):
        copy = pltpu.make_async_copy(own_refs[array], places[array](own), local_sem.at[slot])
        copy.start()
        local.append(copy)

    heads = []
    for group, (head_count, key_size) in enumerate(groups):
        q_ref, qm_ref = ((q_major, qm_major), (q_minor, qm_minor))[group]
        acc_ref = (acc_major, acc_minor)[group]
        value_size = acc_ref.shape[1]
        lanes = qm_ref.shape[2]
        for head in range(head_count):
            first = head * MAPS * key_size
            lane_first = first // lanes * lanes
            block = q_ref[:, lane_first : lane_first + lanes]
            lane = lax.broadcasted_iota(jnp.int32, block.shape, 1) + lane_first
            for m in range(MAPS):
                low = first + m * key_size
                keep = (lane >= low) & (lane < low + key_size)
                picked = jnp.where(keep, block.astype(jnp.float32), 0.0).astype(block.dtype)
                qm_ref[head, m * rows : (m + 1) * rows, :] = picked
            heads.append((group, head, len(heads), lane_first, lanes, value_size, key_size))

    minor_keys = q_minor.shape[1]
    minor_first = minor_keys // 128 * 128

    def fold(key_refs, value_refs, at, diagonal):
        window = pl.ds(at, rows)
        stored = (value_refs[0][window, :], value_refs[1][window, minor_first:])
        turned = [jnp.transpose(v.astype(jnp.float32)).astype(jnp.bfloat16) for v in stored]
        turned[1] = turned[1][minor_keys - minor_first :, :]
        for group, head, index, lane_first, lanes, value_size, key_size in heads:
            qm_ref = (qm_major, qm_minor)[group]
            acc_ref = (acc_major, acc_minor)[group]
            keys = key_refs[group][window, lane_first : lane_first + lanes]
            values = turned[group][head * value_size : (head + 1) * value_size, :]
            scores = lax.dot_general(
                keys, qm_ref[head], (((1,), (1,)), ((), ())), preferred_element_type=jnp.float32
            ) * (key_size ** (-0.5) * LOG2_E)
            if diagonal:
                key_pos = lax.broadcasted_iota(jnp.int32, scores.shape, 0)
                query_pos = lax.broadcasted_iota(jnp.int32, scores.shape, 1) % rows
                visible = key_pos // SEGMENT <= query_pos // SEGMENT
                scores = jnp.where(visible, scores, NEGATIVE)
            peak = jnp.max(scores, axis=0, keepdims=True)
            if not diagonal:
                peak_old = peaks[index]
                peak = jnp.maximum(peak, peak_old)
            weights = jnp.exp2(scores - peak)
            total = jnp.sum(weights, axis=0, keepdims=True)
            sums = jnp.dot(
                values, weights.astype(jnp.bfloat16), preferred_element_type=jnp.float32
            )
            if not diagonal:
                factor = jnp.exp2(peak_old - peak)
                total = total + totals[index] * factor
                sums = sums + acc_ref[head] * factor
            peaks[index] = peak
            totals[index] = total
            acc_ref[head] = sums

    fold((k_major, kv_minor), (v_major, kv_minor), 0, True)

    for step in range(1, gather.z_count):
        for array in range(3):
            gather.pass_on(array, step)

    def earlier(block, carry):
        at = pl.multiple_of(block * rows, rows)
        fold((k_major_all, kv_minor_all), (v_major_all, kv_minor_all), at, False)
        return carry

    y_count = gather.y_count

    def same_y(z_at, carry):
        return earlier(z_at * y_count + gather.y, carry)

    def other_y(index, carry):
        z_at, place = index // (y_count - 1), lax.rem(index, y_count - 1)
        y_at = place + (place >= gather.y).astype(jnp.int32)
        return earlier(z_at * y_count + y_at, carry)

    lax.fori_loop(0, gather.z, same_y, 0)
    for array in range(3):
        gather.wait_y(array)
    lax.fori_loop(0, gather.z * (y_count - 1) + gather.y, other_y, 0)

    for group, (head_count, _) in enumerate(groups):
        acc_ref = (acc_major, acc_minor)[group]
        lam_ref = (lam_major, lam_minor)[group]
        gain_ref = (gain_major, gain_minor)[group]
        out_ref = (out_major, out_minor)[group]
        done = []
        for head in range(head_count):
            index = next(h[2] for h in heads if h[0] == group and h[1] == head)
            ratio = acc_ref[head] / totals[index]
            diff = ratio[:, :rows] - lam_ref[head] * ratio[:, rows:]
            mean = jnp.mean(diff * diff, axis=0, keepdims=True)
            done.append(diff * lax.rsqrt(mean + EPSILON) * gain_ref[...])
        out_ref[...] = jnp.transpose(jnp.concatenate(done, axis=0)).astype(out_ref.dtype)

    for step in range(1, gather.z_count):
        for array in (3, 4):
            gather.pass_on(array, step)
    for array in (3, 4):
        gather.wait_y(array)
    for copy in local:
        copy.wait()
    gather.finish()


def mixer(sp_count, *args):
    q_major, k_major, v_major, q_minor, kv_minor = args[:5]
    up_weight, down_weight = args[9:11]
    heads_major = k_major.shape[1] // (MAPS * DK_MAJOR)
    heads_minor = q_minor.shape[1] // (MAPS * DK_MINOR)
    rows = q_major.shape[0]
    size_major = v_major.shape[1] // heads_major
    width_minor = kv_minor.shape[1] - q_minor.shape[1]
    size_minor = width_minor // heads_minor
    lanes_major = min(MAPS * DK_MAJOR, q_major.shape[1])
    lanes_minor = min(128, q_minor.shape[1])
    z_count, y_count = grid_sizes(sp_count)
    sends = (z_count - 1) + (y_count - 1) * z_count
    tokens = rows * sp_count
    bf16, f32 = jnp.bfloat16, jnp.float32
    head_total = heads_major + heads_minor
    return pl.pallas_call(
        functools.partial(
            mixer_kernel, sp_count, ((heads_major, DK_MAJOR), (heads_minor, DK_MINOR))
        ),
        out_shape=(
            jax.ShapeDtypeStruct(v_major.shape, bf16),
            jax.ShapeDtypeStruct((rows, width_minor), bf16),
            jax.ShapeDtypeStruct((up_weight.shape[0] * sp_count, up_weight.shape[1]), bf16),
            jax.ShapeDtypeStruct((sp_count, *down_weight.shape), bf16),
        ),
        in_specs=[VMEM] * 5 + [SMEM] * 2 + [VMEM] * 4,
        out_specs=(VMEM, VMEM, ANY, ANY),
        scratch_shapes=[
            pltpu.VMEM((tokens, k_major.shape[1]), bf16),
            pltpu.VMEM((tokens, v_major.shape[1]), bf16),
            pltpu.VMEM((tokens, kv_minor.shape[1]), bf16),
            pltpu.VMEM((heads_major, MAPS * rows, lanes_major), bf16),
            pltpu.VMEM((heads_minor, MAPS * rows, lanes_minor), bf16),
            pltpu.VMEM((heads_major, size_major, MAPS * rows), f32),
            pltpu.VMEM((heads_minor, size_minor, MAPS * rows), f32),
            pltpu.VMEM((head_total, 1, MAPS * rows), f32),
            pltpu.VMEM((head_total, 1, MAPS * rows), f32),
            pltpu.SemaphoreType.DMA((5, sends)),
            pltpu.SemaphoreType.DMA((5, sp_count)),
            pltpu.SemaphoreType.DMA((2,)),
        ],
        compiler_params=pltpu.CompilerParams(
            collective_id=0, has_side_effects=True, vmem_limit_bytes=60 * 1024 * 1024
        ),
    )(*args)


class Exchange:
    def __init__(self, tp_count, send_sem, recv_sem):
        own = lax.axis_index("tp")
        self.x_count = tp_count // 2
        self.own, self.x, self.core = own, own // 2, lax.rem(own, 2)
        self.partner = self.x * 2 + 1 - self.core
        self.send_sem, self.recv_sem = send_sem, recv_sem

    def enter(self):
        barrier = pltpu.get_barrier_semaphore()
        peers = [self.partner] + [self.x_peer(step) for step in range(1, self.x_count)]
        for peer in peers:
            pl.semaphore_signal(
                barrier, inc=1, device_id={"tp": peer}, device_id_type=pl.DeviceIdType.MESH
            )
        pl.semaphore_wait(barrier, len(peers))

    def x_peer(self, step):
        return lax.rem(self.x + step, self.x_count) * 2 + self.core

    def copy(self, src, dst, slot, target):
        made = pltpu.make_async_remote_copy(
            src_ref=src,
            dst_ref=dst,
            send_sem=self.send_sem.at[slot],
            recv_sem=self.recv_sem.at[slot],
            device_id={"tp": target},
            device_id_type=pl.DeviceIdType.MESH,
        )
        made.start()
        return made

    def total(self, partial, pair_in, pair_sum, x_in, rows):
        def block(x_at, core):
            return pl.ds(pl.multiple_of((x_at * 2 + core) * rows, rows), rows)

        steps = list(range(1, self.x_count)) + [0]
        at = [lax.rem(self.x + step, self.x_count) for step in range(self.x_count)]
        pair = {}
        for step in steps:
            pair[step] = self.copy(
                partial.at[block(at[step], 1 - self.core), :], pair_in.at[step], step, self.partner
            )
        across = []
        for step in steps:
            pair[step].wait_recv()
            mine = partial[block(at[step], self.core), :].astype(jnp.float32)
            both = mine + pair_in[step].astype(jnp.float32)
            if step:
                pair_sum[step] = both.astype(jnp.bfloat16)
                across.append(
                    self.copy(
                        pair_sum.at[step], x_in.at[step], self.x_count + step, self.x_peer(step)
                    )
                )
        for made in across:
            made.wait_recv()
        for step in range(1, self.x_count):
            both = both + x_in[step].astype(jnp.float32)
        return both, list(pair.values()) + across


def mix_kernel(
    tp_count, partial, residual, gain, stream_ref, normed_ref, pair_in, pair_sum, x_in, held, send_sem, recv_sem
):
    exchange = Exchange(tp_count, send_sem, recv_sem)
    exchange.enter()
    rows = residual.shape[0]
    mixed, copies = exchange.total(partial, pair_in, pair_sum, x_in, rows)
    stream = residual[...].astype(jnp.float32) + mixed
    stream_ref[...] = stream
    mean = jnp.mean(stream * stream, axis=-1, keepdims=True)
    normed = (stream * lax.rsqrt(mean + EPSILON) * gain[...]).astype(jnp.bfloat16)
    held[...] = normed

    def place(index):
        return normed_ref.at[pl.ds(pl.multiple_of(index * rows, rows), rows), :]

    base, count = 2 * exchange.x_count, exchange.x_count
    sent = [exchange.copy(held, place(exchange.own), base + step, exchange.x_peer(step)) for step in range(1, count)]
    passed = [exchange.copy(held, place(exchange.own), base + count, exchange.partner)]
    normed_ref[pl.ds(pl.multiple_of(exchange.own * rows, rows), rows), :] = normed
    for step in range(1, count):
        sent[step - 1].wait_recv()
        source = exchange.x_peer(count - step)
        passed.append(
            exchange.copy(place(source), place(source), base + count + step, exchange.partner)
        )
    for made in passed:
        made.wait_recv()
    for made in copies + sent + passed:
        made.wait_send()


def sum_kernel(tp_count, partial, stream, out_ref, pair_in, pair_sum, x_in, send_sem, recv_sem):
    exchange = Exchange(tp_count, send_sem, recv_sem)
    exchange.enter()
    total, copies = exchange.total(partial, pair_in, pair_sum, x_in, stream.shape[0])
    out_ref[...] = (stream[...] + total).astype(out_ref.dtype)
    for made in copies:
        made.wait_send()


def tp_call(kernel, identity, inputs, out_shape, rows, holds):
    tp_count = lax.axis_size("tp")
    slots = (tp_count // 2, rows, inputs[0].shape[1])
    held = [pltpu.VMEM(slots[1:], jnp.bfloat16)] if holds else []
    return pl.pallas_call(
        functools.partial(kernel, tp_count),
        out_shape=out_shape,
        in_specs=[VMEM] * len(inputs),
        out_specs=jax.tree.map(lambda _: VMEM, out_shape),
        scratch_shapes=[pltpu.VMEM(slots, jnp.bfloat16)] * 3
        + held
        + [pltpu.SemaphoreType.DMA((2 * tp_count,))] * 2,
        compiler_params=pltpu.CompilerParams(
            collective_id=identity, has_side_effects=True, vmem_limit_bytes=32 * 1024 * 1024
        ),
    )(*inputs)


class Sender:
    def __init__(self, sem):
        self.sem, self.made = sem, []

    def prepare(self, src, dst, recv, target, when=None):
        copy = pltpu.make_async_remote_copy(
            src_ref=src,
            dst_ref=dst,
            send_sem=self.sem.at[len(self.made)],
            recv_sem=recv,
            device_id=target,
            device_id_type=pl.DeviceIdType.MESH,
        )
        self.made.append((when, copy))
        return lambda: run_when(when, copy.start)

    def send(self, src, dst, recv, target, when=None):
        self.prepare(src, dst, recv, target, when)()

    def finish(self):
        for when, copy in self.made:
            run_when(when, copy.wait_send)


def run_when(when, action):
    if when is None:
        action()
    else:
        pl.when(when)(lambda: action())


def layer_kernel(
    sizes,
    residual,
    q_major,
    k_major,
    v_major,
    q_minor,
    k_minor,
    v_minor,
    lam_major,
    lam_minor,
    gain_major,
    gain_minor,
    wo_major,
    wo_minor,
    mixer_gain,
    up_ref,
    down_ref,
    out_ref,
    pack,
    kv_all,
    q_in,
    qm,
    acc,
    peaks,
    totals,
    heads_out,
    cat,
    minor_in,
    wo_all,
    stream,
    normed_all,
    up_all,
    down_all,
    hidden,
    d_send,
    d_in,
    mine,
    x_send,
    x_in,
    x_keep,
    z_send,
    z_in,
    z_keep,
    send_sem,
    relay_sem,
    local_sem,
    r_y,
    r_kv,
    r_w,
    r_wo,
    r_h,
    r_g,
    r_d,
    r_x,
    r_z,
    credits,
):
    z_count, y_count, x_count = sizes
    bf16, f32 = jnp.bfloat16, jnp.float32
    own, tp = lax.axis_index("sp"), lax.axis_index("tp")
    z, y = own // y_count, lax.rem(own, y_count)
    x, c = tp // 2, lax.rem(tp, 2)
    oy, ox, oc = 1 - y, 1 - x, 1 - c
    zl = lax.rem(z, 2)
    oz = z + 1 - 2 * zl
    rows, tile = q_major.shape[0], residual.shape[0]
    width = q_minor.shape[1]
    half = width // 2
    unit = up_ref.shape[1] // UNITS
    part_size = [units * unit for units in PART_UNITS]
    part_at = [sum(part_size[:part]) for part in range(PARTS)]
    big, small = sum(part_size), sum(part_size[:-1])
    even = zl == 0
    up_rows = up_ref.shape[0]
    cols = down_ref.shape[1]

    def dev(z_at=z, y_at=y, x_at=x, c_at=c):
        return {"sp": z_at * y_count + y_at, "tp": x_at * 2 + c_at}

    def span(start, count):
        return pl.ds(pl.multiple_of(start * count, count), count)

    def arrive(place, recv):
        pltpu.make_async_remote_copy(
            src_ref=place,
            dst_ref=place,
            send_sem=send_sem.at[0],
            recv_sem=recv,
            device_id=dev(y_at=oy),
            device_id_type=pl.DeviceIdType.MESH,
        ).wait_recv()

    barrier = pltpu.get_barrier_semaphore()
    peers = []
    for dy in range(2):
        for dx in range(2):
            for dc in range(2):
                if dy or dx or dc:
                    peers.append(dev(y_at=oy if dy else y, x_at=ox if dx else x, c_at=oc if dc else c))
    peers += [dev(z_at=lax.rem(z + step, z_count)) for step in range(1, z_count)]
    for peer in peers:
        pl.semaphore_signal(barrier, inc=1, device_id=peer, device_id_type=pl.DeviceIdType.MESH)

    k_low = lax.broadcasted_iota(jnp.int32, (rows, width), 1)
    for head in range(2):
        k_part = (k_low >= head * half) & (k_low < (head + 1) * half)
        turned_v = pltpu.roll(v_minor[...].astype(f32), half, 1)
        pack[head] = jnp.where(k_part, k_minor[...].astype(f32), turned_v).astype(bf16)

    kv_all[z, 0, span(y, rows), :] = k_major[:, span(y, width)]
    kv_all[z, 1, span(y, rows), :] = v_major[:, span(y, width)]
    kv_all[z, 2, span(y, rows), :] = pack[y]
    local = []

    def weight_src(kind, z_at):
        part = kind % PARTS
        start = pl.multiple_of(lax.rem(z_at, 2) * big + part_at[part], unit) if part < PARTS - 1 else part_at[part]
        window = pl.ds(start, part_size[part])
        return up_ref.at[:, window] if kind < PARTS else down_ref.at[window, :]

    def weight_place(kind, source):
        window = pl.ds(part_at[kind % PARTS], part_size[kind % PARTS])
        return up_all.at[span(source, up_rows), window] if kind < PARTS else down_all.at[source, window, :]

    def fits(kind, z_at, when):
        if kind % PARTS < PARTS - 1:
            return when
        held = lax.rem(z_at, 2) == 0
        return held if when is None else held & when

    up_kinds, down_kinds = tuple(range(PARTS)), tuple(range(PARTS, 2 * PARTS))
    local_pairs = [
        (weight_src(kind, z), weight_place(kind, own), fits(kind, z, None)) for kind in up_kinds + down_kinds
    ]
    major_rows, minor_rows = wo_major.shape[0], wo_minor.shape[0]
    tp_count = 2 * x_count
    minor_base = tp_count * major_rows

    def wo_place(part, index):
        if part == 0:
            return wo_all.at[span(index, major_rows), :]
        return wo_all.at[pl.ds(pl.multiple_of(minor_base + index * minor_rows, minor_rows), minor_rows), :]

    for part, ref in enumerate((wo_major, wo_minor)):
        local_pairs.append((ref, wo_place(part, tp), None))
    for at, (src, dst, when) in enumerate(local_pairs):
        made = pltpu.make_async_copy(src, dst, local_sem.at[at])
        run_when(when, made.start)
        local.append((when, made))

    pl.semaphore_wait(barrier, len(peers))

    sender = Sender(send_sem)
    has_up = z < z_count - 1
    next_z = jnp.minimum(z + 1, z_count - 1)

    def kv_place(z_at, part, side):
        return kv_all.at[z_at, part, span(side, rows), :]

    for part, src in enumerate((k_major.at[:, span(oy, width)], v_major.at[:, span(oy, width)], pack.at[oy])):
        sender.send(src, kv_place(z, part, y), r_y.at[part], dev(y_at=oy))
    sender.send(q_major.at[:, span(oy, width)], q_in.at[0], r_y.at[3], dev(y_at=oy))
    sender.send(q_minor, q_in.at[1], r_y.at[4], dev(y_at=oy))
    for part, src in enumerate((k_major.at[:, span(y, width)], v_major.at[:, span(y, width)], pack.at[y])):
        sender.send(src, kv_place(z, part, y), r_kv.at[z, y, part], dev(z_at=next_z), has_up)

    def send_weight(kind, z_at, y_at, when=None):
        return sender.prepare(
            weight_src(kind, z_at),
            weight_place(kind, own),
            r_w.at[kind, own],
            dev(z_at=z_at, y_at=y_at),
            fits(kind, z_at, when),
        )

    def below(kinds, last=1, first=z_count - 1):
        return [
            send_weight(kind, jnp.maximum(z - step, 0), y, z >= step)
            for step in range(first, last - 1, -1)
            for kind in kinds
        ]

    def above(kinds, step, odd=None):
        when = z + step < z_count
        if odd is not None:
            when = when & (lax.rem(z + step, 2) == odd)
        if odd == 1:
            kinds = kinds[:-1]
        return [send_weight(kind, jnp.minimum(z + step, z_count - 1), y, when) for kind in kinds]

    def issue(starts):
        for start in starts:
            start()

    issue(below(up_kinds))
    for kind in up_kinds + down_kinds:
        send_weight(kind, z, oy)()
    for part, ref in enumerate((wo_major, wo_minor)):
        sender.send(ref, wo_place(part, tp), r_wo.at[part, tp], dev(x_at=ox))
        sender.send(ref, wo_place(part, tp), r_wo.at[part, tp], dev(c_at=oc))
    below_far, below_mid, below_near = below(down_kinds, 3), below(down_kinds, 2, 2), below(down_kinds, 1, 1)
    slow = (zl == 1) & (z > 1)
    near_up = above(up_kinds, 1)
    late_up = (zl == 0) & (z > 0)

    scales = (DK_MAJOR ** (-0.5) * LOG2_E, DK_MINOR ** (-0.5) * LOG2_E)
    lane = lax.broadcasted_iota(jnp.int32, (rows, width), 1)

    def pick(group, side, block):
        first, size = (0, DK_MAJOR) if group == 0 else (y * half, DK_MINOR)
        for m in range(MAPS):
            low = first + m * size
            keep = (lane >= low) & (lane < low + size)
            qm[group, side, m * rows : (m + 1) * rows, :] = jnp.where(keep, block.astype(f32), 0.0).astype(bf16)

    def fold(side, z_at, key_side, diagonal):
        window = span(key_side, rows)
        for group in range(2):
            keys = kv_all[z_at, 2 * group, window, :]
            stored = kv_all[z_at, 1 + group, window, :]
            values = jnp.transpose(stored.astype(f32)).astype(bf16)
            scores = lax.dot_general(
                keys, qm[group, side], (((1,), (1,)), ((), ())), preferred_element_type=f32
            ) * scales[group]
            if diagonal:
                key_pos = lax.broadcasted_iota(jnp.int32, scores.shape, 0)
                query_pos = lax.broadcasted_iota(jnp.int32, scores.shape, 1) % rows
                visible = key_pos // SEGMENT <= query_pos // SEGMENT
                scores = jnp.where(visible, scores, NEGATIVE)
            peak = jnp.max(scores, axis=0, keepdims=True)
            if not diagonal:
                peak_old = peaks[group, side]
                peak = jnp.maximum(peak, peak_old)
            weights = jnp.exp2(scores - peak)
            total = jnp.sum(weights, axis=0, keepdims=True)
            sums = jnp.dot(values, weights.astype(bf16), preferred_element_type=f32)
            if not diagonal:
                factor = jnp.exp2(peak_old - peak)
                total = total + totals[group, side] * factor
                sums = sums + acc[group, side] * factor
            peaks[group, side] = peak
            totals[group, side] = total
            acc[group, side] = sums

    pick(0, y, q_major[:, span(y, width)])
    pick(1, y, q_minor[...])
    fold(y, z, y, True)

    for part in range(3):
        arrive(kv_place(z, part, oy), r_y.at[part])
        sender.send(kv_place(z, part, oy), kv_place(z, part, oy), r_kv.at[z, oy, part], dev(z_at=next_z), has_up)

    def credit(kind, back):
        pl.semaphore_signal(
            credits.at[kind, z],
            inc=1,
            device_id=dev(z_at=jnp.maximum(z - back, 0)),
            device_id_type=pl.DeviceIdType.MESH,
        )

    def await_credit(kind, step):
        pl.semaphore_wait(credits.at[kind, jnp.minimum(z + step, z_count - 1)], 1)

    def relay_copy(z_at, side, part):
        return pltpu.make_async_remote_copy(
            src_ref=kv_place(z_at, part, side),
            dst_ref=kv_place(z_at, part, side),
            send_sem=relay_sem.at[z_at, side, part],
            recv_sem=r_kv.at[z_at, side, part],
            device_id=dev(z_at=next_z),
            device_id_type=pl.DeviceIdType.MESH,
        )

    def take(z_at, side):
        for part in range(3):
            arrive(kv_place(z_at, part, side), r_kv.at[z_at, side, part])
            run_when(has_up, relay_copy(z_at, side, part).start)

    def after_last():
        run_when(zl == 1, lambda: issue(near_up))
        for back in range(2, z_count):
            run_when(z >= back, lambda: credit(0, back))

        @pl.when(jnp.logical_not(slow))
        def _():
            issue(below_far + below_mid + below_near)

    for part in range(2):
        arrive(q_in.at[part], r_y.at[3 + part])
        pick(part, oy, q_in[part])

    pl.when(z == 0)(lambda: issue(near_up))

    @pl.when(z > 0)
    def _():
        for side in range(2):
            take(z - 1, side)

    pl.when(z == 1)(after_last)
    fold(oy, z, oy, True)
    fold(1, z, 0, False)

    def earlier(index, carry):
        z_at, key_side = z - 1 - index // 2, lax.rem(index, 2)
        pl.when(index > 1)(lambda: take(z_at, key_side))
        pl.when((index == 2 * z - 1) & (z > 1))(after_last)
        pl.when((index == 2 * z - 4) & slow)(lambda: issue(below_near))
        pl.when((index == 2 * z - 2) & slow)(lambda: issue(below_far))

        def inner(side, carry):
            fold(side, z_at, key_side, False)
            return carry

        lax.fori_loop(0, 2, inner, 0)
        return carry

    lax.fori_loop(0, 2 * z, earlier, 0)

    value_row = lax.broadcasted_iota(jnp.int32, (width, rows), 0)
    value_keep = (value_row >= oy * half) & (value_row < (oy + 1) * half)
    gains = (gain_major[...], jnp.concatenate([gain_minor[...], gain_minor[...]], axis=1))
    lams = (lam_major[y], lam_minor[y])

    def close(side, carry):
        for group in range(2):
            ratio = acc[group, side] / totals[group, side]
            diff = ratio[:, :rows] - lams[group] * ratio[:, rows:]
            if group == 1:
                diff = jnp.where(value_keep, diff, 0.0)
            count = width if group == 0 else half
            mean = jnp.sum(diff * diff, axis=0, keepdims=True) * (1.0 / count)
            done = jnp.transpose(diff * lax.rsqrt(mean + EPSILON)) * gains[group]
            heads_out[group, span(side, rows), :] = done.astype(bf16)
        return carry

    lax.fori_loop(0, 2, close, 0)

    place = tp * y_count + y

    def token_span(y_at, x_at, c_at):
        return span(y_at * (rows // tile) + x_at * 2 + c_at, tile)

    def head_place(group, index):
        return cat.at[:, span(index, width)] if group == 0 else minor_in.at[index]

    for dy, dx, dc in ((1, 1, 1), (1, 1, 0), (1, 0, 1), (1, 0, 0), (0, 1, 1), (0, 1, 0), (0, 0, 1)):
        y_at, x_at, c_at = oy if dy else y, ox if dx else x, oc if dc else c
        for group in range(2):
            sender.send(
                heads_out.at[group, token_span(y_at, x_at, c_at), :],
                head_place(group, place),
                r_h.at[group, place],
                dev(y_at=y_at, x_at=x_at, c_at=c_at),
            )
    cat[:, span(place, width)] = heads_out[0, token_span(y, x, c), :]
    minor_in[place] = heads_out[1, token_span(y, x, c), :]

    def take_weight(kind, source):
        run_when(fits(kind, z, None), lambda: arrive(weight_place(kind, source), r_w.at[kind, source]))

    def pass_weight(kind, z_at, when):
        source = z_at * y_count + y
        when = fits(kind, z, when)
        run_when(when, lambda: arrive(weight_place(kind, source), r_w.at[kind, source]))
        sender.send(weight_place(kind, source), weight_place(kind, source), r_w.at[kind, source], dev(y_at=oy), when)

    for step in range(1, z_count):
        for kind in up_kinds:
            pass_weight(kind, lax.rem(z + step, z_count), z + step < z_count)
    for step in range(2, z_count):
        run_when(z + step < z_count, lambda: await_credit(0, step))
        issue(above(up_kinds, step))

    for when, made in local:
        run_when(when, made.wait)
    for part in range(2):
        index = ox * 2 + c
        arrive(wo_place(part, index), r_wo.at[part, index])
        sender.send(wo_place(part, index), wo_place(part, index), r_wo.at[part, index], dev(c_at=oc))
    for index in (x * 2 + oc, ox * 2 + oc):
        for part in range(2):
            arrive(wo_place(part, index), r_wo.at[part, index])
    for dy, dx, dc in ((0, 0, 1), (0, 1, 0), (0, 1, 1), (1, 0, 0), (1, 0, 1), (1, 1, 0), (1, 1, 1)):
        index = ((ox if dx else x) * 2 + (oc if dc else c)) * y_count + (oy if dy else y)
        for group in range(2):
            arrive(head_place(group, index), r_h.at[group, index])
    major_width = tp_count * y_count * width
    for index in range(tp_count):
        both = minor_in[index * y_count].astype(f32) + minor_in[index * y_count + 1].astype(f32)
        cat[:, major_width + index * width : major_width + (index + 1) * width] = pltpu.roll(both, half, 1).astype(bf16)

    model = residual.shape[1]
    step_cols = 256

    def project(index, carry):
        window = span(index, step_cols)
        mixed = jnp.dot(cat[...], wo_all[:, window], preferred_element_type=f32)
        added = residual[:, window].astype(f32) + mixed
        stream[:, window] = added
        return carry + jnp.sum(added * added, axis=1, keepdims=True)

    square = lax.fori_loop(0, model // step_cols, project, jnp.zeros((tile, 1), f32))
    norm = lax.rsqrt(square * (1.0 / model) + EPSILON)

    def slot(c_at, x_at, zl_at):
        return c_at * (2 * x_count) + x_at * 2 + zl_at

    def rows_at(index):
        return normed_all.at[span(index, tile), :]

    mine_at = slot(c, x, zl)
    normed_all[span(mine_at, tile), :] = (stream[...] * norm * mixer_gain[...]).astype(bf16)

    def share(index, target):
        sender.send(rows_at(index), rows_at(index), r_g.at[index], target)

    partner, x_peer, z_peer = dev(c_at=oc), dev(x_at=ox), dev(z_at=oz)
    share(mine_at, z_peer)
    share(mine_at, x_peer)
    share(mine_at, partner)
    run_when(late_up, lambda: issue(near_up))
    run_when(slow, lambda: issue(below_mid))
    issue(above(down_kinds, 1))
    for step in range(1, z_count - 1):
        for kind in up_kinds:
            pass_weight(kind, lax.rem(z + step, z_count), z + step >= z_count)
    for step in range(z_count - 1, 0, -1):
        for kind in down_kinds:
            pass_weight(kind, lax.rem(z + step, z_count), even & (z + step < z_count))
    index = slot(c, ox, zl)
    arrive(rows_at(index), r_g.at[index])
    share(index, partner)
    for step in range(2, z_count):
        issue(above(down_kinds, step, 0))
    index = slot(c, x, 1 - zl)
    arrive(rows_at(index), r_g.at[index])
    share(index, x_peer)
    share(index, partner)
    for kind in up_kinds:
        pass_weight(kind, lax.rem(z + z_count - 1, z_count), z > 0)
    for back in range(2, z_count):
        run_when((z >= back) & (zl == 1), lambda: credit(1, back))
    for step in range(z_count - 1, 0, -1):
        for kind in down_kinds[:-1]:
            pass_weight(kind, lax.rem(z + step, z_count), (zl == 1) & ((z + step < z_count) | (z == 1)))
    for step in range(2, z_count):
        run_when((z + step < z_count) & (lax.rem(z + step, 2) == 1), lambda: await_credit(1, step))
        issue(above(down_kinds, step, 1))
    index = slot(c, ox, 1 - zl)
    arrive(rows_at(index), r_g.at[index])
    share(index, partner)
    for step in range(z_count):
        source = lax.rem(z + step, z_count) * y_count + oy
        for kind in up_kinds:
            take_weight(kind, source)

    group_rows = 2 * x_count * tile
    hid_cols = 256

    def expand(side):
        def one(index, carry):
            window = span(index, hid_cols)
            pre = jnp.dot(
                normed_all[span(side, group_rows), :], up_all[:, window], preferred_element_type=f32
            )
            hidden[span(side, group_rows), window] = jnp.square(jnp.maximum(pre, 0.0)).astype(bf16)
            return carry

        full = jnp.where(even, big // hid_cols, small // hid_cols)
        lax.fori_loop(0, full, one, 0)
        rest = big % hid_cols
        assert rest == small % hid_cols
        if rest:
            window = pl.ds(pl.multiple_of(full * hid_cols, hid_cols), rest)
            pre = jnp.dot(
                normed_all[span(side, group_rows), :], up_all[:, window], preferred_element_type=f32
            )
            hidden[span(side, group_rows), window] = jnp.square(jnp.maximum(pre, 0.0)).astype(bf16)

    expand(c)
    for x_at in range(x_count):
        for zl_at in range(2):
            index = slot(oc, x_at, zl_at)
            arrive(rows_at(index), r_g.at[index])
    expand(oc)

    for step in range(1, z_count):
        for kind in down_kinds:
            pass_weight(kind, lax.rem(z + step, z_count), even & (z + step >= z_count))

    x_rows = 2 * tile
    blocks = []

    def stage_x(t):
        arrive(d_in.at[t], r_d.at[t])
        x_send[t] = (mine[t, span(ox, x_rows), :] + d_in[t, span(ox, x_rows), :].astype(f32)).astype(bf16)
        sender.send(x_send.at[t], x_in.at[t], r_x.at[t], x_peer)
        x_keep[t] = mine[t, span(x, x_rows), :] + d_in[t, span(x, x_rows), :].astype(f32)

    def stage_z(t):
        arrive(x_in.at[t], r_x.at[t])
        other, same = span(1 - zl, tile), span(zl, tile)
        z_send[t] = (x_keep[t, other, :] + x_in[t, other, :].astype(f32)).astype(bf16)
        sender.send(z_send.at[t], z_in.at[blocks[t]], r_z.at[blocks[t]], z_peer)
        z_keep[t] = x_keep[t, same, :] + x_in[t, same, :].astype(f32)

    def stage_end(t):
        arrive(z_in.at[blocks[t]], r_z.at[blocks[t]])
        window = span(blocks[t], cols)
        total = stream[:, window] + (z_keep[t] + z_in[blocks[t]].astype(f32))
        out_ref[:, window] = total.astype(out_ref.dtype)

    reached = {stage_x: 0, stage_z: 0, stage_end: 0}

    def advance(*targets):
        for stage, target in zip((stage_x, stage_z, stage_end), targets):
            while reached[stage] < min(target, z_count * y_count):
                stage(reached[stage])
                reached[stage] += 1

    lower = [0, *range(z_count - 1, 0, -1)]
    upper = [*range(1, z_count - 1), 0, z_count - 1]

    def z_of(block):
        return lax.rem(z - zl + jnp.where(z < 2, lower[block], upper[block]), z_count)

    count = z_count
    order = [(0, 0), (0, 1), (1, 0)]
    for block in range(2, count):
        order += [(block, 0), (block - 1, 1)]
    order.append((count - 1, 1))
    late_pass = {0: [(count - 2, PARTS)], 1: [(1, PARTS)], 2: [(1, kind) for kind in down_kinds[1:-1]]}
    for t, (block, side) in enumerate(order):
        if block > 1 and not side:
            first = PARTS + 1 if block == count - 2 else PARTS
            late_pass[t] = [(block, kind) for kind in range(first, 2 * PARTS - 1)]
    for t, (block, side) in enumerate(order):
        source = z_of(block) * y_count + (oy if side else y)
        blocks.append(source)
        for ahead, kind in late_pass.get(t, ()):
            pass_weight(kind, z_of(ahead), slow)
        if t == len(order) - 1:
            advance(t, t - 2, t - 6)
        if side:
            for kind in down_kinds:
                take_weight(kind, source)
        start = sender.prepare(d_send.at[t], d_in.at[t], r_d.at[t], partner)

        def multiply(depth):
            block = down_all[source, :depth, :]
            sent = jnp.dot(hidden[span(oc, group_rows), :depth], block, preferred_element_type=f32)
            d_send[t] = sent.astype(bf16)
            start()
            mine[t] = jnp.dot(hidden[span(c, group_rows), :depth], block, preferred_element_type=f32)

        pl.when(even)(lambda: multiply(big))
        pl.when(jnp.logical_not(even))(lambda: multiply(small))
        advance(t, t - 3, t - 6)
    for t in range(len(order) + 1):
        advance(len(order), t, t - 1)
    advance(len(order), len(order), len(order))

    sender.finish()
    for step in range(1, z_count):
        for side in range(2):
            for part in range(3):
                copy = relay_copy(jnp.maximum(z - step, 0), side, part)
                run_when((z >= step) & has_up, copy.wait_send)


def fused(sp_count, tp_count, args):
    residual, q_major, _, v_major, q_minor = args[:5]
    wo_major, wo_minor, _, up_weight, down_weight = args[11:16]
    z_count, y_count = grid_sizes(sp_count)
    x_count = tp_count // 2
    rows, tile, width = q_major.shape[0], residual.shape[0], q_minor.shape[1]
    model = residual.shape[1]
    hid = up_weight.shape[1] // UNITS * sum(PART_UNITS)
    cols = down_weight.shape[1]
    features = tp_count * (wo_major.shape[0] + wo_minor.shape[0])
    group_rows = 2 * x_count * tile
    steps = sp_count
    bf16, f32 = jnp.bfloat16, jnp.float32
    dma = pltpu.SemaphoreType.DMA
    sends = 192
    hbm = pl.BlockSpec(memory_space=pltpu.HBM)
    return pl.pallas_call(
        functools.partial(layer_kernel, (z_count, y_count, x_count)),
        out_shape=jax.ShapeDtypeStruct(residual.shape, residual.dtype),
        in_specs=[VMEM] * 7 + [SMEM] * 2 + [VMEM] * 2 + [hbm] * 2 + [VMEM] + [hbm] * 2,
        out_specs=VMEM,
        scratch_shapes=[
            pltpu.VMEM((2, rows, width), bf16),
            pltpu.VMEM((z_count, 3, y_count * rows, width), bf16),
            pltpu.VMEM((2, rows, width), bf16),
            pltpu.VMEM((2, 2, MAPS * rows, width), bf16),
            pltpu.VMEM((2, 2, width, MAPS * rows), f32),
            pltpu.VMEM((2, 2, 1, MAPS * rows), f32),
            pltpu.VMEM((2, 2, 1, MAPS * rows), f32),
            pltpu.VMEM((2, y_count * rows, width), bf16),
            pltpu.VMEM((tile, features), bf16),
            pltpu.VMEM((tp_count * y_count, tile, width), bf16),
            pltpu.VMEM((features, model), bf16),
            pltpu.VMEM((tile, model), f32),
            pltpu.VMEM((2 * group_rows, model), bf16),
            pltpu.VMEM((model, hid), bf16),
            pltpu.VMEM((sp_count, hid, cols), bf16),
            pltpu.VMEM((2 * group_rows, hid), bf16),
            pltpu.VMEM((steps, group_rows, cols), bf16),
            pltpu.VMEM((steps, group_rows, cols), bf16),
            pltpu.VMEM((steps, group_rows, cols), f32),
            pltpu.VMEM((steps, 2 * tile, cols), bf16),
            pltpu.VMEM((steps, 2 * tile, cols), bf16),
            pltpu.VMEM((steps, 2 * tile, cols), f32),
            pltpu.VMEM((steps, tile, cols), bf16),
            pltpu.VMEM((steps, tile, cols), bf16),
            pltpu.VMEM((steps, tile, cols), f32),
            dma((sends,)),
            dma((z_count, 2, 3)),
            dma((2 * PARTS + 2,)),
            dma((5,)),
            dma((z_count, 2, 3)),
            dma((2 * PARTS, sp_count)),
            dma((2, tp_count)),
            dma((2, tp_count * y_count)),
            dma((2 * group_rows // tile,)),
            dma((steps,)),
            dma((steps,)),
            dma((steps,)),
            pltpu.SemaphoreType.REGULAR((2, z_count)),
        ],
        compiler_params=pltpu.CompilerParams(
            collective_id=0, has_side_effects=True, vmem_limit_bytes=63 * 1024 * 1024
        ),
    )(*args)


def fits_fused(sp_count, tp_count, args):
    q_major, k_major, v_major, q_minor, k_minor, v_minor = args[1:7]
    z_count, y_count = grid_sizes(sp_count)
    width = q_minor.shape[1]
    return (
        y_count == 2
        and tp_count == 4
        and z_count % 2 == 0
        and width == 2 * MAPS * DK_MINOR
        and width == MAPS * DK_MAJOR
        and width % 128 == 0
        and z_count >= 4
        and args[14].shape[1] % (UNITS * 128) == 0
        and v_minor.shape[1] == width
        and q_major.shape[1] == v_major.shape[1] == 2 * width
    )


def body(
    residual,
    query_major,
    keys_major,
    values_major,
    query_minor,
    keys_minor,
    values_minor,
    lambda_major,
    lambda_minor,
    gain_major,
    gain_minor,
    output_major,
    output_minor,
    mixer_gain,
    up_weight,
    down_weight,
):
    sp_count, tp_count = lax.axis_size("sp"), lax.axis_size("tp")
    args = (
        residual,
        query_major,
        keys_major,
        values_major,
        query_minor,
        keys_minor,
        values_minor,
        lambda_major,
        lambda_minor,
        gain_major[None, :],
        gain_minor[None, :],
        output_major,
        output_minor,
        mixer_gain[None, :],
        up_weight,
        down_weight,
    )
    if fits_fused(sp_count, tp_count, args):
        return fused(sp_count, tp_count, args)
    out_major, out_minor, up_full, down_full = mixer(
        lax.axis_size("sp"),
        query_major,
        keys_major,
        values_major,
        query_minor,
        jnp.concatenate([keys_minor, values_minor], axis=1),
        lambda_major,
        lambda_minor,
        gain_major[:, None],
        gain_minor[:, None],
        up_weight,
        down_weight,
    )
    partial_sum = jnp.dot(out_major, output_major, preferred_element_type=jnp.float32)
    partial_sum = partial_sum + jnp.dot(out_minor, output_minor, preferred_element_type=jnp.float32)
    rows = residual.shape[0]
    stream, normed_all = tp_call(
        mix_kernel,
        1,
        (partial_sum.astype(jnp.bfloat16), residual, mixer_gain[None, :]),
        (
            jax.ShapeDtypeStruct(residual.shape, jnp.float32),
            jax.ShapeDtypeStruct(partial_sum.shape, jnp.bfloat16),
        ),
        rows,
        True,
    )
    pre_act = jnp.dot(
        normed_all,
        up_full,
        preferred_element_type=jnp.float32,
    )
    hidden = jnp.square(jax.nn.relu(pre_act)).astype(jnp.bfloat16)
    down_part = jnp.einsum("th,shd->tsd", hidden, down_full, preferred_element_type=jnp.float32)
    down_part = down_part.astype(jnp.bfloat16).reshape(partial_sum.shape)
    return tp_call(
        sum_kernel,
        2,
        (down_part, stream),
        jax.ShapeDtypeStruct(residual.shape, residual.dtype),
        rows,
        False,
    )


def solution(mesh):
    return jax.shard_map(
        body,
        mesh=mesh,
        in_specs=(
            P(("sp", "tp"), None),
            P("sp", "tp"),
            P("sp", "tp"),
            P("sp", "tp"),
            P("sp", "tp"),
            P("sp", "tp"),
            P("sp", "tp"),
            P("tp"),
            P("tp"),
            P(),
            P(),
            P("tp", None),
            P("tp", None),
            P(),
            P("sp", "tp"),
            P("tp", "sp"),
        ),
        out_specs=P(("sp", "tp"), None),
        check_vma=False,
    )
```
